512 devices in a mesh: sp: 32 (over z, x), tp: 16 (over y, core).
Axes of the slice: x: 4, y: 8, z: 8, core: 2. Of those that a mesh axis runs over, the one named last changes fastest.
Arguments:
- probe_vectors: bfloat16 [4096, 2048], P('sp', 'tp'), may hold values from -6 to 6
- address_vectors: bfloat16 [4096, 2048], P('sp', 'tp'), may hold values from -6 to 6
- content_vectors: bfloat16 [4096, 2048], P('sp', 'tp'), may hold values from -6 to 6
- storage_raw_signal: float32 [16, 4096], P('tp', 'sp'), may hold values from -8 to 4
- fade_raw_signal: float32 [16, 4096], P('tp', 'sp'), may hold values from -6 to 6
- channel_fade_exponent: float32 [16], P('tp'), may hold values from -9 to 0
- extra_fade_amount: float32 [16, 4096], P('tp', 'sp'), may hold values from -1 to 0
- sequence_label: int32 [4096], P('sp'), may hold values from 0 to 8, never falling along the last dimension, each value on 1 to 768 neighbouring positions
- exit_valve_raw_signal: bfloat16 [4096, 2048], P('sp', 'tp'), may hold values from -6 to 6
- final_projection_matrix: bfloat16 [2048, 2048], P('tp'), may hold values from -0.125 to 0.125
- incoming_rows_matrix: bfloat16 [4096, 2048], P('sp', 'tp'), may hold values from -48 to 48
- initial_rescale_factor: float32 [2048], P('tp'), may hold values from 0 to 3
- specialist_picks: int32 [4096, 2], P('sp'), may hold values from 0 to 31, all different within a row; in each aligned block of 128 rows (0 to 127, 128 to 255, ...) at most 9 rows name the same one
- picked_specialist_share: bfloat16 [4096, 2], P('sp'), may hold values from 0.29882812 to 1.1953125
- specialist_valve_matrix: bfloat16 [32, 2048, 4096], P('sp', None, 'tp'), may hold values from -0.125 to 0.125
- specialist_raising_matrix: bfloat16 [32, 2048, 4096], P('sp', None, 'tp'), may hold values from -0.125 to 0.125
- specialist_lowering_matrix: bfloat16 [32, 4096, 2048], P('sp', 'tp'), may hold values from -0.09375 to 0.09375
- common_valve_matrix: bfloat16 [2048, 512], P(None, 'tp'), may hold values from -0.125 to 0.125
- common_raising_matrix: bfloat16 [2048, 512], P(None, 'tp'), may hold values from -0.125 to 0.125
- common_lowering_matrix: bfloat16 [512, 2048], P('tp'), may hold values from -0.25 to 0.25
- latter_rescale_factor: float32 [2048], P('tp'), may hold values from 0.1 to 1.9
Outputs:
- result: bfloat16 [4096, 2048], P('sp', 'tp')
The draws below stay inside these ranges and needn't reach their ends.
Inputs may be any that keep to these rules, and one draw needn't show every extreme that they name: `sequence_label`: document numbers never fall; a document has 1 to 768 positions, one exactly 768. `specialist_picks`: each row names 2 different experts; among the rows of one index of sp no expert is named more than 9 times, a bound that some block reaches.
All inputs are finite; a program needn't handle non-finite values.
Results may differ from the reference program's by a relative error of at most 0.018.
Values may be sent and summed in bfloat16 or wider, within the bound.
A program may use at most 64 MiB of HBM per device.

```python
import math
import jax
import jax.numpy as jnp
import numpy as np
from jax import lax

D = 2048
H = 16
DK = 128
DV = 128
BLOCK = 64
FF = 4096
SF = 512
TOP = 2
TOK_DEV = 128
TOKENS = 4096
EXPERTS = 32
CAP = 9
DOC_SPAN = 768
DOCS = 9
N_SP = 32
N_TP = 16


def slow_heads(key):
    share = 0.5
    return jax.random.bernoulli(jax.random.fold_in(key, 11), share, (H,))


def draw_channel_fade_exponent(key, part):
    slower = slow_heads(key)
    jitter = jax.random.uniform(jax.random.fold_in(key, 12), (H,), jnp.float32, -0.3, 0.3)
    slow_rate = math.log(0.6 / DOC_SPAN)
    fast_rate = math.log(2.0 / BLOCK)
    return jnp.where(slower, slow_rate, fast_rate) + jitter


def draw_storage_raw_signal(key, part):
    slower = slow_heads(key)
    base_level = jnp.where(slower, math.log(0.3 * DK / DOC_SPAN), 0.0)
    noise = jnp.clip(jax.random.normal(jax.random.fold_in(key, 13), (H, TOKENS), jnp.float32), -4.0, 4.0)
    return base_level[:, None] + noise


def draw_fade_raw_signal(key, part):
    offsets = jax.random.uniform(jax.random.fold_in(key, 14), (TOKENS // TOK_DEV,), jnp.float32, -1.2, 1.2)
    spread_out = jnp.repeat(offsets, TOK_DEV)
    noise = jnp.clip(jax.random.normal(jax.random.fold_in(key, 15), (H, TOKENS), jnp.float32), -4.0, 4.0)
    return noise + spread_out[None, :]


def draw_extra_fade_amount(key, part):
    places = jax.random.randint(jax.random.fold_in(key, 16), (H, 12), 0, TOKENS)
    depths = jax.random.uniform(jax.random.fold_in(key, 17), (H, 12), jnp.float32, math.log(0.5), math.log(0.6))
    positions = jnp.arange(TOKENS, dtype=jnp.int32)
    hits = (positions[None, None, :] == places[:, :, None]).astype(jnp.float32)
    return jnp.min(hits * depths[:, :, None], 1)


def draw_incoming_rows_matrix(key, part):
    ramp = jnp.exp(jnp.linspace(math.log(0.5), math.log(1.5), D)) * jax.random.uniform(jax.random.fold_in(key, 18), (D,), jnp.float32, 0.7, 1.3)
    row_scale = jnp.exp(jax.random.uniform(jax.random.fold_in(key, 19), (TOKENS, 1), jnp.float32, 0.0, math.log(4.0)))
    base_draw = jnp.clip(jax.random.normal(jax.random.fold_in(key, 21), (TOKENS, D), jnp.float32), -5.0, 5.0)
    return (base_draw * ramp[None, :] * row_scale).astype(jnp.bfloat16)


def draw_initial_rescale_factor(key, part):
    ramp = jnp.exp(jnp.linspace(math.log(0.6), math.log(1.8), D))
    noise = jax.random.uniform(jax.random.fold_in(key, 22), (D,), jnp.float32, 0.8, 1.2)
    return ramp * noise


def block_levels(rng, extent, pieces, smallest, top_value):
    level = 1.0
    for dim, shards_of in pieces:
        draws = jax.random.uniform(jax.random.fold_in(jax.random.fold_in(rng, 6), dim), (shards_of,), jnp.float32, smallest / len(pieces), top_value / len(pieces))
        level = level * jnp.repeat(jnp.exp(draws), extent[dim] // shards_of).reshape((-1,) + (1,) * (len(extent) - 1 - dim))
    return level


def length_profile(number_of, total, limit, skew):
    portions = [(1 << 20) // math.isqrt(grade ** skew) + 1 for grade in range(2, number_of + 1)]
    spare, counts = total - limit - (number_of - 1), [1] * (number_of - 1)
    while spare > 0:
        candidates = [i for i in range(number_of - 1) if counts[i] < limit]
        whole, left = sum([portions[i] for i in candidates]), spare
        for i in candidates:
            extra = min(limit - counts[i], max(1, left * portions[i] // whole), spare)
            counts[i] = counts[i] + extra
            spare = spare - extra
    return np.array([limit] + counts)


def uneven(own_key, amount, total, most, skew):
    if amount == 2:
        one = jax.random.randint(own_key, (), max(1, total - most), min(most, total - 1) + 1)
        return jnp.stack([one, total - one])
    lengths = jnp.asarray(length_profile(amount, total, most, skew), jnp.int32)
    pairs = (amount - 1) // 2
    donor, sink = lengths[1:1 + 2 * pairs:2], lengths[2:2 + 2 * pairs:2]
    room = jnp.minimum(donor - 1, most - sink)
    shifted = jax.random.randint(jax.random.fold_in(own_key, 1), (pairs,), 0, 1 << 20) % (room + 1)
    lengths = lengths.at[1:1 + 2 * pairs:2].set(donor - shifted).at[2:2 + 2 * pairs:2].set(sink + shifted)
    return lengths[jax.random.permutation(jax.random.fold_in(own_key, 2), amount)]


def assign_block(own_key, own, number, rows, count, top, reach, skew):
    sequence = jax.random.permutation(own_key, count)
    packed, usual = load_shares(count, rows * top, reach, skew, True), load_shares(count, rows * top, reach, skew, False)
    places = jnp.arange(count)

    def named(tallies, turn):
        used = int((tallies > 0).sum())
        fixed = max(1, used // 4)
        shifted = fixed + (places - fixed + turn * (used - fixed)) % max(1, count - fixed)
        return jnp.zeros((count,), jnp.int32).at[sequence[jnp.where(places < fixed, places, shifted)]].set(jnp.asarray(tallies, jnp.int32))

    tallies = jnp.where(number % 4 == 0, named(packed, number // 4), named(usual, number - number // 4 - 1))
    mixed = jax.random.permutation(jax.random.fold_in(own, 3), count)
    donor, sink = mixed[0:count // 2 * 2:2], mixed[1:count // 2 * 2:2]
    slack = jnp.minimum(tallies[donor] - 1, reach - tallies[sink]) // 2
    slack = jnp.where((donor == sequence[0]) | (sink == sequence[0]) | (tallies[sink] == 0), 0, jnp.maximum(slack, 0))
    shifted = jax.random.randint(jax.random.fold_in(own, 4), (count // 2,), 0, 1 << 20) % (slack + 1)
    tallies = tallies.at[donor].add(-shifted).at[sink].add(shifted)
    members = jnp.searchsorted(jnp.cumsum(tallies), jnp.arange(rows * top), side="right").astype(jnp.int32)
    table = members.reshape(top, rows).T
    table = table[jax.random.permutation(jax.random.fold_in(own, 1), rows)]
    turn = jax.random.randint(jax.random.fold_in(own, 2), (rows, 1), 0, top)
    return jnp.take_along_axis(table, (jnp.arange(top)[None, :] + turn) % top, axis=1)


def load_shares(count, total, limit, lean, full):
    weights = [(1 << 20) // math.isqrt(grade ** lean) + 1 for grade in range(1, count + 1)]
    largest = limit if full else min(limit, max(-(-total // count), total * weights[0] // sum(weights)))
    least = 1 if total - largest >= count - 1 else 0
    holding, rest = [largest] + [least] * (count - 1), total - largest - least * (count - 1)
    while rest > 0:
        free = [i for i in range(1, count) if holding[i] < largest] or [i for i in range(1, count) if holding[i] < limit]
        pool, remaining = sum([weights[i] for i in free]), rest
        for i in free:
            addition = min(limit - holding[i], max(1, remaining * weights[i] // pool), rest)
            holding[i] = holding[i] + addition
            rest = rest - addition
    return np.array(holding)


def scatter_about(key, shape, width, most, shards=(), kind=jnp.bfloat16):
    drawn = width * jax.random.normal(key, shape, jnp.float32)
    if shards:
        drawn = drawn * block_levels(key, shape, shards, -0.22, 0.18)
    return jnp.clip(drawn, -most, most).astype(kind)


def setup_inputs(seed: int = 0) -> dict:
    splits = jax.random.split(jax.random.key(seed), 22)
    probe_vectors = scatter_about(splits[0], (TOKENS, H * DK), 1.0, 6.0, ((0, 32), (1, 16)))
    address_vectors = scatter_about(splits[1], (TOKENS, H * DK), 1.0, 6.0, ((0, 32), (1, 16)))
    content_vectors = scatter_about(splits[2], (TOKENS, H * DV), 1.0, 6.0, ((0, 32), (1, 16)))
    storage_raw_signal = draw_storage_raw_signal(jax.random.fold_in(splits[21], 71), 0)
    fade_raw_signal = draw_fade_raw_signal(jax.random.fold_in(splits[21], 71), 0)
    channel_fade_exponent = draw_channel_fade_exponent(jax.random.fold_in(splits[21], 71), 0)
    extra_fade_amount = draw_extra_fade_amount(jax.random.fold_in(splits[21], 71), 0)
    sequence_label = jnp.searchsorted(jnp.cumsum(uneven(splits[7], DOCS, TOKENS, DOC_SPAN, 1)), jnp.arange(TOKENS), side="right").astype(jnp.int32)
    exit_valve_raw_signal = scatter_about(splits[8], (TOKENS, H * DV), 1.0, 6.0, ((0, 32), (1, 16)))
    final_projection_matrix = scatter_about(splits[9], (H * DV, D), (H * DV) ** -0.5, 0.125, ((0, 16),))
    incoming_rows_matrix = draw_incoming_rows_matrix(jax.random.fold_in(splits[21], 71), 0)
    initial_rescale_factor = draw_initial_rescale_factor(jax.random.fold_in(splits[21], 71), 0)
    specialist_picks_keys = jax.random.split(jax.random.fold_in(splits[12], 1), TOKENS // TOK_DEV)
    specialist_picks_turns = jax.random.permutation(jax.random.fold_in(splits[12], 3), TOKENS // TOK_DEV)
    specialist_picks = jax.vmap(lambda own, number: assign_block(jax.random.fold_in(splits[12], 2), own, number, TOK_DEV, EXPERTS, TOP, CAP, 1))(specialist_picks_keys, specialist_picks_turns).reshape((TOKENS, TOP))
    picked_specialist_share = jnp.clip(0.29882812 + 0.8964844 * jax.random.uniform(splits[13], (TOKENS, TOP), jnp.float32) ** block_levels(splits[13], (TOKENS, TOP), ((0, 32),), -0.2, 0.2), 0.29882812, 1.1953125).astype(jnp.bfloat16)
    specialist_valve_matrix = scatter_about(splits[14], (EXPERTS, D, FF), D ** -0.5, 0.125, ((0, 32), (2, 16)))
    specialist_raising_matrix = scatter_about(splits[15], (EXPERTS, D, FF), D ** -0.5, 0.125, ((0, 32), (2, 16)))
    specialist_lowering_matrix = scatter_about(splits[16], (EXPERTS, FF, D), FF ** -0.5, 0.09375, ((0, 32), (1, 16)))
    common_valve_matrix = scatter_about(splits[17], (D, SF), D ** -0.5, 0.125, ((1, 16),))
    common_raising_matrix = scatter_about(splits[18], (D, SF), D ** -0.5, 0.125, ((1, 16),))
    common_lowering_matrix = scatter_about(splits[19], (SF, D), SF ** -0.5, 0.25, ((0, 16),))
    latter_rescale_factor = jnp.clip(1.0 + 0.18 * jax.random.normal(splits[20], (D,), jnp.float32), 0.1, 1.9)
    return dict(probe_vectors=probe_vectors, address_vectors=address_vectors, content_vectors=content_vectors, storage_raw_signal=storage_raw_signal, fade_raw_signal=fade_raw_signal, channel_fade_exponent=channel_fade_exponent, extra_fade_amount=extra_fade_amount, sequence_label=sequence_label, exit_valve_raw_signal=exit_valve_raw_signal, final_projection_matrix=final_projection_matrix, incoming_rows_matrix=incoming_rows_matrix, initial_rescale_factor=initial_rescale_factor, specialist_picks=specialist_picks, picked_specialist_share=picked_specialist_share, specialist_valve_matrix=specialist_valve_matrix, specialist_raising_matrix=specialist_raising_matrix, specialist_lowering_matrix=specialist_lowering_matrix, common_valve_matrix=common_valve_matrix, common_raising_matrix=common_raising_matrix, common_lowering_matrix=common_lowering_matrix, latter_rescale_factor=latter_rescale_factor)


HIGH = lax.Precision.HIGHEST
ALPHA = 2.0 ** 0.25

def stored_value(array):
    return lax.optimization_barrier(array.astype(jnp.bfloat16)).astype(jnp.float32)

def unit_rows(array):
    return array * lax.rsqrt(lax.optimization_barrier(jnp.sum(array * array, -1, keepdims=True)) + 1e-06)

def layer_norm(summed, gain):
    row_mean = lax.optimization_barrier(jnp.mean(summed, -1, keepdims=True))
    centred = summed - row_mean
    row_var = lax.optimization_barrier(jnp.mean(centred * centred, -1, keepdims=True))
    return centred * lax.rsqrt(row_var + 1e-05) * gain

def correction_memory_layer(probe_vectors, address_vectors, content_vectors, storage_raw_signal, fade_raw_signal, channel_fade_exponent, extra_fade_amount, sequence_label):
    query_unit = unit_rows(probe_vectors.astype(jnp.float32).reshape(TOKENS, H, DK)) * DK ** (-0.5)
    key_unit = unit_rows(address_vectors.astype(jnp.float32).reshape(TOKENS, H, DK))
    value_rows = content_vectors.astype(jnp.float32).reshape(TOKENS, H, DV)
    write_gate = jax.nn.sigmoid(storage_raw_signal).T
    fade_factor = jnp.exp(extra_fade_amount - jnp.exp(channel_fade_exponent)[:, None] * jax.nn.softplus(fade_raw_signal)).T
    prior = jnp.concatenate([sequence_label[:1], sequence_label[:-1]])
    keep_state = (sequence_label == prior).astype(jnp.float32)

    def advance(carry_state, inputs):
        query_t, key_t, value_t, write_t, decay_t, keep_t = inputs
        carry_state = carry_state * keep_t
        read_back = jnp.einsum('hd,hde->he', key_t, carry_state, precision=HIGH)
        erased = carry_state - write_t[:, None, None] * key_t[:, :, None] * read_back[:, None, :]
        carry_state = decay_t[:, None, None] * erased + write_t[:, None, None] * key_t[:, :, None] * value_t[:, None, :]
        output_t = jnp.einsum('hd,hde->he', query_t, carry_state, precision=HIGH)
        return (carry_state, output_t)
    initial = jnp.zeros((H, DK, DV), jnp.float32)
    unused, memory_layer_result = lax.scan(advance, initial, (query_unit, key_unit, value_rows, write_gate, fade_factor, keep_state))
    return memory_layer_result

def expert_layer(middle, specialist_picks, picked_specialist_share, specialist_valve_matrix, specialist_raising_matrix, specialist_lowering_matrix, common_valve_matrix, common_raising_matrix, common_lowering_matrix):
    picks = TOKENS * TOP
    slots = N_SP * CAP
    flat_routes = specialist_picks.reshape(picks)
    flat_weights = picked_specialist_share.reshape(picks).astype(jnp.float32)
    group_ff = FF // N_TP
    group_sf = SF // N_TP

    def visit(total, expert):
        chosen = flat_routes == expert
        rank_in = jnp.cumsum(chosen.astype(jnp.int32)) - 1
        target = jnp.where(chosen, rank_in, slots)
        owner = jnp.full((slots,), picks, jnp.int32).at[target].set(jnp.arange(picks, dtype=jnp.int32), mode='drop')
        live = (owner < picks).astype(jnp.float32)
        safe_owner = jnp.minimum(owner, picks - 1)
        source_row = safe_owner // TOP
        shared_flag = (safe_owner % TOP == 0).astype(jnp.float32) * live
        weight_e = flat_weights[safe_owner] * live
        inputs_e = middle[source_row]
        gate_e = jnp.dot(inputs_e, specialist_valve_matrix[expert], preferred_element_type=jnp.float32)
        up_e = jnp.dot(inputs_e, specialist_raising_matrix[expert], preferred_element_type=jnp.float32)
        hidden_e = (jax.nn.silu(gate_e) * up_e * weight_e[:, None]).astype(jnp.bfloat16)
        shared_g = jnp.dot(inputs_e, common_valve_matrix, preferred_element_type=jnp.float32)
        shared_u = jnp.dot(inputs_e, common_raising_matrix, preferred_element_type=jnp.float32)
        shared_hidden = (jax.nn.silu(shared_g) * shared_u * shared_flag[:, None]).astype(jnp.bfloat16)
        down_e = specialist_lowering_matrix[expert]
        summed = jnp.zeros((slots, D), jnp.float32)
        for group in range(N_TP):
            term = jnp.dot(hidden_e[:, group * group_ff:(group + 1) * group_ff], down_e[group * group_ff:(group + 1) * group_ff], preferred_element_type=jnp.float32)
            term = term + jnp.dot(shared_hidden[:, group * group_sf:(group + 1) * group_sf], common_lowering_matrix[group * group_sf:(group + 1) * group_sf], preferred_element_type=jnp.float32)
            summed = summed + stored_value(term)
        route_out = stored_value(summed)
        total = total.at[source_row].add(route_out * live[:, None])
        return (total, None)
    start = jnp.zeros((TOKENS, D), jnp.float32)
    mixture, unused = lax.scan(visit, start, jnp.arange(EXPERTS, dtype=jnp.int32))
    return mixture

def reference(probe_vectors, address_vectors, content_vectors, storage_raw_signal, fade_raw_signal, channel_fade_exponent, extra_fade_amount, sequence_label, exit_valve_raw_signal, final_projection_matrix, incoming_rows_matrix, initial_rescale_factor, specialist_picks, picked_specialist_share, specialist_valve_matrix, specialist_raising_matrix, specialist_lowering_matrix, common_valve_matrix, common_raising_matrix, common_lowering_matrix, latter_rescale_factor):
    memory_layer_result = correction_memory_layer(probe_vectors, address_vectors, content_vectors, storage_raw_signal, fade_raw_signal, channel_fade_exponent, extra_fade_amount, sequence_label)
    scaled = memory_layer_result * lax.rsqrt(lax.optimization_barrier(jnp.mean(memory_layer_result * memory_layer_result, -1, keepdims=True)) + 1e-06)
    heads_out = (scaled.reshape(TOKENS, H * DV) * jax.nn.silu(exit_valve_raw_signal.astype(jnp.float32))).astype(jnp.bfloat16)
    group_rows = H * DV // N_TP
    projected = jnp.zeros((TOKENS, D), jnp.float32)
    for group in range(N_TP):
        term = jnp.dot(heads_out[:, group * group_rows:(group + 1) * group_rows], final_projection_matrix[group * group_rows:(group + 1) * group_rows], preferred_element_type=jnp.float32)
        projected = projected + stored_value(term)
    first_sum = ALPHA * incoming_rows_matrix.astype(jnp.float32) + projected
    middle = layer_norm(first_sum, initial_rescale_factor).astype(jnp.bfloat16)
    mixture = expert_layer(middle, specialist_picks, picked_specialist_share, specialist_valve_matrix, specialist_raising_matrix, specialist_lowering_matrix, common_valve_matrix, common_raising_matrix, common_lowering_matrix)
    second_sum = ALPHA * middle.astype(jnp.float32) + mixture
    return layer_norm(second_sum, latter_rescale_factor).astype(jnp.bfloat16)
```

```python
import functools

import jax
import jax.numpy as jnp
from jax import lax
from jax.experimental import pallas as pl
from jax.experimental.pallas import tpu as pltpu
from jax.sharding import PartitionSpec as P

BLOCK = 64
ALPHA = 2.0**0.25
F32 = jnp.float32
BF16 = jnp.bfloat16
MESH = pl.DeviceIdType.MESH
REACH = 3


def iota(shape, dim):
    return lax.broadcasted_iota(jnp.int32, shape, dim)


def mm(a, b):
    return jnp.dot(a.astype(BF16), b.astype(BF16), preferred_element_type=F32)


def mm_nt(a, b):
    return lax.dot_general(
        a.astype(BF16), b.astype(BF16), (((1,), (1,)), ((), ())), preferred_element_type=F32
    )


def mm_tn(a, b):
    return lax.dot_general(
        a.astype(BF16), b.astype(BF16), (((0,), (0,)), ((), ())), preferred_element_type=F32
    )


def silu(v):
    return v / (1.0 + jnp.exp(-v))


def kernel(dims, *refs):
    n_sp, n_tp, rows, experts, cap, stride = dims
    ny = n_tp // 2
    slots = n_sp * cap
    padded = n_sp * stride
    names = dims_names()
    hbm = dict(zip(names, refs[: len(names)]))
    chan_ref, out_hbm = refs[len(names)], refs[len(names) + 1]
    scratch = refs[len(names) + 2 :]
    vm = dict(zip(names, scratch[: len(names)]))
    (
        prev_label, pay, pieces, carry_out, carry_in,
        part1, pair1, send1, recv1,
        stat1, stat2,
        sent, arrived, gathered, acc_g, acc_s,
        part2, pair2, send2, recv2,
        rsend, returned, out_vm,
        load_sem, out_sem, lab_sem, pa_s, pa_r, pb_s,
        d1_s, d1_r, y1_s, y1_r, st1_s, st1_r,
        dis_s, dis_r, big_s, big_r, small_s, small_r, own_s, own_r,
        d2_s, d2_r, y2_s, y2_r, ret_s, ret_r, st2_s, st2_r,
    ) = scratch[len(names) :]

    s = lax.axis_index("sp")
    t = lax.axis_index("tp")
    y = t // 2
    c = lax.rem(t, 2)
    other = 1 - c

    def at_sp(k):
        return {"sp": k, "tp": t}

    def at_tp(k):
        return {"sp": s, "tp": k}

    def remote(src, dst, send_sem, recv_sem, device):
        return pltpu.make_async_remote_copy(
            src_ref=src, dst_ref=dst, send_sem=send_sem, recv_sem=recv_sem,
            device_id=device, device_id_type=MESH,
        )

    loads = {
        name: pltpu.make_async_copy(hbm[name], vm[name], load_sem.at[k])
        for k, name in enumerate(names)
    }
    for name in names:
        loads[name].start()
    barrier = pltpu.get_barrier_semaphore()

    def greet_sp(k, carry):
        pl.semaphore_signal(
            barrier, inc=1, device_id=at_sp(lax.rem(s + k, n_sp)), device_id_type=MESH
        )
        return carry

    def greet_tp(k, carry):
        pl.semaphore_signal(
            barrier, inc=1, device_id=at_tp(lax.rem(t + k, n_tp)), device_id_type=MESH
        )
        return carry

    lax.fori_loop(1, n_sp, greet_sp, 0)
    lax.fori_loop(1, n_tp, greet_tp, 0)

    for name in ("probe", "address", "content", "storage", "fade", "extra", "label"):
        loads[name].wait()
    pl.semaphore_wait(barrier, n_sp + n_tp - 2)
    lab_copy = remote(
        vm["label"], prev_label, lab_sem.at[0], lab_sem.at[1], at_sp(lax.rem(s + 1, n_sp))
    )
    lab_copy.start()

    row_i, col_i = iota((rows, rows), 0), iota((rows, rows), 1)
    eye = row_i == col_i
    lower, strict = row_i >= col_i, row_i > col_i
    same_block = (row_i < BLOCK) == (col_i < BLOCK)

    def to_col(row):
        return jnp.sum(jnp.where(eye, row, 0.0), axis=1, keepdims=True)

    def to_row(col):
        return jnp.sum(jnp.where(eye, col, 0.0), axis=0, keepdims=True)

    queries = vm["probe"][...].astype(F32)
    keys = vm["address"][...].astype(F32)
    values = vm["content"][...].astype(F32)
    q_unit = queries * lax.rsqrt(
        jnp.sum(queries * queries, -1, keepdims=True) + 1e-06
    ) * queries.shape[-1] ** (-0.5)
    k_unit = keys * lax.rsqrt(jnp.sum(keys * keys, -1, keepdims=True) + 1e-06)
    gate = to_col(1.0 / (1.0 + jnp.exp(-vm["storage"][...])))
    fade = vm["fade"][...]
    softplus = jnp.maximum(fade, 0.0) + jnp.log(1.0 + jnp.exp(-jnp.abs(fade)))
    rate = jnp.exp(jnp.full(fade.shape, chan_ref[0], F32))
    decay = vm["extra"][...] - rate * softplus
    c_col = jnp.sum(jnp.where(lower, decay, 0.0), axis=1, keepdims=True)
    c_row = to_row(c_col)
    label_row = vm["label"][...].astype(F32)
    label_col = to_col(label_row)
    label_first, label_last = label_row[:, :1], label_row[:, rows - 1 :]
    c_last = c_row[:, rows - 1 :]
    reach = jnp.where(
        lower & (label_col == label_row), jnp.exp(jnp.where(lower, c_col - c_row, 0.0)), 0.0
    )
    weighted = k_unit * gate
    coupling = jnp.where(strict, mm_nt(weighted, k_unit) * reach, 0.0)
    power = jnp.where(same_block, coupling, 0.0)
    across = jnp.where(same_block, 0.0, coupling)
    inverse = jnp.where(eye, 1.0, 0.0) - power
    for _ in range(BLOCK.bit_length() - 2):
        power = mm(power, power)
        inverse = inverse + mm(inverse, power)
    inverse = inverse - mm(inverse, mm(across, inverse))
    growth = jnp.exp(c_col) * (label_col == label_first).astype(F32)
    both = mm(inverse, jnp.concatenate([weighted * growth, values * gate], axis=1))
    tail_keys = k_unit * (jnp.exp(c_last - c_col) * (label_col == label_last).astype(F32))
    ends = mm_tn(tail_keys, both)
    end_growth = jnp.exp(c_last) * (label_last == label_first).astype(F32)
    scores = mm_nt(q_unit, k_unit) * reach
    outs = mm(scores, both)
    width = q_unit.shape[-1]
    q_grown = q_unit * growth - outs[:, :width]
    own_mixed = outs[:, width:]
    lab_copy.wait()
    joined = (label_first == prev_label[...].astype(F32)[:, rows - 1 :]).astype(F32)
    state_map = (jnp.where(eye, end_growth, 0.0) - ends[:, :width]) * joined
    pay[0:width, :] = state_map.astype(BF16)
    pay[width:, :] = ends[:, width:].astype(BF16)
    first = [
        remote(pay, pieces.at[k], pa_s.at[k], pa_r.at[k], at_sp(lax.rem(s + k + 1, n_sp)))
        for k in range(REACH)
    ]
    for k in reversed(range(REACH)):
        first[k].start()

    for name in names:
        if name not in ("probe", "address", "content", "storage", "fade", "extra", "label"):
            loads[name].wait()
    pick0, pick1 = vm["picks"][0:1, :], vm["picks"][1:2, :]
    share = vm["share"][...].astype(F32)
    expert_i = iota((experts, rows), 0)
    to0, to1 = (expert_i == pick0).astype(F32), (expert_i == pick1).astype(F32)
    chosen = to0 + to1
    rank = mm(chosen, (row_i < col_i).astype(F32))
    coded = jnp.where(chosen > 0.0, rank + 1.0, 0.0)
    shares = to0 * share[0:1, :] + to1 * share[1:2, :]
    slot_i = iota((padded, experts), 0)
    from_e = iota((padded, experts), 1) * stride
    spread = ((slot_i >= from_e) & (slot_i < from_e + stride)).astype(F32)
    place = iota((n_sp, stride, rows), 1).reshape(padded, rows)
    wide = mm(spread, jnp.concatenate([coded, shares, to0], axis=1))
    hot = wide[:, :rows] == (place + 1).astype(F32)
    dispatch = hot.astype(BF16)
    slot_share = jnp.sum(jnp.where(hot, wide[:, rows : 2 * rows], 0.0), axis=1, keepdims=True)
    slot_first = jnp.sum(jnp.where(hot, wide[:, 2 * rows :], 0.0), axis=1, keepdims=True)
    lane = iota((padded, rows), 1)
    here = (lane == place).astype(F32)
    told = mm_tn(spread, jnp.concatenate([here * slot_share, here * slot_first], axis=1))
    told = mm(spread, told)
    notes = jnp.where(place == cap, told[:, :rows], 0.0) + jnp.where(
        place == cap + 1, told[:, rows:], 0.0
    )
    compact_i = iota((slots, padded), 0).astype(F32)
    source = jnp.floor((compact_i + 0.5) * (1.0 / cap))
    within = compact_i - source * cap
    column = iota((slots, padded), 1).astype(F32)
    compact = (column == source * stride + within).astype(BF16)
    note_row = (column == source * stride + cap).astype(BF16)
    flag_row = (column == source * stride + cap + 1).astype(BF16)
    slot_lane = iota((slots, rows), 1).astype(F32) == within[:, :rows]

    for k in range(REACH):
        first[k].wait_recv()
    map1, shift1 = pieces[0, 0:width, :], pieces[0, width:, :].astype(F32)
    map2, shift2 = pieces[1, 0:width, :], pieces[1, width:, :].astype(F32)
    map3, shift3 = pieces[2, 0:width, :], pieces[2, width:, :]
    shift23 = shift2 + mm(map2, shift3)
    shift123 = shift1 + mm(map1, shift23)
    carry_out[...] = shift123.astype(BF16)
    second = remote(
        carry_out, carry_in, pb_s.at[0], pb_s.at[1], at_sp(lax.rem(s + REACH, n_sp))
    )
    second.start()
    map123 = mm(mm(map1, map2), map3)
    valve = silu(vm["exit"][...].astype(F32))
    second.wait_recv()
    incoming = (shift123 + mm(map123, carry_in[...])) * joined
    mixed = own_mixed + mm(q_grown, incoming)
    scaled = mixed * lax.rsqrt(jnp.mean(mixed * mixed, -1, keepdims=True) + 1e-06)
    heads_out = (scaled * valve).astype(BF16)

    far_first = sorted(range(1, ny), key=lambda k: -min(k, ny - k))

    def scattered_sum(part, pair, send, recv, d_s, d_r, y_s, y_r):
        near = {}
        for k in far_first + [0]:
            chip = lax.rem(y + k, ny)
            near[k] = remote(
                part.at[chip, other], pair.at[chip], d_s.at[k], d_r.at[k], at_tp(2 * y + other)
            )
            near[k].start()
        far = {}
        for k in far_first:
            chip = lax.rem(y + k, ny)
            near[k].wait_recv()
            send[chip] = (part[chip, c].astype(F32) + pair[chip].astype(F32)).astype(BF16)
            far[k] = remote(send.at[chip], recv.at[y], y_s.at[k], y_r.at[k], at_tp(2 * chip + c))
            far[k].start()
        near[0].wait_recv()
        total = part[y, c].astype(F32) + pair[y].astype(F32)
        for k in reversed(far_first):
            far[k].wait_recv()
            total = total + recv[lax.rem(y - k + ny, ny)].astype(F32)
        for k in near:
            near[k].wait_send()
        for k in far:
            far[k].wait_send()
        return total

    for chip in range(ny):
        product = mm(heads_out, vm["final"][:, chip * 2 * width : (chip + 1) * 2 * width])
        part1[chip, 0] = product[:, :width].astype(BF16)
        part1[chip, 1] = product[:, width:].astype(BF16)
    projected = scattered_sum(part1, pair1, send1, recv1, d1_s, d1_r, y1_s, y1_r)

    def normed(summed, gain, stat, s_sem, r_sem):
        features = summed.shape[-1] * n_tp
        stat[t, 0:1, :] = to_row(jnp.sum(summed, -1, keepdims=True))
        stat[t, 1:2, :] = to_row(jnp.sum(summed * summed, -1, keepdims=True))
        told = [
            remote(
                stat.at[t], stat.at[t], s_sem.at[k], r_sem.at[k], at_tp(lax.rem(t + k, n_tp))
            )
            for k in range(1, n_tp)
        ]
        for copy in told:
            copy.start()
        for copy in told:
            copy.wait()
        totals = jnp.sum(stat[...], axis=0)
        mean = totals[0:1, :] / features
        var = totals[1:2, :] / features - mean * mean
        scale = lax.rsqrt(var + 1e-05)
        return (summed - to_col(mean)) * to_col(scale) * gain

    first_sum = ALPHA * vm["incoming"][...].astype(F32) + projected
    middle = normed(first_sum, vm["gain1"][...], stat1, st1_s, st1_r).astype(BF16)

    def exchange(src, dst, s_sem, r_sem):
        def copy(k):
            to = lax.rem(s + k, n_sp)
            return remote(src.at[to], dst.at[s], s_sem.at[k], r_sem.at[k], at_sp(to))

        def start(k, carry):
            copy(k).start()
            return carry

        def finish(k, carry):
            copy(k).wait()
            return carry

        lax.fori_loop(1, n_sp, start, 0)
        dst[s] = src[s]
        lax.fori_loop(1, n_sp, finish, 0)
        return dst[...].reshape(padded, -1)

    payload = jnp.dot(dispatch, middle, preferred_element_type=F32) + notes
    sent[...] = payload.astype(BF16).reshape(n_sp, stride, rows)
    came = exchange(sent, arrived, dis_s, dis_r)
    own_rows = jnp.dot(compact, came, preferred_element_type=F32).astype(BF16)

    lanes = pl.ds(pl.multiple_of(c * width, width), width)
    ahead = lax.rem(y + 1 - 2 * c + ny, ny)
    behind = lax.rem(y - 1 + 2 * c + ny, ny)
    most, least = ny // 2, (ny - 1) // 2

    def origin(k):
        return lax.rem(y - k * (1 - 2 * c) + 2 * ny, ny)

    gathered[y, :, lanes] = own_rows

    def block(chip):
        return gathered.at[chip, :, lanes]

    def hand(k, chip):
        return remote(block(chip), block(chip), own_s.at[k], own_r.at[k], at_tp(2 * y + other))

    def big(k):
        chip = origin(k)
        return remote(block(chip), block(chip), big_s.at[k], big_r.at[k], at_tp(2 * ahead + c))

    def small(k):
        chip = origin(-k)
        return remote(
            block(chip), block(chip), small_s.at[k], small_r.at[k], at_tp(2 * behind + c)
        )

    def big_wait(k):
        chip = origin(k + 1)
        remote(
            block(chip), block(chip), big_s.at[k], big_r.at[k], at_tp(2 * ahead + c)
        ).wait_recv()

    def small_wait(k):
        chip = origin(-k - 1)
        remote(
            block(chip), block(chip), small_s.at[k], small_r.at[k], at_tp(2 * behind + c)
        ).wait_recv()

    def hand_wait(k, chip):
        other_lanes = pl.ds(pl.multiple_of(other * width, width), width)
        there = gathered.at[chip, :, other_lanes]
        remote(there, there, own_s.at[k], own_r.at[k], at_tp(2 * y + other)).wait_recv()

    def absorb(chip, fresh):
        block_in = gathered[chip]
        at = pl.ds(pl.multiple_of(chip * 2 * width, 2 * width), 2 * width)
        gates = jnp.dot(block_in, vm["valve"][at, :], preferred_element_type=F32)
        ups = jnp.dot(block_in, vm["raise"][at, :], preferred_element_type=F32)
        common = lax.dot_general(
            block_in, vm["common"][:, at], (((1,), (1,)), ((), ())), preferred_element_type=F32
        )
        if fresh:
            acc_g[0], acc_g[1], acc_s[...] = gates, ups, common
        else:
            acc_g[0] += gates
            acc_g[1] += ups
            acc_s[...] += common

    big(0).start()
    if least:
        small(0).start()
    hand(0, y).start()
    share_rows = jnp.dot(note_row, came, preferred_element_type=F32)
    slot_weight = jnp.sum(jnp.where(slot_lane, share_rows, 0.0), axis=1, keepdims=True)
    flag_rows = jnp.dot(flag_row, came, preferred_element_type=F32)
    slot_flag = jnp.sum(jnp.where(slot_lane, flag_rows, 0.0), axis=1, keepdims=True)
    hand_wait(0, y)
    absorb(y, True)
    for k in range(1, most + 1):
        big_wait(k - 1)
        if k < most:
            big(k).start()
        hand(2 * k - 1, origin(k)).start()
        if k <= least:
            small_wait(k - 1)
            if k < least:
                small(k).start()
            hand(2 * k, origin(-k)).start()
        hand_wait(2 * k - 1, origin(-k))
        absorb(origin(-k), False)
        if k <= least:
            hand_wait(2 * k, origin(k))
            absorb(origin(k), False)

    hidden = (silu(acc_g[0]) * acc_g[1] * slot_weight).astype(BF16)
    sf = acc_s.shape[1] // 2
    common = acc_s[...]
    shared = (silu(common[:, :sf]) * common[:, sf:] * slot_flag).astype(BF16)
    for chip in range(ny):
        at = slice(chip * 2 * width, (chip + 1) * 2 * width)
        product = jnp.dot(hidden, vm["lower"][:, at], preferred_element_type=F32) + jnp.dot(
            shared, vm["common_low"][:, at], preferred_element_type=F32
        )
        part2[chip, 0] = product[:, :width].astype(BF16)
        part2[chip, 1] = product[:, width:].astype(BF16)
    summed = scattered_sum(part2, pair2, send2, recv2, d2_s, d2_r, y2_s, y2_r)

    rsend[...] = mm_tn(compact, summed).astype(BF16).reshape(n_sp, stride, rows)
    back = exchange(rsend, returned, ret_s, ret_r)
    mixture = mm_tn(dispatch, back)
    second_sum = ALPHA * middle.astype(F32) + mixture
    out_vm[...] = normed(second_sum, vm["gain2"][...], stat2, st2_s, st2_r).astype(BF16)
    out_copy = pltpu.make_async_copy(out_vm, out_hbm, out_sem)
    out_copy.start()

    for copy in first:
        copy.wait_send()
    second.wait_send()
    for k in range(most):
        big(k).wait_send()
        hand(2 * k + 1, origin(k + 1)).wait_send()
    for k in range(least):
        small(k).wait_send()
        hand(2 * k + 2, origin(-k - 1)).wait_send()
    hand(0, y).wait_send()
    out_copy.wait()


def dims_names():
    return (
        "probe", "address", "content", "storage", "fade", "extra", "label",
        "picks", "share", "exit", "incoming", "gain1", "gain2", "final",
        "valve", "raise", "lower", "common", "common_low",
    )


def shards(
    probe, address, content, storage, fade, channel, extra, label, exit_valve, final,
    incoming, gain1, picks, share, valve, raising, lowering, common_valve, common_raising,
    common_lowering, gain2,
):
    n_sp, n_tp = lax.axis_size("sp"), lax.axis_size("tp")
    ny = n_tp // 2
    rows, width = probe.shape
    experts = n_sp * valve.shape[0]
    cap = max(2, 9 * rows * picks.shape[1] // (8 * experts))
    stride = -(-(cap + 2) // 16) * 16
    slots = n_sp * cap
    ff, features = valve.shape[2], valve.shape[1]
    sf = common_valve.shape[1]
    dims = (n_sp, n_tp, rows, experts, cap, stride)
    args = {
        "probe": probe, "address": address, "content": content, "storage": storage,
        "fade": fade, "extra": extra, "label": label[None, :], "picks": picks.T,
        "share": share.T, "exit": exit_valve, "incoming": incoming, "gain1": gain1[None, :],
        "gain2": gain2[None, :], "final": final, "valve": valve[0], "raise": raising[0],
        "lower": lowering[0],
        "common": jnp.concatenate([common_valve.T, common_raising.T], axis=0),
        "common_low": common_lowering,
    }
    names = dims_names()
    operands = [args[n] for n in names]
    dma = pltpu.SemaphoreType.DMA
    own = [pltpu.VMEM(a.shape, a.dtype) for a in operands]

    def vmem(*shape, kind=BF16):
        return pltpu.VMEM(shape, kind)

    return pl.pallas_call(
        functools.partial(kernel, dims),
        out_shape=jax.ShapeDtypeStruct((rows, width), BF16),
        in_specs=[pl.BlockSpec(memory_space=pl.ANY)] * len(operands)
        + [pl.BlockSpec(memory_space=pltpu.SMEM)],
        out_specs=pl.BlockSpec(memory_space=pl.ANY),
        scratch_shapes=own
        + [
            vmem(1, rows, kind=jnp.int32), vmem(2 * width, width), vmem(REACH, 2 * width, width),
            vmem(width, width), vmem(width, width),
            vmem(ny, 2, rows, width), vmem(ny, rows, width), vmem(ny, rows, width),
            vmem(ny, rows, width),
            vmem(n_tp, 2, rows, kind=F32), vmem(n_tp, 2, rows, kind=F32),
            vmem(n_sp, stride, width), vmem(n_sp, stride, width),
            vmem(ny, slots, 2 * width), vmem(2, slots, ff, kind=F32), vmem(slots, 2 * sf, kind=F32),
            vmem(ny, 2, slots, width), vmem(ny, slots, width), vmem(ny, slots, width),
            vmem(ny, slots, width),
            vmem(n_sp, stride, width), vmem(n_sp, stride, width), vmem(rows, width),
            dma((len(operands),)), dma, dma((2,)), dma((REACH,)), dma((REACH,)), dma((2,)),
            dma((ny,)), dma((ny,)), dma((ny,)), dma((ny,)), dma((n_tp,)), dma((n_tp,)),
            dma((n_sp,)), dma((n_sp,)), dma((ny,)), dma((ny,)), dma((ny,)), dma((ny,)),
            dma((ny,)), dma((ny,)),
            dma((ny,)), dma((ny,)), dma((ny,)), dma((ny,)), dma((n_sp,)), dma((n_sp,)),
            dma((n_tp,)), dma((n_tp,)),
        ],
        compiler_params=pltpu.CompilerParams(
            collective_id=0, has_side_effects=True, vmem_limit_bytes=60 * 1024 * 1024
        ),
        name="layer",
    )(*operands, channel)


def solution(mesh):
    return jax.shard_map(
        shards,
        mesh=mesh,
        in_specs=(
            P("sp", "tp"), P("sp", "tp"), P("sp", "tp"), P("tp", "sp"), P("tp", "sp"), P("tp"),
            P("tp", "sp"), P("sp"), P("sp", "tp"), P("tp", None), P("sp", "tp"), P("tp"),
            P("sp", None), P("sp", None), P("sp", None, "tp"), P("sp", None, "tp"),
            P("sp", "tp", None), P(None, "tp"), P(None, "tp"), P("tp", None), P("tp"),
        ),
        out_specs=P("sp", "tp"),
        check_vma=False,
    )
```

```python
import functools

import jax
import jax.numpy as jnp
from jax import lax
from jax.experimental import pallas as pl
from jax.experimental.pallas import tpu as pltpu
from jax.sharding import PartitionSpec as P

BLOCK = 64
ALPHA = 2.0**0.25
F32 = jnp.float32
BF16 = jnp.bfloat16
MESH = pl.DeviceIdType.MESH
REACH = 3


def iota(shape, dim):
    return lax.broadcasted_iota(jnp.int32, shape, dim)


def mm(a, b):
    return jnp.dot(a.astype(BF16), b.astype(BF16), preferred_element_type=F32)


def mm_nt(a, b):
    return lax.dot_general(
        a.astype(BF16), b.astype(BF16), (((1,), (1,)), ((), ())), preferred_element_type=F32
    )


def mm_tn(a, b):
    return lax.dot_general(
        a.astype(BF16), b.astype(BF16), (((0,), (0,)), ((), ())), preferred_element_type=F32
    )


def silu(v):
    return v / (1.0 + jnp.exp(-v))


def kernel(dims, *refs):
    n_sp, n_tp, rows, experts, cap, stride = dims
    ny = n_tp // 2
    slots = n_sp * cap
    padded = n_sp * stride
    names = dims_names()
    hbm = dict(zip(names, refs[: len(names)]))
    out_hbm = refs[len(names)]
    scratch = refs[len(names) + 1 :]
    vm = dict(zip(names, scratch[: len(names)]))
    (
        pay, pieces, carry_out, carry_in,
        part1, pair1, send1, recv1,
        stat0, stat1, stat2,
        sent, arrived, told, heard, gathered, acc_g, acc_s,
        part2, pair2, send2, recv2,
        rsend, returned, out_vm,
        load_sem, out_sem, pa_s, pa_r, pb_s,
        d1_r, y1_r, mean_s, sq1_s, sq2_s,
        dis_s, note_s, ret_s, big_r, small_r, own_r, gone_s,
        d2_r, y2_r,
    ) = scratch[len(names) :]

    s = lax.axis_index("sp")
    t = lax.axis_index("tp")
    y = t // 2
    c = lax.rem(t, 2)
    other = 1 - c

    def at_sp(k):
        return {"sp": k, "tp": t}

    def at_tp(k):
        return {"sp": s, "tp": k}

    def remote(src, dst, send_sem, recv_sem, device):
        return pltpu.make_async_remote_copy(
            src_ref=src, dst_ref=dst, send_sem=send_sem, recv_sem=recv_sem,
            device_id=device, device_id_type=MESH,
        )

    barrier = pltpu.get_barrier_semaphore()

    def greet_sp(k, carry):
        pl.semaphore_signal(
            barrier, inc=1, device_id=at_sp(lax.rem(s + k, n_sp)), device_id_type=MESH
        )
        return carry

    def greet_tp(k, carry):
        pl.semaphore_signal(
            barrier, inc=1, device_id=at_tp(lax.rem(t + k, n_tp)), device_id_type=MESH
        )
        return carry

    lax.fori_loop(1, n_sp, greet_sp, 0)
    lax.fori_loop(1, n_tp, greet_tp, 0)
    sf = vm["common"].shape[0] // 2
    loads = {}
    for k, name in enumerate(names):
        into = vm[name]
        if name == "common":
            into = vm["common"].at[0:sf]
        if name == "common_raise":
            into = vm["common"].at[sf:]
        loads[name] = pltpu.make_async_copy(hbm[name], into, load_sem.at[k])
    early = ("probe", "address", "content", "storage", "fade", "extra", "channel", "label")
    for name in early:
        loads[name].start()
    for name in names:
        if name not in early:
            loads[name].start()
    for name in early:
        loads[name].wait()

    row_i, col_i = iota((rows, rows), 0), iota((rows, rows), 1)
    eye = row_i == col_i
    lower, strict = row_i >= col_i, row_i > col_i
    same_block = (row_i < BLOCK) == (col_i < BLOCK)

    def to_col(row):
        return jnp.sum(jnp.where(eye, row, 0.0), axis=1, keepdims=True)

    def to_row(col):
        return jnp.sum(jnp.where(eye, col, 0.0), axis=0, keepdims=True)

    queries = vm["probe"][...].astype(F32)
    keys = vm["address"][...].astype(F32)
    values = vm["content"][...].astype(F32)
    q_unit = queries * lax.rsqrt(
        jnp.sum(queries * queries, -1, keepdims=True) + 1e-06
    ) * queries.shape[-1] ** (-0.5)
    k_unit = keys * lax.rsqrt(jnp.sum(keys * keys, -1, keepdims=True) + 1e-06)
    gate = to_col(1.0 / (1.0 + jnp.exp(-vm["storage"][...])))
    fade = vm["fade"][...]
    softplus = jnp.maximum(fade, 0.0) + jnp.log(1.0 + jnp.exp(-jnp.abs(fade)))
    rate = jnp.exp(vm["channel"][...])
    decay = vm["extra"][...] - rate * softplus
    c_col = jnp.sum(jnp.where(lower, decay, 0.0), axis=1, keepdims=True)
    c_row = to_row(c_col)
    label_row = vm["label"][...].astype(F32)
    label_col = to_col(label_row)
    label_first, label_last = label_row[:, :1], label_row[:, rows - 1 :]
    c_last = c_row[:, rows - 1 :]
    reach = jnp.where(
        lower & (label_col == label_row), jnp.exp(jnp.where(lower, c_col - c_row, 0.0)), 0.0
    )
    weighted = k_unit * gate
    coupling = jnp.where(strict, mm_nt(weighted, k_unit) * reach, 0.0)
    power = jnp.where(same_block, coupling, 0.0)
    across = jnp.where(same_block, 0.0, coupling)
    inverse = jnp.where(eye, 1.0, 0.0) - power
    for _ in range(BLOCK.bit_length() - 2):
        power = mm(power, power)
        inverse = inverse + mm(inverse, power)
    inverse = inverse - mm(inverse, mm(across, inverse))
    growth = jnp.exp(c_col) * (label_col == label_first).astype(F32)
    both = mm(inverse, jnp.concatenate([weighted * growth, values * gate], axis=1))
    tail_keys = k_unit * (jnp.exp(c_last - c_col) * (label_col == label_last).astype(F32))
    ends = mm_tn(tail_keys, both)
    end_growth = jnp.exp(c_last) * (label_last == label_first).astype(F32)
    scores = mm_nt(q_unit, k_unit) * reach
    outs = mm(scores, both)
    width = q_unit.shape[-1]
    q_grown = q_unit * growth - outs[:, :width]
    own_mixed = outs[:, width:]
    state_map = (jnp.where(eye, end_growth, 0.0) - ends[:, :width]).astype(BF16)
    shift = ends[:, width:]
    marks_at = width + 16
    pay[0:width, :] = shift.astype(BF16)
    pay[width : width + 8, :] = jnp.broadcast_to(label_first, (8, width)).astype(BF16)
    pay[width + 8 : marks_at, :] = jnp.broadcast_to(label_last, (8, width)).astype(BF16)
    pay[marks_at:, :] = state_map
    pl.semaphore_wait(barrier, n_sp + n_tp - 2)
    tops = [pay.shape[0]] * (REACH - 1) + [marks_at]
    first = [
        remote(
            pay.at[0:top], pieces.at[k, 0:top], pa_s.at[k], pa_r.at[k],
            at_sp(lax.rem(s + k + 1, n_sp)),
        )
        for k, top in enumerate(tops)
    ]
    for k in reversed(range(REACH)):
        first[k].start()

    for name in names:
        if name not in early:
            loads[name].wait()
    pick0, pick1 = vm["picks"][0:1, :], vm["picks"][1:2, :]
    share = vm["share"][...].astype(F32)
    expert_i = iota((experts, rows), 0)
    to0, to1 = (expert_i == pick0).astype(F32), (expert_i == pick1).astype(F32)
    chosen = to0 + to1
    rank = mm(chosen, (row_i < col_i).astype(F32))
    coded = jnp.where(chosen > 0.0, rank + 1.0, 0.0)
    shares = to0 * share[0:1, :] + to1 * share[1:2, :]
    slot_i = iota((padded, experts), 0)
    from_e = iota((padded, experts), 1) * stride
    spread = ((slot_i >= from_e) & (slot_i < from_e + stride)).astype(F32)
    place = iota((n_sp, stride, rows), 1).reshape(padded, rows)
    wide = mm(spread, jnp.concatenate([coded, shares, to0], axis=1))
    hot = wide[:, :rows] == (place + 1).astype(F32)
    dispatch = hot.astype(BF16)
    slot_share = jnp.sum(jnp.where(hot, wide[:, rows : 2 * rows], 0.0), axis=1, keepdims=True)
    slot_first = jnp.sum(jnp.where(hot, wide[:, 2 * rows :], 0.0), axis=1, keepdims=True)
    here = (iota((padded, rows), 1) == place).astype(F32)

    def per_slot(column):
        return jnp.sum((here * column).reshape(n_sp, stride, rows), axis=1, keepdims=True)

    told[...] = jnp.zeros_like(told)
    told[:, 0:1, :] = per_slot(slot_share).astype(BF16)
    told[:, 1:2, :] = per_slot(slot_first).astype(BF16)
    compact_i = iota((slots, padded), 0).astype(F32)
    source = jnp.floor((compact_i + 0.5) * (1.0 / cap))
    within = compact_i - source * cap
    column = iota((slots, padded), 1).astype(F32)
    compact = (column == source * stride + within).astype(BF16)
    slot_lane = iota((slots, rows), 1).astype(F32) == within[:, :rows]
    valve = silu(vm["exit"][...].astype(F32))

    for k in range(REACH):
        first[k].wait_recv()

    def piece(k):
        label = pieces[k, width:marks_at, :].astype(F32)
        return pieces[k, 0:width, :], label[0:1, :], label[8:9, :]

    shift1, first1, last1 = piece(0)
    shift2, first2, last2 = piece(1)
    shift3, _, last3 = piece(2)
    map1 = pieces[0, marks_at:, :] * (first1 == last2).astype(BF16)
    map2 = pieces[1, marks_at:, :] * (first2 == last3).astype(BF16)
    joined = (label_first == last1).astype(F32)
    shift12 = shift1.astype(F32) + mm(map1, shift2)
    map12 = mm(map1, map2).astype(BF16)
    entering = (shift12 + mm(map12, shift3)) * joined
    carry_out[...] = (shift + mm(state_map, entering)).astype(BF16)
    second = remote(
        carry_out, carry_in, pb_s.at[0], pb_s.at[1], at_sp(lax.rem(s + REACH, n_sp))
    )
    second.start()
    second.wait_recv()
    incoming = (shift12 + mm(map12, carry_in[...])) * joined
    mixed = own_mixed + mm(q_grown, incoming)
    scaled = mixed * lax.rsqrt(jnp.mean(mixed * mixed, -1, keepdims=True) + 1e-06)
    heads_out = (scaled * valve).astype(BF16)

    far_first = sorted(range(1, ny), key=lambda k: -min(k, ny - k))

    def scattered_sum(part, pair, send, recv, d_r, y_r):
        near = {}
        for k in far_first + [0]:
            chip = lax.rem(y + k, ny)
            near[k] = remote(
                part.at[chip, other], pair.at[chip], d_r.at[ny], d_r.at[k], at_tp(2 * y + other)
            )
            near[k].start()
        for k in far_first:
            chip = lax.rem(y + k, ny)
            near[k].wait_recv()
            send[chip] = (part[chip, c].astype(F32) + pair[chip].astype(F32)).astype(BF16)
            remote(send.at[chip], recv.at[k], y_r.at[1], y_r.at[0], at_tp(2 * chip + c)).start()
        near[0].wait_recv()
        total = part[y, c].astype(F32) + pair[y].astype(F32)
        if far_first:
            there = recv.at[1:ny]
            remote(there, there, y_r.at[1], y_r.at[0], at_tp(t)).wait_recv()
            for k in far_first:
                total = total + recv[k].astype(F32)
        return total

    def sums_left(part, recv, d_r, y_r):
        remote(part.at[:, 0], part.at[:, 0], d_r.at[ny], d_r.at[ny], at_tp(t)).wait_send()
        if far_first:
            there = recv.at[1:ny]
            remote(there, there, y_r.at[1], y_r.at[0], at_tp(t)).wait_send()

    def tell(stat, sems, line):
        stat[t] = line
        for k in range(1, n_tp):
            to = lax.rem(t + k, n_tp)
            remote(stat.at[t], stat.at[t], sems.at[0], sems.at[1], at_tp(to)).start()

    def heard_all(stat, sems):
        there = stat.at[1:n_tp]
        remote(there, there, sems.at[0], sems.at[1], at_tp(t)).wait()
        return jnp.sum(stat[...], axis=0)

    scaled_in = ALPHA * vm["incoming"][...].astype(F32)
    row_sum = jnp.sum(scaled_in, -1, keepdims=True)
    for chip in range(ny):
        product = mm(heads_out, vm["final"][:, chip * 2 * width : (chip + 1) * 2 * width])
        part1[chip, 0] = product[:, :width].astype(BF16)
        part1[chip, 1] = product[:, width:].astype(BF16)
        row_sum = row_sum + jnp.sum(product, -1, keepdims=True)
    tell(stat0, mean_s, to_row(row_sum))
    projected = scattered_sum(part1, pair1, send1, recv1, d1_r, y1_r)
    features = width * n_tp
    mean = to_col(heard_all(stat0, mean_s) / features)
    centred = scaled_in + projected - mean

    nx = 4
    nz = n_sp // nx
    hops = sorted(
        ((dz, dx) for dz in range(nz) for dx in range(nx) if dz or dx),
        key=lambda d: -min(d[0], nz - d[0]) - min(d[1], nx - d[1]),
    )

    def scatter(src, dst, sems):
        z, x = s // nx, lax.rem(s, nx)
        for dz, dx in hops:
            to = lax.rem(z + dz, nz) * nx + lax.rem(x + dx, nx)
            remote(src.at[to], dst.at[s], sems.at[0], sems.at[1], at_sp(to)).start()
        dst[s] = src[s]

    def collected(dst, sems):
        there = dst.at[1:n_sp]
        remote(there, there, sems.at[0], sems.at[1], at_sp(s)).wait()
        return dst[...].reshape(dst.shape[0] * dst.shape[1], dst.shape[2])

    gained = (centred * vm["gain1"][...]).astype(BF16)
    payload = jnp.dot(dispatch, gained, preferred_element_type=F32)
    sent[...] = payload.astype(BF16).reshape(n_sp, stride, rows)
    scatter(sent, arrived, dis_s)
    tell(stat1, sq1_s, to_row(jnp.sum(centred * centred, -1, keepdims=True)))
    row_scale = lax.rsqrt(heard_all(stat1, sq1_s) / features + 1e-05)
    slot_scale = jnp.sum(jnp.where(hot, row_scale, 0.0), axis=1, keepdims=True)
    scales = per_slot(slot_scale)
    coarse = scales.astype(BF16)
    told[:, 2:3, :] = coarse
    told[:, 3:4, :] = (scales - coarse.astype(F32)).astype(BF16)
    scatter(told, heard, note_s)
    middle = (centred * to_col(row_scale) * vm["gain1"][...]).astype(BF16)
    came = collected(arrived, dis_s)
    own_rows = jnp.dot(compact, came, preferred_element_type=F32).astype(BF16)

    lanes = pl.ds(pl.multiple_of(c * width, width), width)
    ahead = lax.rem(y + 1 - 2 * c + ny, ny)
    behind = lax.rem(y - 1 + 2 * c + ny, ny)
    most, least = ny // 2, (ny - 1) // 2

    def origin(k):
        return lax.rem(y - k * (1 - 2 * c) + 2 * ny, ny)

    gathered[y, :, lanes] = own_rows

    def block(chip):
        return gathered.at[chip, :, lanes]

    def hand(k, chip):
        return remote(block(chip), block(chip), gone_s.at[0], own_r.at[k], at_tp(2 * y + other))

    def big(k):
        chip = origin(k)
        return remote(block(chip), block(chip), gone_s.at[1], big_r.at[k], at_tp(2 * ahead + c))

    def small(k):
        chip = origin(-k)
        return remote(
            block(chip), block(chip), gone_s.at[1], small_r.at[k], at_tp(2 * behind + c)
        )

    def big_wait(k):
        chip = origin(k + 1)
        remote(
            block(chip), block(chip), gone_s.at[1], big_r.at[k], at_tp(2 * ahead + c)
        ).wait_recv()

    def small_wait(k):
        chip = origin(-k - 1)
        remote(
            block(chip), block(chip), gone_s.at[1], small_r.at[k], at_tp(2 * behind + c)
        ).wait_recv()

    def hand_wait(k, chip):
        other_lanes = pl.ds(pl.multiple_of(other * width, width), width)
        there = gathered.at[chip, :, other_lanes]
        remote(there, there, gone_s.at[0], own_r.at[k], at_tp(2 * y + other)).wait_recv()

    def absorb(chip, fresh):
        block_in = gathered[chip]
        at = pl.ds(pl.multiple_of(chip * 2 * width, 2 * width), 2 * width)
        gates = jnp.dot(block_in, vm["valve"][at, :], preferred_element_type=F32)
        ups = jnp.dot(block_in, vm["raise"][at, :], preferred_element_type=F32)
        common = lax.dot_general(
            block_in, vm["common"][:, at], (((1,), (1,)), ((), ())), preferred_element_type=F32
        )
        if fresh:
            acc_g[0], acc_g[1], acc_s[...] = gates, ups, common
        else:
            acc_g[0] += gates
            acc_g[1] += ups
            acc_s[...] += common

    big(0).start()
    if least:
        small(0).start()
    hand(0, y).start()
    hand_wait(0, y)
    absorb(y, True)
    for k in range(1, most + 1):
        big_wait(k - 1)
        if k < most:
            big(k).start()
        hand(2 * k - 1, origin(k)).start()
        if k <= least:
            small_wait(k - 1)
            if k < least:
                small(k).start()
            hand(2 * k, origin(-k)).start()
        hand_wait(2 * k - 1, origin(-k))
        absorb(origin(-k), False)
        if k <= least:
            hand_wait(2 * k, origin(k))
            absorb(origin(k), False)

    notes = collected(heard, note_s)

    note_column = iota((slots, notes.shape[0]), 1).astype(F32)
    note_source = source[:, :1] * told.shape[1]

    def noted(j):
        line = (note_column == note_source + j).astype(BF16)
        found = jnp.dot(line, notes, preferred_element_type=F32)
        return jnp.sum(jnp.where(slot_lane, found, 0.0), axis=1, keepdims=True)

    weight, flag, scale = noted(0), noted(1), noted(2) + noted(3)
    hidden = (silu(acc_g[0] * scale) * acc_g[1] * (scale * weight)).astype(BF16)
    common = acc_s[...] * scale
    shared = (silu(common[:, :sf]) * common[:, sf:] * flag).astype(BF16)
    for chip in range(ny):
        at = slice(chip * 2 * width, (chip + 1) * 2 * width)
        product = jnp.dot(hidden, vm["lower"][:, at], preferred_element_type=F32) + jnp.dot(
            shared, vm["common_low"][:, at], preferred_element_type=F32
        )
        part2[chip, 0] = product[:, :width].astype(BF16)
        part2[chip, 1] = product[:, width:].astype(BF16)
    summed = scattered_sum(part2, pair2, send2, recv2, d2_r, y2_r)

    rsend[...] = mm_tn(compact, summed).astype(BF16).reshape(n_sp, stride, rows)
    scatter(rsend, returned, ret_s)
    back = collected(returned, ret_s)
    mixture = mm_tn(dispatch, back)
    second_sum = ALPHA * middle.astype(F32) + mixture
    sums = [jnp.sum(v, -1, keepdims=True) for v in (second_sum, second_sum * second_sum)]
    tell(stat2, sq2_s, jnp.concatenate([to_row(v) for v in sums], axis=0))
    totals = heard_all(stat2, sq2_s) / features
    mean2, square2 = totals[0:1, :], totals[1:2, :]
    scale2 = lax.rsqrt(square2 - mean2 * mean2 + 1e-05)
    out_vm[...] = (
        (second_sum - to_col(mean2)) * to_col(scale2) * vm["gain2"][...]
    ).astype(BF16)
    out_copy = pltpu.make_async_copy(out_vm, out_hbm, out_sem)
    out_copy.start()

    for copy in first:
        copy.wait_send()
    second.wait_send()
    remote(send2, send2, gone_s.at[0], gone_s.at[0], at_tp(t)).wait_send()
    if far_first:
        there = send2.at[1:ny]
        remote(there, there, gone_s.at[1], gone_s.at[1], at_tp(t)).wait_send()
    sums_left(part1, recv1, d1_r, y1_r)
    sums_left(part2, recv2, d2_r, y2_r)
    out_copy.wait()


def dims_names():
    return (
        "probe", "address", "content", "storage", "fade", "extra", "label",
        "picks", "share", "exit", "incoming", "gain1", "gain2", "final",
        "valve", "raise", "lower", "common", "common_raise", "common_low", "channel",
    )


def shards(
    probe, address, content, storage, fade, channel, extra, label, exit_valve, final,
    incoming, gain1, picks, share, valve, raising, lowering, common_valve, common_raising,
    common_lowering, gain2,
):
    n_sp, n_tp = lax.axis_size("sp"), lax.axis_size("tp")
    ny = n_tp // 2
    rows, width = probe.shape
    experts = n_sp * valve.shape[0]
    cap = max(2, 9 * rows * picks.shape[1] // (8 * experts))
    stride = -(-(cap + 2) // 16) * 16
    slots = n_sp * cap
    ff, features = valve.shape[2], valve.shape[1]
    sf = common_valve.shape[1]
    dims = (n_sp, n_tp, rows, experts, cap, stride)
    args = {
        "probe": probe, "address": address, "content": content, "storage": storage,
        "fade": fade, "extra": extra, "label": label[None, :], "picks": picks.T,
        "share": share.T, "exit": exit_valve, "incoming": incoming, "gain1": gain1[None, :],
        "gain2": gain2[None, :], "final": final, "valve": valve[0], "raise": raising[0],
        "lower": lowering[0],
        "common": common_valve.T, "common_raise": common_raising.T,
        "common_low": common_lowering, "channel": channel[None, :],
    }
    names = dims_names()
    operands = [args[n] for n in names]
    dma = pltpu.SemaphoreType.DMA
    shapes = {n: a.shape for n, a in args.items()}
    shapes["common"] = (2 * sf, features)
    shapes["common_raise"] = (8, 128)
    own = [pltpu.VMEM(shapes[n], args[n].dtype) for n in names]

    def vmem(*shape, kind=BF16):
        return pltpu.VMEM(shape, kind)

    return pl.pallas_call(
        functools.partial(kernel, dims),
        out_shape=jax.ShapeDtypeStruct((rows, width), BF16),
        in_specs=[pl.BlockSpec(memory_space=pl.ANY)] * len(operands),
        out_specs=pl.BlockSpec(memory_space=pl.ANY),
        scratch_shapes=own
        + [
            vmem(2 * width + 16, width), vmem(REACH, 2 * width + 16, width),
            vmem(width, width), vmem(width, width),
            vmem(ny, 2, rows, width), vmem(ny, rows, width), vmem(ny, rows, width),
            vmem(ny, rows, width),
            vmem(n_tp, 1, rows, kind=F32), vmem(n_tp, 1, rows, kind=F32),
            vmem(n_tp, 2, rows, kind=F32),
            vmem(n_sp, stride, width), vmem(n_sp, stride, width),
            vmem(n_sp, 16, width), vmem(n_sp, 16, width),
            vmem(ny, slots, 2 * width), vmem(2, slots, ff, kind=F32), vmem(slots, 2 * sf, kind=F32),
            vmem(ny, 2, slots, width), vmem(ny, slots, width), vmem(ny, slots, width),
            vmem(ny, slots, width),
            vmem(n_sp, stride, width), vmem(n_sp, stride, width), vmem(rows, width),
            dma((len(operands),)), dma, dma((REACH,)), dma((REACH,)), dma((2,)),
            dma((ny + 1,)), dma((2,)), dma((2,)), dma((2,)), dma((2,)),
            dma((2,)), dma((2,)), dma((2,)), dma((ny,)), dma((ny,)), dma((ny,)), dma((2,)),
            dma((ny + 1,)), dma((2,)),
        ],
        compiler_params=pltpu.CompilerParams(
            collective_id=0, has_side_effects=True, vmem_limit_bytes=60 * 1024 * 1024
        ),
        name="layer",
    )(*operands)


def solution(mesh):
    return jax.shard_map(
        shards,
        mesh=mesh,
        in_specs=(
            P("sp", "tp"), P("sp", "tp"), P("sp", "tp"), P("tp", "sp"), P("tp", "sp"), P("tp"),
            P("tp", "sp"), P("sp"), P("sp", "tp"), P("tp", None), P("sp", "tp"), P("tp"),
            P("sp", None), P("sp", None), P("sp", None, "tp"), P("sp", None, "tp"),
            P("sp", "tp", None), P(None, "tp"), P(None, "tp"), P("tp", None), P("tp"),
        ),
        out_specs=P("sp", "tp"),
        check_vma=False,
    )
```

```python
import functools

import jax
import jax.numpy as jnp
from jax import lax
from jax.experimental import pallas as pl
from jax.experimental.pallas import tpu as pltpu
from jax.sharding import PartitionSpec as P

BLOCK = 64
ALPHA = 2.0**0.25
F32 = jnp.float32
BF16 = jnp.bfloat16
MESH = pl.DeviceIdType.MESH
REACH = 3
CHUNKS = 2


def iota(shape, dim):
    return lax.broadcasted_iota(jnp.int32, shape, dim)


def mm(a, b):
    return jnp.dot(a.astype(BF16), b.astype(BF16), preferred_element_type=F32)


def mm_nt(a, b):
    return lax.dot_general(
        a.astype(BF16), b.astype(BF16), (((1,), (1,)), ((), ())), preferred_element_type=F32
    )


def mm_tn(a, b):
    return lax.dot_general(
        a.astype(BF16), b.astype(BF16), (((0,), (0,)), ((), ())), preferred_element_type=F32
    )


def silu(v):
    return v / (1.0 + jnp.exp(-v))


def kernel(dims, *refs):
    n_sp, n_tp, rows, experts, cap, stride = dims
    ny = n_tp // 2
    slots = n_sp * cap
    padded = n_sp * stride
    names = dims_names()
    hbm = dict(zip(names, refs[: len(names)]))
    out_hbm = refs[len(names)]
    scratch = refs[len(names) + 1 :]
    vm = dict(zip(names, scratch[: len(names)]))
    (
        pay, pieces, carry_out, carry_in,
        part1, pair1, send1, recv1,
        stat0, stat1, stat2,
        sent, arrived, told, heard, gathered, acc_g, acc_s,
        part2, pair2, send2, recv2, send3, recv3,
        rsend, returned, out_vm,
        load_sem, out_sem, pa_s, pa_r, pb_s,
        d1_r, y1_r, mean_s, sq1_s, sq2_s,
        dis_s, note_s, ret_s, big_r, small_r, own_r, gone_s,
        near_r, far_r, back_r,
    ) = scratch[len(names) :]

    s = lax.axis_index("sp")
    t = lax.axis_index("tp")
    y = t // 2
    c = lax.rem(t, 2)
    other = 1 - c

    def at_sp(k):
        return {"sp": k, "tp": t}

    def at_tp(k):
        return {"sp": s, "tp": k}

    def remote(src, dst, send_sem, recv_sem, device):
        return pltpu.make_async_remote_copy(
            src_ref=src, dst_ref=dst, send_sem=send_sem, recv_sem=recv_sem,
            device_id=device, device_id_type=MESH,
        )

    barrier = pltpu.get_barrier_semaphore()

    def greet_sp(k, carry):
        pl.semaphore_signal(
            barrier, inc=1, device_id=at_sp(lax.rem(s + k, n_sp)), device_id_type=MESH
        )
        return carry

    def greet_tp(k, carry):
        pl.semaphore_signal(
            barrier, inc=1, device_id=at_tp(lax.rem(t + k, n_tp)), device_id_type=MESH
        )
        return carry

    lax.fori_loop(1, n_sp, greet_sp, 0)
    lax.fori_loop(1, n_tp, greet_tp, 0)
    sf = vm["common"].shape[0] // 2
    loads = {}
    for k, name in enumerate(names):
        into = vm[name]
        if name == "common":
            into = vm["common"].at[0:sf]
        if name == "common_raise":
            into = vm["common"].at[sf:]
        loads[name] = pltpu.make_async_copy(hbm[name], into, load_sem.at[k])
    early = ("probe", "address", "content", "storage", "fade", "extra", "channel", "label")
    for name in early:
        loads[name].start()
    for name in names:
        if name not in early:
            loads[name].start()
    for name in early:
        loads[name].wait()

    row_i, col_i = iota((rows, rows), 0), iota((rows, rows), 1)
    eye = row_i == col_i
    lower, strict = row_i >= col_i, row_i > col_i
    same_block = (row_i < BLOCK) == (col_i < BLOCK)

    def to_col(row):
        return jnp.sum(jnp.where(eye, row, 0.0), axis=1, keepdims=True)

    def to_row(col):
        return jnp.sum(jnp.where(eye, col, 0.0), axis=0, keepdims=True)

    queries = vm["probe"][...].astype(F32)
    keys = vm["address"][...].astype(F32)
    values = vm["content"][...].astype(F32)
    q_unit = queries * lax.rsqrt(
        jnp.sum(queries * queries, -1, keepdims=True) + 1e-06
    ) * queries.shape[-1] ** (-0.5)
    k_unit = keys * lax.rsqrt(jnp.sum(keys * keys, -1, keepdims=True) + 1e-06)
    gate = to_col(1.0 / (1.0 + jnp.exp(-vm["storage"][...])))
    fade = vm["fade"][...]
    softplus = jnp.maximum(fade, 0.0) + jnp.log(1.0 + jnp.exp(-jnp.abs(fade)))
    rate = jnp.exp(vm["channel"][...])
    decay = vm["extra"][...] - rate * softplus
    c_col = jnp.sum(jnp.where(lower, decay, 0.0), axis=1, keepdims=True)
    c_row = to_row(c_col)
    label_row = vm["label"][...].astype(F32)
    label_col = to_col(label_row)
    label_first, label_last = label_row[:, :1], label_row[:, rows - 1 :]
    c_last = c_row[:, rows - 1 :]
    reach = jnp.where(
        lower & (label_col == label_row), jnp.exp(jnp.where(lower, c_col - c_row, 0.0)), 0.0
    )
    weighted = k_unit * gate
    coupling = jnp.where(strict, mm_nt(weighted, k_unit) * reach, 0.0)
    power = jnp.where(same_block, coupling, 0.0)
    across = jnp.where(same_block, 0.0, coupling)
    inverse = jnp.where(eye, 1.0, 0.0) - power
    for _ in range(BLOCK.bit_length() - 2):
        power = mm(power, power)
        inverse = inverse + mm(inverse, power)
    inverse = inverse - mm(inverse, mm(across, inverse))
    growth = jnp.exp(c_col) * (label_col == label_first).astype(F32)
    both = mm(inverse, jnp.concatenate([weighted * growth, values * gate], axis=1))
    tail_keys = k_unit * (jnp.exp(c_last - c_col) * (label_col == label_last).astype(F32))
    ends = mm_tn(tail_keys, both)
    end_growth = jnp.exp(c_last) * (label_last == label_first).astype(F32)
    scores = mm_nt(q_unit, k_unit) * reach
    outs = mm(scores, both)
    width = q_unit.shape[-1]
    q_grown = q_unit * growth - outs[:, :width]
    own_mixed = outs[:, width:]
    state_map = (jnp.where(eye, end_growth, 0.0) - ends[:, :width]).astype(BF16)
    shift = ends[:, width:]
    marks_at = width + 16
    pay[0:width, :] = shift.astype(BF16)
    pay[width : width + 8, :] = jnp.broadcast_to(label_first, (8, width)).astype(BF16)
    pay[width + 8 : marks_at, :] = jnp.broadcast_to(label_last, (8, width)).astype(BF16)
    pay[marks_at:, :] = state_map
    pl.semaphore_wait(barrier, n_sp + n_tp - 2)
    tops = [pay.shape[0]] * (REACH - 1) + [marks_at]
    first = [
        remote(
            pay.at[0:top], pieces.at[k, 0:top], pa_s.at[k], pa_r.at[k],
            at_sp(lax.rem(s + k + 1, n_sp)),
        )
        for k, top in enumerate(tops)
    ]
    for k in reversed(range(REACH)):
        first[k].start()

    for name in names:
        if name not in early:
            loads[name].wait()
    pick0, pick1 = vm["picks"][0:1, :], vm["picks"][1:2, :]
    share = vm["share"][...].astype(F32)
    expert_i = iota((experts, rows), 0)
    to0, to1 = (expert_i == pick0).astype(F32), (expert_i == pick1).astype(F32)
    chosen = to0 + to1
    rank = mm(chosen, (row_i < col_i).astype(F32))
    coded = jnp.where(chosen > 0.0, rank + 1.0, 0.0)
    shares = to0 * share[0:1, :] + to1 * share[1:2, :]
    slot_i = iota((padded, experts), 0)
    from_e = iota((padded, experts), 1) * stride
    spread = ((slot_i >= from_e) & (slot_i < from_e + stride)).astype(F32)
    place = iota((n_sp, stride, rows), 1).reshape(padded, rows)
    wide = mm(spread, jnp.concatenate([coded, shares, to0], axis=1))
    hot = wide[:, :rows] == (place + 1).astype(F32)
    dispatch = hot.astype(BF16)
    slot_share = jnp.sum(jnp.where(hot, wide[:, rows : 2 * rows], 0.0), axis=1, keepdims=True)
    slot_first = jnp.sum(jnp.where(hot, wide[:, 2 * rows :], 0.0), axis=1, keepdims=True)
    here = (iota((padded, rows), 1) == place).astype(F32)

    def per_slot(column):
        return jnp.sum((here * column).reshape(n_sp, stride, rows), axis=1, keepdims=True)

    told[...] = jnp.zeros_like(told)
    told[:, 0:1, :] = per_slot(slot_share).astype(BF16)
    told[:, 1:2, :] = per_slot(slot_first).astype(BF16)
    compact_i = iota((slots, padded), 0).astype(F32)
    source = jnp.floor((compact_i + 0.5) * (1.0 / cap))
    within = compact_i - source * cap
    column = iota((slots, padded), 1).astype(F32)
    compact = (column == source * stride + within).astype(BF16)
    slot_lane = iota((slots, rows), 1).astype(F32) == within[:, :rows]
    valve = silu(vm["exit"][...].astype(F32))

    for k in range(REACH):
        first[k].wait_recv()

    def piece(k):
        label = pieces[k, width:marks_at, :].astype(F32)
        return pieces[k, 0:width, :], label[0:1, :], label[8:9, :]

    shift1, first1, last1 = piece(0)
    shift2, first2, last2 = piece(1)
    shift3, _, last3 = piece(2)
    map1 = pieces[0, marks_at:, :] * (first1 == last2).astype(BF16)
    map2 = pieces[1, marks_at:, :] * (first2 == last3).astype(BF16)
    joined = (label_first == last1).astype(F32)
    shift12 = shift1.astype(F32) + mm(map1, shift2)
    map12 = mm(map1, map2).astype(BF16)
    entering = (shift12 + mm(map12, shift3)) * joined
    carry_out[...] = (shift + mm(state_map, entering)).astype(BF16)
    second = remote(
        carry_out, carry_in, pb_s.at[0], pb_s.at[1], at_sp(lax.rem(s + REACH, n_sp))
    )
    second.start()
    second.wait_recv()
    incoming = (shift12 + mm(map12, carry_in[...])) * joined
    mixed = own_mixed + mm(q_grown, incoming)
    scaled = mixed * lax.rsqrt(jnp.mean(mixed * mixed, -1, keepdims=True) + 1e-06)
    heads_out = (scaled * valve).astype(BF16)

    far_first = sorted(range(1, ny), key=lambda k: -min(k, ny - k))

    def scattered_sum(part, pair, send, recv, d_r, y_r):
        near = {}
        for k in far_first + [0]:
            chip = lax.rem(y + k, ny)
            near[k] = remote(
                part.at[chip, other], pair.at[chip], d_r.at[ny], d_r.at[k], at_tp(2 * y + other)
            )
            near[k].start()
        for k in far_first:
            chip = lax.rem(y + k, ny)
            near[k].wait_recv()
            send[chip] = (part[chip, c].astype(F32) + pair[chip].astype(F32)).astype(BF16)
            remote(send.at[chip], recv.at[k], y_r.at[1], y_r.at[0], at_tp(2 * chip + c)).start()
        near[0].wait_recv()
        total = part[y, c].astype(F32) + pair[y].astype(F32)
        if far_first:
            there = recv.at[1:ny]
            remote(there, there, y_r.at[1], y_r.at[0], at_tp(t)).wait_recv()
            for k in far_first:
                total = total + recv[k].astype(F32)
        return total

    def sums_left(part, recv, d_r, y_r):
        remote(part.at[:, 0], part.at[:, 0], d_r.at[ny], d_r.at[ny], at_tp(t)).wait_send()
        if far_first:
            there = recv.at[1:ny]
            remote(there, there, y_r.at[1], y_r.at[0], at_tp(t)).wait_send()

    def tell(stat, sems, line):
        stat[t] = line
        for k in range(1, n_tp):
            to = lax.rem(t + k, n_tp)
            remote(stat.at[t], stat.at[t], sems.at[0], sems.at[1], at_tp(to)).start()

    def heard_all(stat, sems):
        there = stat.at[1:n_tp]
        remote(there, there, sems.at[0], sems.at[1], at_tp(t)).wait()
        return jnp.sum(stat[...], axis=0)

    scaled_in = ALPHA * vm["incoming"][...].astype(F32)
    row_sum = jnp.sum(scaled_in, -1, keepdims=True)
    for k in far_first + [0]:
        chip = lax.rem(y + k, ny)
        at = pl.ds(pl.multiple_of(chip * 2 * width, 2 * width), 2 * width)
        product = mm(heads_out, vm["final"][:, at])
        part1[chip, 0] = product[:, :width].astype(BF16)
        part1[chip, 1] = product[:, width:].astype(BF16)
        row_sum = row_sum + jnp.sum(product, -1, keepdims=True)
    tell(stat0, mean_s, to_row(row_sum))
    projected = scattered_sum(part1, pair1, send1, recv1, d1_r, y1_r)
    features = width * n_tp
    mean = to_col(heard_all(stat0, mean_s) / features)
    centred = scaled_in + projected - mean

    nx = 4
    nz = n_sp // nx
    hops = sorted(
        ((dz, dx) for dz in range(nz) for dx in range(nx) if dz or dx),
        key=lambda d: -min(d[0], nz - d[0]) - min(d[1], nx - d[1]),
    )

    def scatter(src, dst, sems):
        z, x = s // nx, lax.rem(s, nx)
        for dz, dx in hops:
            to = lax.rem(z + dz, nz) * nx + lax.rem(x + dx, nx)
            remote(src.at[to], dst.at[s], sems.at[0], sems.at[1], at_sp(to)).start()
        dst[s] = src[s]

    def collected(dst, sems):
        there = dst.at[1:n_sp]
        remote(there, there, sems.at[0], sems.at[1], at_sp(s)).wait()
        return dst[...].reshape(dst.shape[0] * dst.shape[1], dst.shape[2])

    gained = (centred * vm["gain1"][...]).astype(BF16)
    payload = jnp.dot(dispatch, gained, preferred_element_type=F32)
    sent[...] = payload.astype(BF16).reshape(n_sp, stride, rows)
    scatter(sent, arrived, dis_s)
    tell(stat1, sq1_s, to_row(jnp.sum(centred * centred, -1, keepdims=True)))
    came = collected(arrived, dis_s)
    own_rows = jnp.dot(compact, came, preferred_element_type=F32).astype(BF16)

    lanes = pl.ds(pl.multiple_of(c * width, width), width)
    turn = 1 - 2 * c
    ahead = lax.rem(y + turn + ny, ny)
    behind = lax.rem(y - turn + ny, ny)
    most, least = ny // 2, (ny - 1) // 2
    piece_rows = slots // CHUNKS

    def rows_of(q):
        return slice(q * piece_rows, (q + 1) * piece_rows)

    def along(d):
        return lax.rem(y + d * turn + 2 * ny, ny)

    gathered[y, :, lanes] = own_rows

    def block(chip, q):
        return gathered.at[chip, rows_of(q), lanes]

    def passed(chip, q, sem, to):
        there = block(chip, q)
        return remote(there, there, gone_s.at[1], sem, at_tp(2 * to + c))

    def big(k, q, origin):
        return passed(along(-origin), q, big_r.at[k * CHUNKS + q], ahead)

    def small(k, q, origin):
        return passed(along(origin), q, small_r.at[k * CHUNKS + q], behind)

    def chips_at(k):
        return [along(k)] if k == 0 or k > least else [along(-k), along(k)]

    def hand(k, q):
        for chip in reversed(chips_at(k)):
            there = block(chip, q)
            remote(
                there, there, gone_s.at[0], own_r.at[k * CHUNKS + q], at_tp(2 * y + other)
            ).start()

    def wait_bytes(count, sem):
        there = pair2.at[0:count, 0:piece_rows]
        remote(there, there, sem, sem, at_tp(t)).wait_recv()

    def absorb(k, q):
        chips, at_rows = chips_at(k), rows_of(q)
        wait_bytes(len(chips), own_r.at[k * CHUNKS + q])
        for chip in chips:
            block_in = gathered[chip, at_rows, :]
            at = pl.ds(pl.multiple_of(chip * 2 * width, 2 * width), 2 * width)
            gates = jnp.dot(block_in, vm["valve"][at, :], preferred_element_type=F32)
            ups = jnp.dot(block_in, vm["raise"][at, :], preferred_element_type=F32)
            common = lax.dot_general(
                block_in, vm["common"][:, at], (((1,), (1,)), ((), ())), preferred_element_type=F32
            )
            if k == 0:
                acc_g[0, at_rows], acc_g[1, at_rows], acc_s[at_rows] = gates, ups, common
            else:
                acc_g[0, at_rows] += gates
                acc_g[1, at_rows] += ups
                acc_s[at_rows] += common

    def all_noted():
        notes = collected(heard, note_s)
        note_column = iota((slots, notes.shape[0]), 1).astype(F32)
        note_source = source[:, :1] * told.shape[1]

        def noted(j):
            line = (note_column == note_source + j).astype(BF16)
            found = jnp.dot(line, notes, preferred_element_type=F32)
            return jnp.sum(jnp.where(slot_lane, found, 0.0), axis=1, keepdims=True)

        return noted(0), noted(1), noted(2) + noted(3)

    for q in range(CHUNKS):
        if most:
            big(0, q, 0).start()
        if least:
            small(0, q, 0).start()
    for q in range(CHUNKS):
        hand(0, q)
    row_scale = lax.rsqrt(heard_all(stat1, sq1_s) / features + 1e-05)
    slot_scale = jnp.sum(jnp.where(hot, row_scale, 0.0), axis=1, keepdims=True)
    scales = per_slot(slot_scale)
    coarse = scales.astype(BF16)
    told[:, 2:3, :] = coarse
    told[:, 3:4, :] = (scales - coarse.astype(F32)).astype(BF16)
    scatter(told, heard, note_s)
    middle = (centred * to_col(row_scale) * vm["gain1"][...]).astype(BF16)
    waiting = [(0, q) for q in range(CHUNKS)]
    slot_notes = None
    for k in range(1, most + 1):
        for q in range(CHUNKS):
            big(k - 1, q, k).wait_recv()
            if k < most:
                big(k, q, k).start()
            if k <= least:
                small(k - 1, q, k).wait_recv()
                if k < least:
                    small(k, q, k).start()
            hand(k, q)
            absorb(*waiting.pop(0))
            waiting.append((k, q))
        if k == most - 1:
            slot_notes = all_noted()
    if slot_notes is None:
        slot_notes = all_noted()

    def expert(q):
        at_rows = rows_of(q)
        weight, flag, scale = (v[at_rows] for v in slot_notes)
        hidden = (silu(acc_g[0, at_rows] * scale) * acc_g[1, at_rows] * (scale * weight)).astype(
            BF16
        )
        common = acc_s[at_rows] * scale
        shared = (silu(common[:, :sf]) * common[:, sf:] * flag).astype(BF16)
        for chip in range(ny):
            at = slice(chip * 2 * width, (chip + 1) * 2 * width)
            product = jnp.dot(hidden, vm["lower"][:, at], preferred_element_type=F32) + jnp.dot(
                shared, vm["common_low"][:, at], preferred_element_type=F32
            )
            part2[chip, 0, at_rows] = product[:, :width].astype(BF16)
            part2[chip, 1, at_rows] = product[:, width:].astype(BF16)
        for g, group in enumerate(groups):
            for d in group:
                chip = along(d)
                remote(
                    part2.at[chip, other, at_rows], pair2.at[chip, at_rows], gone_s.at[2],
                    near_r.at[2 * q + g], at_tp(2 * y + other),
                ).start()

    soon = sorted({most % ny, least % ny, -least % ny} - {0})
    groups = [soon, [d for d in range(ny) if d not in soon]]
    for q in range(CHUNKS):
        absorb(*waiting.pop(0))
        expert(q)

    def chip_sum(d, q):
        chip, at_rows = along(d), rows_of(q)
        return part2[chip, c, at_rows].astype(F32) + pair2[chip, at_rows].astype(F32)

    def ring_step(j, q, reach, sign, send, recv, sem, gone, to):
        at_rows = rows_of(q)
        value = chip_sum(sign * (reach - j), q)
        if j:
            came_in(j - 1, q, send, recv, sem, gone, to).wait_recv()
            value = value + recv[j - 1, at_rows].astype(F32)
        send[j, at_rows] = value.astype(BF16)
        came_in(j, q, send, recv, sem, gone, to).start()

    def came_in(j, q, send, recv, sem, gone, to):
        at_rows = rows_of(q)
        return remote(
            send.at[j, at_rows], recv.at[j, at_rows], gone, sem.at[j * CHUNKS + q],
            at_tp(2 * to + c),
        )

    large = (send2, recv2, far_r, gone_s.at[3], ahead)
    little = (send3, recv3, back_r, gone_s.at[4], behind)
    for j in range(most):
        for q in range(CHUNKS):
            if j < 2 and groups[j]:
                wait_bytes(len(groups[j]), near_r.at[2 * q + j])
            ring_step(j, q, most, 1, *large)
            if j < least:
                ring_step(j, q, least, -1, *little)
    for q in range(CHUNKS):
        if most < 2:
            wait_bytes(len(groups[1]), near_r.at[2 * q + 1])
        value = chip_sum(0, q)
        if most:
            came_in(most - 1, q, *large).wait_recv()
            value = value + recv2[most - 1, rows_of(q)].astype(F32)
        if least:
            came_in(least - 1, q, *little).wait_recv()
            value = value + recv3[least - 1, rows_of(q)].astype(F32)
        share_sp = n_sp // CHUNKS
        owners = slice(q * share_sp, (q + 1) * share_sp)
        spots = slice(q * share_sp * stride, (q + 1) * share_sp * stride)
        rsend[owners] = (
            mm_tn(compact[rows_of(q), spots], value)
            .astype(BF16)
            .reshape(share_sp, stride, rows)
        )
        for k in range(share_sp):
            to = q * share_sp + lax.rem(s + k, share_sp)

            @pl.when(to != s)
            def _(to=to):
                remote(
                    rsend.at[to], returned.at[s], ret_s.at[0], ret_s.at[1], at_sp(to)
                ).start()

    returned[s] = rsend[s]
    back = collected(returned, ret_s)
    mixture = mm_tn(dispatch, back)
    second_sum = ALPHA * middle.astype(F32) + mixture
    sums = [jnp.sum(v, -1, keepdims=True) for v in (second_sum, second_sum * second_sum)]
    tell(stat2, sq2_s, jnp.concatenate([to_row(v) for v in sums], axis=0))
    totals = heard_all(stat2, sq2_s) / features
    mean2, square2 = totals[0:1, :], totals[1:2, :]
    scale2 = lax.rsqrt(square2 - mean2 * mean2 + 1e-05)
    out_vm[...] = (
        (second_sum - to_col(mean2)) * to_col(scale2) * vm["gain2"][...]
    ).astype(BF16)
    out_copy = pltpu.make_async_copy(out_vm, out_hbm, out_sem)
    out_copy.start()

    for copy in first:
        copy.wait_send()
    second.wait_send()
    def all_gone(there, sem):
        remote(there, there, sem, sem, at_tp(t)).wait_send()

    all_gone(pair2, gone_s.at[0])
    all_gone(pair2, gone_s.at[2])
    if most:
        all_gone(pair2.at[1:ny], gone_s.at[1])
        all_gone(send2, gone_s.at[3])
    if least:
        all_gone(send3, gone_s.at[4])
    sums_left(part1, recv1, d1_r, y1_r)
    out_copy.wait()


def dims_names():
    return (
        "probe", "address", "content", "storage", "fade", "extra", "label",
        "picks", "share", "exit", "incoming", "gain1", "gain2", "final",
        "valve", "raise", "lower", "common", "common_raise", "common_low", "channel",
    )


def shards(
    probe, address, content, storage, fade, channel, extra, label, exit_valve, final,
    incoming, gain1, picks, share, valve, raising, lowering, common_valve, common_raising,
    common_lowering, gain2,
):
    n_sp, n_tp = lax.axis_size("sp"), lax.axis_size("tp")
    ny = n_tp // 2
    rows, width = probe.shape
    experts = n_sp * valve.shape[0]
    cap = max(2, 9 * rows * picks.shape[1] // (8 * experts))
    stride = -(-(cap + 2) // 16) * 16
    slots = n_sp * cap
    ff, features = valve.shape[2], valve.shape[1]
    sf = common_valve.shape[1]
    most, least = max(1, ny // 2), max(1, (ny - 1) // 2)
    dims = (n_sp, n_tp, rows, experts, cap, stride)
    args = {
        "probe": probe, "address": address, "content": content, "storage": storage,
        "fade": fade, "extra": extra, "label": label[None, :], "picks": picks.T,
        "share": share.T, "exit": exit_valve, "incoming": incoming, "gain1": gain1[None, :],
        "gain2": gain2[None, :], "final": final, "valve": valve[0], "raise": raising[0],
        "lower": lowering[0],
        "common": common_valve.T, "common_raise": common_raising.T,
        "common_low": common_lowering, "channel": channel[None, :],
    }
    names = dims_names()
    operands = [args[n] for n in names]
    dma = pltpu.SemaphoreType.DMA
    shapes = {n: a.shape for n, a in args.items()}
    shapes["common"] = (2 * sf, features)
    shapes["common_raise"] = (8, 128)
    own = [pltpu.VMEM(shapes[n], args[n].dtype) for n in names]

    def vmem(*shape, kind=BF16):
        return pltpu.VMEM(shape, kind)

    return pl.pallas_call(
        functools.partial(kernel, dims),
        out_shape=jax.ShapeDtypeStruct((rows, width), BF16),
        in_specs=[pl.BlockSpec(memory_space=pl.ANY)] * len(operands),
        out_specs=pl.BlockSpec(memory_space=pl.ANY),
        scratch_shapes=own
        + [
            vmem(2 * width + 16, width), vmem(REACH, 2 * width + 16, width),
            vmem(width, width), vmem(width, width),
            vmem(ny, 2, rows, width), vmem(ny, rows, width), vmem(ny, rows, width),
            vmem(ny, rows, width),
            vmem(n_tp, 1, rows, kind=F32), vmem(n_tp, 1, rows, kind=F32),
            vmem(n_tp, 2, rows, kind=F32),
            vmem(n_sp, stride, width), vmem(n_sp, stride, width),
            vmem(n_sp, 16, width), vmem(n_sp, 16, width),
            vmem(ny, slots, 2 * width), vmem(2, slots, ff, kind=F32), vmem(slots, 2 * sf, kind=F32),
            vmem(ny, 2, slots, width), vmem(ny, slots, width), vmem(most, slots, width),
            vmem(most, slots, width), vmem(least, slots, width), vmem(least, slots, width),
            vmem(n_sp, stride, width), vmem(n_sp, stride, width), vmem(rows, width),
            dma((len(operands),)), dma, dma((REACH,)), dma((REACH,)), dma((2,)),
            dma((ny + 1,)), dma((2,)), dma((2,)), dma((2,)), dma((2,)),
            dma((2,)), dma((2,)), dma((2,)), dma((most * CHUNKS,)), dma((least * CHUNKS,)), dma(((most + 1) * CHUNKS,)), dma((5,)),
            dma((2 * CHUNKS,)), dma((most * CHUNKS,)), dma((least * CHUNKS,)),
        ],
        compiler_params=pltpu.CompilerParams(
            collective_id=0, has_side_effects=True, vmem_limit_bytes=60 * 1024 * 1024
        ),
        name="layer",
    )(*operands)


def solution(mesh):
    return jax.shard_map(
        shards,
        mesh=mesh,
        in_specs=(
            P("sp", "tp"), P("sp", "tp"), P("sp", "tp"), P("tp", "sp"), P("tp", "sp"), P("tp"),
            P("tp", "sp"), P("sp"), P("sp", "tp"), P("tp", None), P("sp", "tp"), P("tp"),
            P("sp", None), P("sp", None), P("sp", None, "tp"), P("sp", None, "tp"),
            P("sp", "tp", None), P(None, "tp"), P(None, "tp"), P("tp", None), P("tp"),
        ),
        out_specs=P("sp", "tp"),
        check_vma=False,
    )
```

```python
import functools

import jax
import jax.numpy as jnp
from jax import lax
from jax.experimental import pallas as pl
from jax.experimental.pallas import tpu as pltpu
from jax.sharding import PartitionSpec as P

BLOCK = 64
ALPHA = 2.0**0.25
F32 = jnp.float32
BF16 = jnp.bfloat16
MESH = pl.DeviceIdType.MESH
REACH = 3
CHUNKS = 2


def iota(shape, dim):
    return lax.broadcasted_iota(jnp.int32, shape, dim)


def mm(a, b):
    return jnp.dot(a.astype(BF16), b.astype(BF16), preferred_element_type=F32)


def mm_nt(a, b):
    return lax.dot_general(
        a.astype(BF16), b.astype(BF16), (((1,), (1,)), ((), ())), preferred_element_type=F32
    )


def mm_tn(a, b):
    return lax.dot_general(
        a.astype(BF16), b.astype(BF16), (((0,), (0,)), ((), ())), preferred_element_type=F32
    )


def silu(v):
    return v / (1.0 + jnp.exp(-v))


def kernel(dims, *refs):
    n_sp, n_tp, rows, experts, cap, stride = dims
    ny = n_tp // 2
    slots = n_sp * cap
    padded = n_sp * stride
    names = dims_names()
    hbm = dict(zip(names, refs[: len(names)]))
    out_ref = refs[len(names)]
    scratch = refs[len(names) + 1 :]
    vm = dict(zip(names, scratch[: len(names)]))
    (
        pay, pieces, carry_out, carry_in,
        part1, pair1, send1, recv1,
        stat0, stat1, stat2,
        sent, arrived, told, heard, gathered, acc_g, acc_s,
        part2, pair2, send2, recv2,
        rsend, returned,
        load_sem, pa_s, pa_r, pb_s,
        near1_r, far1_r, gone1_s, mean_s, sq1_s, sq2_s,
        dis_s, note_s, ret_s, wire_r, own_r, gone_s,
        near2_r, far2_r, gone2_s,
    ) = scratch[len(names) :]

    s = lax.axis_index("sp")
    t = lax.axis_index("tp")
    y = t // 2
    c = lax.rem(t, 2)
    other = 1 - c

    def at_sp(k):
        return {"sp": k, "tp": t}

    def at_tp(k):
        return {"sp": s, "tp": k}

    def remote(src, dst, send_sem, recv_sem, device):
        return pltpu.make_async_remote_copy(
            src_ref=src, dst_ref=dst, send_sem=send_sem, recv_sem=recv_sem,
            device_id=device, device_id_type=MESH,
        )

    barrier = pltpu.get_barrier_semaphore()

    def greet_sp(k, carry):
        pl.semaphore_signal(
            barrier, inc=1, device_id=at_sp(lax.rem(s + k, n_sp)), device_id_type=MESH
        )
        return carry

    def greet_tp(k, carry):
        pl.semaphore_signal(
            barrier, inc=1, device_id=at_tp(lax.rem(t + k, n_tp)), device_id_type=MESH
        )
        return carry

    lax.fori_loop(1, n_sp, greet_sp, 0)
    lax.fori_loop(1, n_tp, greet_tp, 0)
    sf = vm["common"].shape[0] // 2
    loads = {}
    for k, name in enumerate(names):
        into = vm[name]
        if name == "common":
            into = vm["common"].at[0:sf]
        if name == "common_raise":
            into = vm["common"].at[sf:]
        loads[name] = pltpu.make_async_copy(hbm[name], into, load_sem.at[k])
    early = ("probe", "address", "content", "storage", "fade", "extra", "channel", "label")
    for name in early:
        loads[name].start()
    for name in names:
        if name not in early:
            loads[name].start()
    for name in early:
        loads[name].wait()

    row_i, col_i = iota((rows, rows), 0), iota((rows, rows), 1)
    eye = row_i == col_i
    lower, strict = row_i >= col_i, row_i > col_i
    same_block = (row_i < BLOCK) == (col_i < BLOCK)

    def to_col(row):
        return jnp.sum(jnp.where(eye, row, 0.0), axis=1, keepdims=True)

    def to_row(col):
        return jnp.sum(jnp.where(eye, col, 0.0), axis=0, keepdims=True)

    queries = vm["probe"][...].astype(F32)
    keys = vm["address"][...].astype(F32)
    values = vm["content"][...].astype(F32)
    q_unit = queries * lax.rsqrt(
        jnp.sum(queries * queries, -1, keepdims=True) + 1e-06
    ) * queries.shape[-1] ** (-0.5)
    k_unit = keys * lax.rsqrt(jnp.sum(keys * keys, -1, keepdims=True) + 1e-06)
    gate = to_col(1.0 / (1.0 + jnp.exp(-vm["storage"][...])))
    fade = vm["fade"][...]
    softplus = jnp.maximum(fade, 0.0) + jnp.log(1.0 + jnp.exp(-jnp.abs(fade)))
    rate = jnp.exp(vm["channel"][...])
    decay = vm["extra"][...] - rate * softplus
    c_col = jnp.sum(jnp.where(lower, decay, 0.0), axis=1, keepdims=True)
    c_row = to_row(c_col)
    label_row = vm["label"][...].astype(F32)
    label_col = to_col(label_row)
    label_first, label_last = label_row[:, :1], label_row[:, rows - 1 :]
    c_last = c_row[:, rows - 1 :]
    reach = jnp.where(
        lower & (label_col == label_row), jnp.exp(jnp.where(lower, c_col - c_row, 0.0)), 0.0
    )
    weighted = k_unit * gate
    coupling = jnp.where(strict, mm_nt(weighted, k_unit) * reach, 0.0)
    power = jnp.where(same_block, coupling, 0.0)
    across = jnp.where(same_block, 0.0, coupling)
    inverse = jnp.where(eye, 1.0, 0.0) - power
    for _ in range(BLOCK.bit_length() - 2):
        power = mm(power, power)
        inverse = inverse + mm(inverse, power)
    inverse = inverse - mm(inverse, mm(across, inverse))
    growth = jnp.exp(c_col) * (label_col == label_first).astype(F32)
    both = mm(inverse, jnp.concatenate([weighted * growth, values * gate], axis=1))
    tail_keys = k_unit * (jnp.exp(c_last - c_col) * (label_col == label_last).astype(F32))
    ends = mm_tn(tail_keys, both)
    end_growth = jnp.exp(c_last) * (label_last == label_first).astype(F32)
    scores = mm_nt(q_unit, k_unit) * reach
    outs = mm(scores, both)
    width = q_unit.shape[-1]
    q_grown = q_unit * growth - outs[:, :width]
    own_mixed = outs[:, width:]
    state_map = (jnp.where(eye, end_growth, 0.0) - ends[:, :width]).astype(BF16)
    shift = ends[:, width:]
    marks_at = width + 16
    pay[0:width, :] = shift.astype(BF16)
    pay[width : width + 8, :] = jnp.broadcast_to(label_first, (8, width)).astype(BF16)
    pay[width + 8 : marks_at, :] = jnp.broadcast_to(label_last, (8, width)).astype(BF16)
    pay[marks_at:, :] = state_map
    pl.semaphore_wait(barrier, n_sp + n_tp - 2)
    tops = [pay.shape[0]] * (REACH - 1) + [marks_at]
    first = [
        remote(
            pay.at[0:top], pieces.at[k, 0:top], pa_s.at[k], pa_r.at[k],
            at_sp(lax.rem(s + k + 1, n_sp)),
        )
        for k, top in enumerate(tops)
    ]
    for k in reversed(range(REACH)):
        first[k].start()

    for name in names:
        if name not in early:
            loads[name].wait()
    pick0, pick1 = vm["picks"][0:1, :], vm["picks"][1:2, :]
    share = vm["share"][...].astype(F32)
    expert_i = iota((experts, rows), 0)
    to0, to1 = (expert_i == pick0).astype(F32), (expert_i == pick1).astype(F32)
    chosen = to0 + to1
    rank = mm(chosen, (row_i < col_i).astype(F32))
    coded = jnp.where(chosen > 0.0, rank + 1.0, 0.0)
    shares = to0 * share[0:1, :] + to1 * share[1:2, :]
    slot_i = iota((padded, experts), 0)
    from_e = iota((padded, experts), 1) * stride
    spread = ((slot_i >= from_e) & (slot_i < from_e + stride)).astype(F32)
    place = iota((n_sp, stride, rows), 1).reshape(padded, rows)
    wide = mm(spread, jnp.concatenate([coded, shares, to0], axis=1))
    hot = wide[:, :rows] == (place + 1).astype(F32)
    dispatch = hot.astype(BF16)
    slot_share = jnp.sum(jnp.where(hot, wide[:, rows : 2 * rows], 0.0), axis=1, keepdims=True)
    slot_first = jnp.sum(jnp.where(hot, wide[:, 2 * rows :], 0.0), axis=1, keepdims=True)
    here = (iota((padded, rows), 1) == place).astype(F32)

    def per_slot(column):
        return jnp.sum((here * column).reshape(n_sp, stride, rows), axis=1, keepdims=True)

    told[...] = jnp.zeros_like(told)
    told[:, 0:1, :] = per_slot(slot_share).astype(BF16)
    told[:, 1:2, :] = per_slot(slot_first).astype(BF16)
    compact_i = iota((slots, padded), 0).astype(F32)
    source = jnp.floor((compact_i + 0.5) * (1.0 / cap))
    within = compact_i - source * cap
    column = iota((slots, padded), 1).astype(F32)
    compact = (column == source * stride + within).astype(BF16)
    slot_lane = iota((slots, rows), 1).astype(F32) == within[:, :rows]
    valve = silu(vm["exit"][...].astype(F32))

    for k in range(REACH):
        first[k].wait_recv()

    def piece(k):
        label = pieces[k, width:marks_at, :].astype(F32)
        return pieces[k, 0:width, :], label[0:1, :], label[8:9, :]

    shift1, first1, last1 = piece(0)
    shift2, first2, last2 = piece(1)
    shift3, _, last3 = piece(2)
    map1 = pieces[0, marks_at:, :] * (first1 == last2).astype(BF16)
    map2 = pieces[1, marks_at:, :] * (first2 == last3).astype(BF16)
    joined = (label_first == last1).astype(F32)
    shift12 = shift1.astype(F32) + mm(map1, shift2)
    map12 = mm(map1, map2).astype(BF16)
    entering = (shift12 + mm(map12, shift3)) * joined
    carry_out[...] = (shift + mm(state_map, entering)).astype(BF16)
    second = remote(
        carry_out, carry_in, pb_s.at[0], pb_s.at[1], at_sp(lax.rem(s + REACH, n_sp))
    )
    second.start()
    second.wait_recv()
    incoming = (shift12 + mm(map12, carry_in[...])) * joined
    mixed = own_mixed + mm(q_grown, incoming)
    scaled = mixed * lax.rsqrt(jnp.mean(mixed * mixed, -1, keepdims=True) + 1e-06)
    heads_out = (scaled * valve).astype(BF16)

    def along(d):
        return lax.rem(y + d + 2 * ny, ny)

    def sigma_of(q):
        return 1 if q % 2 == 0 else -1

    soon, rest = (3, -3, 4), (1, -1, 2, -2, 0)

    class TpSum:
        def __init__(self, part, pair, send, recv, near_r, far_r, gone, chunk_rows):
            self.part, self.pair, self.send, self.recv = part, pair, send, recv
            self.near_r, self.far_r, self.gone, self.rows = near_r, far_r, gone, chunk_rows

        def at(self, q):
            return slice(q * self.rows, (q + 1) * self.rows)

        def put(self, d, at_rows, product):
            chip = along(d)
            self.part[chip, 0, at_rows] = product[:, :width].astype(BF16)
            self.part[chip, 1, at_rows] = product[:, width:].astype(BF16)

        def near(self, q, g):
            for d in (soon, rest)[g]:
                chip = along(d)
                remote(
                    self.part.at[chip, other, self.at(q)], self.pair.at[chip, self.at(q)],
                    self.gone.at[0], self.near_r.at[2 * q + g], at_tp(2 * y + other),
                ).start()

        def near_wait(self, q, g):
            there = self.pair.at[0 : len((soon, rest)[g]), self.at(q)]
            sem = self.near_r.at[2 * q + g]
            remote(there, there, sem, sem, at_tp(t)).wait_recv()

        def chip_sum(self, d, q):
            chip = along(d)
            mine = self.part[chip, c, self.at(q)].astype(F32)
            return mine + self.pair[chip, self.at(q)].astype(F32)

        def copy(self, line, q, to):
            return remote(
                self.send.at[line, self.at(q)], self.recv.at[line, self.at(q)], self.gone.at[1],
                self.far_r.at[line * CHUNKS + q], at_tp(2 * along(to) + c),
            )

        def go(self, line, q, to, value):
            self.send[line, self.at(q)] = value.astype(BF16)
            self.copy(line, q, to).start()

        def got(self, line, q):
            self.copy(line, q, 1).wait_recv()
            return self.recv[line, self.at(q)].astype(F32)

        def leg1(self, q):
            self.near_wait(q, 0)
            self.go(2, q, -2 * sigma_of(q), self.chip_sum(4, q))
            for i, sigma in enumerate((1, -1)):
                self.go(i, q, -sigma, self.chip_sum(-3 * sigma, q))

        def neighbours(self, q):
            self.near_wait(q, 1)
            for i, sigma in enumerate((1, -1)):
                self.go(3 + i, q, sigma, self.chip_sum(sigma, q))

        def leg2(self, q):
            for i, sigma in enumerate((1, -1)):
                value = self.chip_sum(-2 * sigma, q) + self.got(i, q)
                if sigma == sigma_of(q):
                    value = value + self.got(2, q)
                self.go(5 + i, q, -2 * sigma, value)

        def total(self, q):
            value = self.chip_sum(0, q)
            for line in (3, 4, 5, 6):
                value = value + self.got(line, q)
            return value

        def all_gone(self):
            there = self.part.at[:, 0]
            remote(there, there, self.gone.at[0], self.gone.at[0], at_tp(t)).wait_send()
            remote(
                self.send, self.send, self.gone.at[1], self.gone.at[1], at_tp(t)
            ).wait_send()

    def tell(stat, sems, line):
        stat[t] = line
        for k in range(1, n_tp):
            to = lax.rem(t + k, n_tp)
            remote(stat.at[t], stat.at[t], sems.at[0], sems.at[1], at_tp(to)).start()

    def heard_all(stat, sems):
        there = stat.at[1:n_tp]
        remote(there, there, sems.at[0], sems.at[1], at_tp(t)).wait()
        return jnp.sum(stat[...], axis=0)

    scaled_in = ALPHA * vm["incoming"][...].astype(F32)
    row_sum = jnp.sum(scaled_in, -1, keepdims=True)
    first_tp = TpSum(part1, pair1, send1, recv1, near1_r, far1_r, gone1_s, rows // CHUNKS)
    for g, group in enumerate((soon, rest)):
        for d in group:
            at = pl.ds(pl.multiple_of(along(d) * 2 * width, 2 * width), 2 * width)
            product = mm(heads_out, vm["final"][:, at])
            first_tp.put(d, slice(0, rows), product)
            row_sum = row_sum + jnp.sum(product, -1, keepdims=True)
        for q in range(CHUNKS):
            first_tp.near(q, g)
    for q in range(CHUNKS):
        first_tp.leg1(q)
    tell(stat0, mean_s, to_row(row_sum))
    for q in range(CHUNKS):
        first_tp.neighbours(q)
    for q in range(CHUNKS):
        first_tp.leg2(q)
    projected = jnp.concatenate([first_tp.total(q) for q in range(CHUNKS)], axis=0)
    features = width * n_tp
    mean = to_col(heard_all(stat0, mean_s) / features)
    centred = scaled_in + projected - mean

    nx = 4
    nz = n_sp // nx
    hops = sorted(
        ((dz, dx) for dz in range(nz) for dx in range(nx) if dz or dx),
        key=lambda d: -min(d[0], nz - d[0]) - min(d[1], nx - d[1]),
    )

    def scatter(src, dst, sems):
        z, x = s // nx, lax.rem(s, nx)
        for dz, dx in hops:
            to = lax.rem(z + dz, nz) * nx + lax.rem(x + dx, nx)
            remote(src.at[to], dst.at[s], sems.at[0], sems.at[1], at_sp(to)).start()
        dst[s] = src[s]

    def collected(dst, sems):
        there = dst.at[1:n_sp]
        remote(there, there, sems.at[0], sems.at[1], at_sp(s)).wait()
        return dst[...].reshape(dst.shape[0] * dst.shape[1], dst.shape[2])

    gained = (centred * vm["gain1"][...]).astype(BF16)
    payload = jnp.dot(dispatch, gained, preferred_element_type=F32)
    sent[...] = payload.astype(BF16).reshape(n_sp, stride, rows)
    scatter(sent, arrived, dis_s)
    tell(stat1, sq1_s, to_row(jnp.sum(centred * centred, -1, keepdims=True)))
    came = collected(arrived, dis_s)
    own_rows = jnp.dot(compact, came, preferred_element_type=F32).astype(BF16)

    lanes = pl.ds(pl.multiple_of(c * width, width), width)
    piece_rows = slots // CHUNKS

    def rows_of(q):
        return slice(q * piece_rows, (q + 1) * piece_rows)

    gathered[y, :, lanes] = own_rows

    def block(chip, q):
        return gathered.at[chip, rows_of(q), lanes]

    chips_of = ((0,), (2, -2), (1, -1), (3, -3, 4))

    def passed(d, q, to, line):
        there = block(along(d), q)
        return remote(
            there, there, gone_s.at[1], wire_r.at[line * CHUNKS + q], at_tp(2 * along(to) + c)
        )

    def came(d, q, line):
        passed(d, q, 1, line).wait_recv()

    def hand(k, q):
        for d in chips_of[k]:
            there = block(along(d), q)
            remote(
                there, there, gone_s.at[0], own_r.at[k * CHUNKS + q], at_tp(2 * y + other)
            ).start()

    def wait_bytes(count, sem):
        there = pair2.at[0:count, 0:piece_rows]
        remote(there, there, sem, sem, at_tp(t)).wait_recv()

    def absorb(k, q):
        chips, at_rows = [along(d) for d in chips_of[k]], rows_of(q)
        wait_bytes(len(chips), own_r.at[k * CHUNKS + q])
        for chip in chips:
            block_in = gathered[chip, at_rows, :]
            at = pl.ds(pl.multiple_of(chip * 2 * width, 2 * width), 2 * width)
            gates = jnp.dot(block_in, vm["valve"][at, :], preferred_element_type=F32)
            ups = jnp.dot(block_in, vm["raise"][at, :], preferred_element_type=F32)
            common = lax.dot_general(
                block_in, vm["common"][:, at], (((1,), (1,)), ((), ())), preferred_element_type=F32
            )
            if k == 0:
                acc_g[0, at_rows], acc_g[1, at_rows], acc_s[at_rows] = gates, ups, common
            else:
                acc_g[0, at_rows] += gates
                acc_g[1, at_rows] += ups
                acc_s[at_rows] += common

    def all_noted():
        notes = collected(heard, note_s)
        note_column = iota((slots, notes.shape[0]), 1).astype(F32)
        note_source = source[:, :1] * told.shape[1]

        def noted(j):
            line = (note_column == note_source + j).astype(BF16)
            found = jnp.dot(line, notes, preferred_element_type=F32)
            return jnp.sum(jnp.where(slot_lane, found, 0.0), axis=1, keepdims=True)

        return noted(0), noted(1), noted(2) + noted(3)

    for line, d in enumerate((2, -2, 1, -1)):
        for q in range(CHUNKS):
            passed(0, q, d, line).start()
    for q in range(CHUNKS):
        hand(0, q)
    row_scale = lax.rsqrt(heard_all(stat1, sq1_s) / features + 1e-05)
    slot_scale = jnp.sum(jnp.where(hot, row_scale, 0.0), axis=1, keepdims=True)
    scales = per_slot(slot_scale)
    coarse = scales.astype(BF16)
    told[:, 2:3, :] = coarse
    told[:, 3:4, :] = (scales - coarse.astype(F32)).astype(BF16)
    scatter(told, heard, note_s)
    middle = (centred * to_col(row_scale) * vm["gain1"][...]).astype(BF16)
    for q in range(CHUNKS):
        for line, sigma in enumerate((1, -1)):
            came(-2 * sigma, q, line)
            passed(-2 * sigma, q, sigma, 4 + line).start()
            if sigma == sigma_of(q):
                passed(-2 * sigma, q, 2 * sigma, 6).start()
        hand(1, q)
    for q in range(CHUNKS):
        absorb(0, q)
    for q in range(CHUNKS):
        for line, sigma in enumerate((1, -1)):
            came(-sigma, q, 2 + line)
        hand(2, q)
    for q in range(CHUNKS):
        absorb(1, q)
    slot_notes = all_noted()
    for q in range(CHUNKS):
        for line, sigma in enumerate((1, -1)):
            came(-3 * sigma, q, 4 + line)
        came(4, q, 6)
        hand(3, q)
        absorb(2, q)

    def expert(q):
        at_rows = rows_of(q)
        weight, flag, scale = (v[at_rows] for v in slot_notes)
        hidden = (silu(acc_g[0, at_rows] * scale) * acc_g[1, at_rows] * (scale * weight)).astype(
            BF16
        )
        common = acc_s[at_rows] * scale
        shared = (silu(common[:, :sf]) * common[:, sf:] * flag).astype(BF16)
        for g, group in enumerate((soon, rest)):
            for d in group:
                at = pl.ds(pl.multiple_of(along(d) * 2 * width, 2 * width), 2 * width)
                product = jnp.dot(hidden, vm["lower"][:, at], preferred_element_type=F32) + jnp.dot(
                    shared, vm["common_low"][:, at], preferred_element_type=F32
                )
                second_tp.put(d, at_rows, product)
            second_tp.near(q, g)

    second_tp = TpSum(part2, pair2, send2, recv2, near2_r, far2_r, gone2_s, piece_rows)
    for q in range(CHUNKS):
        absorb(3, q)
        expert(q)
    for q in range(CHUNKS):
        second_tp.leg1(q)
    for q in range(CHUNKS):
        second_tp.neighbours(q)
    for q in range(CHUNKS):
        second_tp.leg2(q)
    for q in range(CHUNKS):
        value = second_tp.total(q)
        share_sp = n_sp // CHUNKS
        owners = slice(q * share_sp, (q + 1) * share_sp)
        spots = slice(q * share_sp * stride, (q + 1) * share_sp * stride)
        rsend[owners] = (
            mm_tn(compact[rows_of(q), spots], value)
            .astype(BF16)
            .reshape(share_sp, stride, rows)
        )
        for k in range(share_sp):
            to = q * share_sp + lax.rem(s + k, share_sp)

            @pl.when(to != s)
            def _(to=to):
                remote(
                    rsend.at[to], returned.at[s], ret_s.at[0], ret_s.at[1], at_sp(to)
                ).start()

    returned[s] = rsend[s]
    back = collected(returned, ret_s)
    mixture = mm_tn(dispatch, back)
    second_sum = ALPHA * middle.astype(F32) + mixture
    sums = [jnp.sum(v, -1, keepdims=True) for v in (second_sum, second_sum * second_sum)]
    tell(stat2, sq2_s, jnp.concatenate([to_row(v) for v in sums], axis=0))
    totals = heard_all(stat2, sq2_s) / features
    mean2, square2 = totals[0:1, :], totals[1:2, :]
    scale2 = lax.rsqrt(square2 - mean2 * mean2 + 1e-05)
    out_ref[...] = (
        (second_sum - to_col(mean2)) * to_col(scale2) * vm["gain2"][...]
    ).astype(BF16)

    for copy in first:
        copy.wait_send()
    second.wait_send()
    def all_gone(there, sem):
        remote(there, there, sem, sem, at_tp(t)).wait_send()

    all_gone(pair2, gone_s.at[0])
    all_gone(pair2.at[1:ny], gone_s.at[1])
    first_tp.all_gone()
    second_tp.all_gone()


def dims_names():
    return (
        "probe", "address", "content", "storage", "fade", "extra", "label",
        "picks", "share", "exit", "incoming", "gain1", "gain2", "final",
        "valve", "raise", "lower", "common", "common_raise", "common_low", "channel",
    )


def shards(
    probe, address, content, storage, fade, channel, extra, label, exit_valve, final,
    incoming, gain1, picks, share, valve, raising, lowering, common_valve, common_raising,
    common_lowering, gain2,
):
    n_sp, n_tp = lax.axis_size("sp"), lax.axis_size("tp")
    ny = n_tp // 2
    rows, width = probe.shape
    experts = n_sp * valve.shape[0]
    cap = max(2, 9 * rows * picks.shape[1] // (8 * experts))
    stride = -(-(cap + 2) // 16) * 16
    slots = n_sp * cap
    ff, features = valve.shape[2], valve.shape[1]
    sf = common_valve.shape[1]
    dims = (n_sp, n_tp, rows, experts, cap, stride)
    args = {
        "probe": probe, "address": address, "content": content, "storage": storage,
        "fade": fade, "extra": extra, "label": label[None, :], "picks": picks.T,
        "share": share.T, "exit": exit_valve, "incoming": incoming, "gain1": gain1[None, :],
        "gain2": gain2[None, :], "final": final, "valve": valve[0], "raise": raising[0],
        "lower": lowering[0],
        "common": common_valve.T, "common_raise": common_raising.T,
        "common_low": common_lowering, "channel": channel[None, :],
    }
    names = dims_names()
    operands = [args[n] for n in names]
    dma = pltpu.SemaphoreType.DMA
    shapes = {n: a.shape for n, a in args.items()}
    shapes["common"] = (2 * sf, features)
    shapes["common_raise"] = (8, 128)
    own = [pltpu.VMEM(shapes[n], args[n].dtype) for n in names]

    def vmem(*shape, kind=BF16):
        return pltpu.VMEM(shape, kind)

    return pl.pallas_call(
        functools.partial(kernel, dims),
        out_shape=jax.ShapeDtypeStruct((rows, width), BF16),
        in_specs=[pl.BlockSpec(memory_space=pltpu.HBM)] * len(operands),
        out_specs=pl.BlockSpec(memory_space=pltpu.VMEM),
        scratch_shapes=own
        + [
            vmem(2 * width + 16, width), vmem(REACH, 2 * width + 16, width),
            vmem(width, width), vmem(width, width),
            vmem(ny, 2, rows, width), vmem(ny, rows, width), vmem(7, rows, width),
            vmem(7, rows, width),
            vmem(n_tp, 1, rows, kind=F32), vmem(n_tp, 1, rows, kind=F32),
            vmem(n_tp, 2, rows, kind=F32),
            vmem(n_sp, stride, width), vmem(n_sp, stride, width),
            vmem(n_sp, 16, width), vmem(n_sp, 16, width),
            vmem(ny, slots, 2 * width), vmem(2, slots, ff, kind=F32), vmem(slots, 2 * sf, kind=F32),
            vmem(ny, 2, slots, width), vmem(ny, slots, width), vmem(7, slots, width),
            vmem(7, slots, width),
            vmem(n_sp, stride, width), vmem(n_sp, stride, width),
            dma((len(operands),)), dma((REACH,)), dma((REACH,)), dma((2,)),
            dma((2 * CHUNKS,)), dma((7 * CHUNKS,)), dma((2,)), dma((2,)), dma((2,)), dma((2,)),
            dma((2,)), dma((2,)), dma((2,)), dma((7 * CHUNKS,)), dma((4 * CHUNKS,)), dma((2,)),
            dma((2 * CHUNKS,)), dma((7 * CHUNKS,)), dma((2,)),
        ],
        compiler_params=pltpu.CompilerParams(
            collective_id=0, has_side_effects=True, vmem_limit_bytes=60 * 1024 * 1024
        ),
        name="layer",
    )(*operands)


def solution(mesh):
    return jax.shard_map(
        shards,
        mesh=mesh,
        in_specs=(
            P("sp", "tp"), P("sp", "tp"), P("sp", "tp"), P("tp", "sp"), P("tp", "sp"), P("tp"),
            P("tp", "sp"), P("sp"), P("sp", "tp"), P("tp", None), P("sp", "tp"), P("tp"),
            P("sp", None), P("sp", None), P("sp", None, "tp"), P("sp", None, "tp"),
            P("sp", "tp", None), P(None, "tp"), P(None, "tp"), P("tp", None), P("tp"),
        ),
        out_specs=P("sp", "tp"),
        check_vma=False,
    )
```

```python
import functools

import jax
import jax.numpy as jnp
from jax import lax
from jax.experimental import pallas as pl
from jax.experimental.pallas import tpu as pltpu
from jax.sharding import PartitionSpec as P

BLOCK = 64
ALPHA = 2.0**0.25
F32 = jnp.float32
BF16 = jnp.bfloat16
MESH = pl.DeviceIdType.MESH
REACH = 3
CHUNKS = 2


def iota(shape, dim):
    return lax.broadcasted_iota(jnp.int32, shape, dim)


def mm(a, b):
    return jnp.dot(a.astype(BF16), b.astype(BF16), preferred_element_type=F32)


def mm_nt(a, b):
    return lax.dot_general(
        a.astype(BF16), b.astype(BF16), (((1,), (1,)), ((), ())), preferred_element_type=F32
    )


def mm_tn(a, b):
    return lax.dot_general(
        a.astype(BF16), b.astype(BF16), (((0,), (0,)), ((), ())), preferred_element_type=F32
    )


def silu(v):
    return v / (1.0 + jnp.exp(-v))


def kernel(dims, *refs):
    n_sp, n_tp, rows, experts, cap, stride = dims
    ny = n_tp // 2
    slots = n_sp * cap
    padded = n_sp * stride
    names = dims_names()
    hbm = dict(zip(names, refs[: len(names)]))
    out_ref = refs[len(names)]
    scratch = refs[len(names) + 1 :]
    vm = dict(zip(names, scratch[: len(names)]))
    (
        pay, pieces, carry_out, carry_in,
        part1, pair1, send1, recv1,
        stat0, stat1, stat2,
        sent, arrived, told, heard, gathered, acc_g, acc_s,
        part2, pair2, send2, recv2,
        rsend, returned, undo, widen,
        load_sem, pa_s, pa_r, pb_s,
        near1_r, far1_r, gone1_s, mean_s, sq1_s, sq2_s,
        dis_s, note_s, ret_s, wire_r, own_r, gone_s,
        near2_r, far2_r, gone2_s,
    ) = scratch[len(names) :]

    s = lax.axis_index("sp")
    t = lax.axis_index("tp")
    y = t // 2
    c = lax.rem(t, 2)
    other = 1 - c

    def at_sp(k):
        return {"sp": k, "tp": t}

    def at_tp(k):
        return {"sp": s, "tp": k}

    def remote(src, dst, send_sem, recv_sem, device):
        return pltpu.make_async_remote_copy(
            src_ref=src, dst_ref=dst, send_sem=send_sem, recv_sem=recv_sem,
            device_id=device, device_id_type=MESH,
        )

    barrier = pltpu.get_barrier_semaphore()

    nx = 4
    nz = n_sp // nx
    hops = sorted(
        ((dz, dx) for dz in range(nz) for dx in range(nx) if dz or dx),
        key=lambda d: -min(d[0], nz - d[0]) - min(d[1], nx - d[1]),
    )
    z, x = s // nx, lax.rem(s, nx)

    def beside(dz, dx):
        return lax.rem(z + dz, nz) * nx + lax.rem(x + dx, nx)

    for dz, dx in hops:
        pl.semaphore_signal(
            barrier, inc=1, device_id=at_sp(beside(dz, dx)), device_id_type=MESH
        )
    for k in sorted(range(1, n_tp), key=lambda k: -min(k, n_tp - k)):
        pl.semaphore_signal(
            barrier, inc=1, device_id=at_tp(lax.rem(t + k, n_tp)), device_id_type=MESH
        )
    sf = vm["common"].shape[0] // 2
    loads = {}
    for k, name in enumerate(names):
        into = vm[name]
        if name == "common":
            into = vm["common"].at[0:sf]
        if name == "common_raise":
            into = vm["common"].at[sf:]
        loads[name] = pltpu.make_async_copy(hbm[name], into, load_sem.at[k])
    early = ("probe", "address", "content", "storage", "fade", "extra", "channel", "label")
    for name in early:
        loads[name].start()
    for name in names:
        if name not in early:
            loads[name].start()
    for name in early:
        loads[name].wait()

    row_i, col_i = iota((rows, rows), 0), iota((rows, rows), 1)
    eye = row_i == col_i
    lower, strict = row_i >= col_i, row_i > col_i
    same_block = (row_i < BLOCK) == (col_i < BLOCK)

    def to_col(row):
        return jnp.sum(jnp.where(eye, row, 0.0), axis=1, keepdims=True)

    def to_row(col):
        return jnp.sum(jnp.where(eye, col, 0.0), axis=0, keepdims=True)

    queries = vm["probe"][...].astype(F32)
    keys = vm["address"][...].astype(F32)
    values = vm["content"][...].astype(F32)
    q_unit = queries * lax.rsqrt(
        jnp.sum(queries * queries, -1, keepdims=True) + 1e-06
    ) * queries.shape[-1] ** (-0.5)
    k_unit = keys * lax.rsqrt(jnp.sum(keys * keys, -1, keepdims=True) + 1e-06)
    gate = to_col(1.0 / (1.0 + jnp.exp(-vm["storage"][...])))
    fade = vm["fade"][...]
    softplus = jnp.maximum(fade, 0.0) + jnp.log(1.0 + jnp.exp(-jnp.abs(fade)))
    rate = jnp.exp(vm["channel"][...])
    decay = vm["extra"][...] - rate * softplus
    c_col = jnp.sum(jnp.where(lower, decay, 0.0), axis=1, keepdims=True)
    c_row = to_row(c_col)
    label_row = vm["label"][...].astype(F32)
    label_col = to_col(label_row)
    label_first, label_last = label_row[:, :1], label_row[:, rows - 1 :]
    c_last = c_row[:, rows - 1 :]
    reach = jnp.where(
        lower & (label_col == label_row), jnp.exp(jnp.where(lower, c_col - c_row, 0.0)), 0.0
    )
    weighted = k_unit * gate
    coupling = jnp.where(strict, mm_nt(weighted, k_unit) * reach, 0.0)
    power = jnp.where(same_block, coupling, 0.0)
    across = jnp.where(same_block, 0.0, coupling)
    inverse = jnp.where(eye, 1.0, 0.0) - power
    for _ in range(BLOCK.bit_length() - 2):
        power = mm(power, power)
        inverse = inverse + mm(inverse, power)
    inverse = inverse - mm(inverse, mm(across, inverse))
    growth = jnp.exp(c_col) * (label_col == label_first).astype(F32)
    both = mm(inverse, jnp.concatenate([weighted * growth, values * gate], axis=1))
    tail_keys = k_unit * (jnp.exp(c_last - c_col) * (label_col == label_last).astype(F32))
    ends = mm_tn(tail_keys, both)
    end_growth = jnp.exp(c_last) * (label_last == label_first).astype(F32)
    scores = mm_nt(q_unit, k_unit) * reach
    outs = mm(scores, both)
    width = q_unit.shape[-1]
    q_grown = q_unit * growth - outs[:, :width]
    own_mixed = outs[:, width:]
    state_map = (jnp.where(eye, end_growth, 0.0) - ends[:, :width]).astype(BF16)
    shift = ends[:, width:]
    marks_at = width + 16
    pay[0:width, :] = shift.astype(BF16)
    pay[width : width + 8, :] = jnp.broadcast_to(label_first, (8, width)).astype(BF16)
    pay[width + 8 : marks_at, :] = jnp.broadcast_to(label_last, (8, width)).astype(BF16)
    pay[marks_at:, :] = state_map
    pl.semaphore_wait(barrier, n_sp + n_tp - 2)
    tops = [pay.shape[0]] * (REACH - 1) + [marks_at]
    first = [
        remote(
            pay.at[0:top], pieces.at[k, 0:top], pa_s.at[k], pa_r.at[k],
            at_sp(lax.rem(s + k + 1, n_sp)),
        )
        for k, top in enumerate(tops)
    ]
    for k in reversed(range(REACH)):
        first[k].start()

    for name in names:
        if name not in early:
            loads[name].wait()
    pick0, pick1 = vm["picks"][0:1, :], vm["picks"][1:2, :]
    share = vm["share"][...].astype(F32)
    expert_i = iota((experts, rows), 0)
    to0, to1 = (expert_i == pick0).astype(F32), (expert_i == pick1).astype(F32)
    chosen = to0 + to1
    rank = mm(chosen, (row_i < col_i).astype(F32))
    coded = jnp.where(chosen > 0.0, rank + 1.0, 0.0)
    shares = to0 * share[0:1, :] + to1 * share[1:2, :]
    slot_i = iota((padded, experts), 0)
    from_e = iota((padded, experts), 1) * stride
    spread = ((slot_i >= from_e) & (slot_i < from_e + stride)).astype(F32)
    place = iota((n_sp, stride, rows), 1).reshape(padded, rows)
    wide = mm(spread, jnp.concatenate([coded, shares, to0], axis=1))
    hot = wide[:, :rows] == (place + 1).astype(F32)
    dispatch = hot.astype(BF16)
    undo[...] = hot.astype(F32).T.astype(BF16)
    slot_share = jnp.sum(jnp.where(hot, wide[:, rows : 2 * rows], 0.0), axis=1, keepdims=True)
    slot_first = jnp.sum(jnp.where(hot, wide[:, 2 * rows :], 0.0), axis=1, keepdims=True)
    here = (iota((padded, rows), 1) == place).astype(F32)

    def per_slot(column):
        return jnp.sum((here * column).reshape(n_sp, stride, rows), axis=1, keepdims=True)

    told[...] = jnp.zeros_like(told)
    told[:, 0:1, :] = per_slot(slot_share).astype(BF16)
    told[:, 1:2, :] = per_slot(slot_first).astype(BF16)
    compact_i = iota((slots, padded), 0).astype(F32)
    source = jnp.floor((compact_i + 0.5) * (1.0 / cap))
    within = compact_i - source * cap
    column = iota((slots, padded), 1).astype(F32)
    compact = (column == source * stride + within).astype(BF16)
    open_i = iota((padded, slots), 1).astype(F32)
    open_source = jnp.floor((open_i + 0.5) * (1.0 / cap))
    spread_out = (
        iota((padded, slots), 0).astype(F32) == open_source * (stride - cap) + open_i
    ).astype(BF16)
    widen[...] = spread_out
    slot_lane = iota((slots, rows), 1).astype(F32) == within[:, :rows]
    valve = silu(vm["exit"][...].astype(F32))

    for k in range(REACH):
        first[k].wait_recv()

    def piece(k):
        label = pieces[k, width:marks_at, :].astype(F32)
        return pieces[k, 0:width, :], label[0:1, :], label[8:9, :]

    shift1, first1, last1 = piece(0)
    shift2, first2, last2 = piece(1)
    shift3, _, last3 = piece(2)
    map1 = pieces[0, marks_at:, :] * (first1 == last2).astype(BF16)
    map2 = pieces[1, marks_at:, :] * (first2 == last3).astype(BF16)
    joined = (label_first == last1).astype(F32)
    shift12 = shift1.astype(F32) + mm(map1, shift2)
    map12 = mm(map1, map2).astype(BF16)
    entering = (shift12 + mm(map12, shift3)) * joined
    carry_out[...] = (shift + mm(state_map, entering)).astype(BF16)
    second = remote(
        carry_out, carry_in, pb_s.at[0], pb_s.at[1], at_sp(lax.rem(s + REACH, n_sp))
    )
    second.start()
    from_carry = mm(q_grown, map12).astype(BF16)
    known = own_mixed + mm(q_grown, shift12) * joined
    second.wait_recv()
    mixed = known + mm(from_carry, carry_in[...]) * joined
    scaled = mixed * lax.rsqrt(jnp.mean(mixed * mixed, -1, keepdims=True) + 1e-06)
    heads_out = (scaled * valve).astype(BF16)

    def along(d):
        return lax.rem(y + d + 2 * ny, ny)

    def sigma_of(q):
        return 1 if q % 2 == 0 else -1

    soon, rest = (3, -3, 4), (1, -1, 2, -2, 0)

    class TpSum:
        def __init__(self, part, pair, send, recv, near_r, far_r, gone, chunk_rows):
            self.part, self.pair, self.send, self.recv = part, pair, send, recv
            self.near_r, self.far_r, self.gone, self.rows = near_r, far_r, gone, chunk_rows

        def at(self, q):
            return slice(q * self.rows, (q + 1) * self.rows)

        def put(self, d, at_rows, product):
            chip = along(d)
            self.part[chip, 0, at_rows] = product[:, :width].astype(BF16)
            self.part[chip, 1, at_rows] = product[:, width:].astype(BF16)

        def near(self, q, g):
            for d in (soon, rest)[g]:
                chip = along(d)
                remote(
                    self.part.at[chip, other, self.at(q)], self.pair.at[chip, self.at(q)],
                    self.gone.at[0], self.near_r.at[2 * q + g], at_tp(2 * y + other),
                ).start()

        def near_wait(self, q, g):
            there = self.pair.at[0 : len((soon, rest)[g]), self.at(q)]
            sem = self.near_r.at[2 * q + g]
            remote(there, there, sem, sem, at_tp(t)).wait_recv()

        def chip_sum(self, d, q):
            chip = along(d)
            mine = self.part[chip, c, self.at(q)].astype(F32)
            return mine + self.pair[chip, self.at(q)].astype(F32)

        def copy(self, line, q, to):
            return remote(
                self.send.at[line, self.at(q)], self.recv.at[line, self.at(q)], self.gone.at[1],
                self.far_r.at[line * CHUNKS + q], at_tp(2 * along(to) + c),
            )

        def go(self, line, q, to, value):
            self.send[line, self.at(q)] = value.astype(BF16)
            self.copy(line, q, to).start()

        def got(self, line, q):
            self.copy(line, q, 1).wait_recv()
            return self.recv[line, self.at(q)].astype(F32)

        def leg1(self, q):
            self.near_wait(q, 0)
            self.go(2, q, -2 * sigma_of(q), self.chip_sum(4, q))
            for i, sigma in enumerate((1, -1)):
                self.go(i, q, -sigma, self.chip_sum(-3 * sigma, q))

        def neighbours(self, q):
            self.near_wait(q, 1)
            for i, sigma in enumerate((1, -1)):
                self.go(3 + i, q, sigma, self.chip_sum(sigma, q))

        def leg2(self, q):
            for i, sigma in enumerate((1, -1)):
                value = self.chip_sum(-2 * sigma, q) + self.got(i, q)
                if sigma == sigma_of(q):
                    value = value + self.got(2, q)
                self.go(5 + i, q, -2 * sigma, value)

        def total(self, q):
            value = self.chip_sum(0, q)
            for line in (3, 4, 5, 6):
                value = value + self.got(line, q)
            return value

        def all_gone(self):
            there = self.part.at[:, 0]
            remote(there, there, self.gone.at[0], self.gone.at[0], at_tp(t)).wait_send()
            remote(
                self.send, self.send, self.gone.at[1], self.gone.at[1], at_tp(t)
            ).wait_send()

    def tell(stat, sems, line):
        stat[t] = line
        for k in range(1, n_tp):
            to = lax.rem(t + k, n_tp)
            remote(stat.at[t], stat.at[t], sems.at[0], sems.at[1], at_tp(to)).start()

    def heard_all(stat, sems):
        there = stat.at[1:n_tp]
        remote(there, there, sems.at[0], sems.at[1], at_tp(t)).wait()
        return jnp.sum(stat[...], axis=0)

    scaled_in = ALPHA * vm["incoming"][...].astype(F32)
    row_sum = jnp.sum(scaled_in, -1, keepdims=True)
    first_tp = TpSum(part1, pair1, send1, recv1, near1_r, far1_r, gone1_s, rows // CHUNKS)
    for g, group in enumerate((soon, rest)):
        for d in group:
            at = pl.ds(pl.multiple_of(along(d) * 2 * width, 2 * width), 2 * width)
            product = mm(heads_out, vm["final"][:, at])
            first_tp.put(d, slice(0, rows), product)
            row_sum = row_sum + jnp.sum(product, -1, keepdims=True)
        for q in range(CHUNKS):
            first_tp.near(q, g)
    for q in range(CHUNKS):
        first_tp.leg1(q)
    tell(stat0, mean_s, to_row(row_sum))
    for q in range(CHUNKS):
        first_tp.neighbours(q)
    for q in range(CHUNKS):
        first_tp.leg2(q)
    projected = jnp.concatenate([first_tp.total(q) for q in range(CHUNKS)], axis=0)
    features = width * n_tp
    mean = to_col(heard_all(stat0, mean_s) / features)
    centred = scaled_in + projected - mean

    sent_rows = -(-cap // 2) * 2

    def scattered(src, dst, sems, to):
        top = min(src.shape[1], sent_rows)
        return remote(
            src.at[to, 0:top], dst.at[s, 0:top], sems.at[0], sems.at[1], at_sp(to)
        )

    def scatter(src, dst, sems):
        for dz, dx in hops:
            scattered(src, dst, sems, beside(dz, dx)).start()
        dst[s] = src[s]

    def collected(dst, sems):
        top = min(dst.shape[1], sent_rows)
        there = dst.at[1:n_sp, 0:top]
        remote(there, there, sems.at[0], sems.at[1], at_sp(s)).wait()
        came = jnp.where(iota(dst.shape, 1) < top, dst[...].astype(F32), 0.0).astype(BF16)
        return came.reshape(dst.shape[0] * dst.shape[1], dst.shape[2])

    gained = (centred * vm["gain1"][...]).astype(BF16)
    payload = jnp.dot(dispatch, gained, preferred_element_type=F32)
    sent[...] = payload.astype(BF16).reshape(n_sp, stride, rows)
    scatter(sent, arrived, dis_s)
    tell(stat1, sq1_s, to_row(jnp.sum(centred * centred, -1, keepdims=True)))
    came = collected(arrived, dis_s)
    own_rows = jnp.dot(compact, came, preferred_element_type=F32).astype(BF16)

    lanes = pl.ds(pl.multiple_of(c * width, width), width)
    piece_rows = slots // CHUNKS

    def rows_of(q):
        return slice(q * piece_rows, (q + 1) * piece_rows)

    gathered[y, :, lanes] = own_rows

    def block(chip, q):
        return gathered.at[chip, rows_of(q), lanes]

    chips_of = ((0,), (2, -2), (1, -1), (3, -3, 4))

    def passed(d, q, to, line):
        there = block(along(d), q)
        return remote(
            there, there, gone_s.at[1], wire_r.at[line * CHUNKS + q], at_tp(2 * along(to) + c)
        )

    def came(d, q, line):
        passed(d, q, 1, line).wait_recv()

    def hand(k, q):
        for d in chips_of[k]:
            there = block(along(d), q)
            remote(
                there, there, gone_s.at[0], own_r.at[k * CHUNKS + q], at_tp(2 * y + other)
            ).start()

    def wait_bytes(count, sem):
        there = pair2.at[0:count, 0:piece_rows]
        remote(there, there, sem, sem, at_tp(t)).wait_recv()

    def absorb(k, q):
        chips, at_rows = [along(d) for d in chips_of[k]], rows_of(q)
        wait_bytes(len(chips), own_r.at[k * CHUNKS + q])
        gates = ups = common = 0.0
        for chip in chips:
            block_in = gathered[chip, at_rows, :]
            at = pl.ds(pl.multiple_of(chip * 2 * width, 2 * width), 2 * width)
            gates += jnp.dot(block_in, vm["valve"][at, :], preferred_element_type=F32)
            ups += jnp.dot(block_in, vm["raise"][at, :], preferred_element_type=F32)
            common += lax.dot_general(
                block_in, vm["common"][:, at], (((1,), (1,)), ((), ())), preferred_element_type=F32
            )
        if k:
            gates, ups = gates + acc_g[0, at_rows], ups + acc_g[1, at_rows]
            common = common + acc_s[at_rows]
        if k < 3:
            acc_g[0, at_rows], acc_g[1, at_rows], acc_s[at_rows] = gates, ups, common
        return gates, ups, common

    def all_noted():
        notes = collected(heard, note_s)
        note_column = iota((slots, notes.shape[0]), 1).astype(F32)
        note_source = source[:, :1] * told.shape[1]

        def noted(j):
            line = (note_column == note_source + j).astype(BF16)
            found = jnp.dot(line, notes, preferred_element_type=F32)
            return jnp.sum(jnp.where(slot_lane, found, 0.0), axis=1, keepdims=True)

        return noted(0), noted(1), noted(2) + noted(3)

    for line, d in enumerate((2, -2, 1, -1)):
        for q in range(CHUNKS):
            passed(0, q, d, line).start()
    for q in range(CHUNKS):
        hand(0, q)
    row_scale = lax.rsqrt(heard_all(stat1, sq1_s) / features + 1e-05)
    slot_scale = jnp.sum(jnp.where(hot, row_scale, 0.0), axis=1, keepdims=True)
    scales = per_slot(slot_scale)
    coarse = scales.astype(BF16)
    told[:, 2:3, :] = coarse
    told[:, 3:4, :] = (scales - coarse.astype(F32)).astype(BF16)
    scatter(told, heard, note_s)
    middle = (centred * to_col(row_scale) * vm["gain1"][...]).astype(BF16)
    for q in range(CHUNKS):
        for line, sigma in enumerate((1, -1)):
            came(-2 * sigma, q, line)
            passed(-2 * sigma, q, sigma, 4 + line).start()
            if sigma == sigma_of(q):
                passed(-2 * sigma, q, 2 * sigma, 6).start()
        hand(1, q)
    for q in range(CHUNKS):
        absorb(0, q)
    for q in range(CHUNKS):
        for line, sigma in enumerate((1, -1)):
            came(-sigma, q, 2 + line)
        hand(2, q)
    for q in range(CHUNKS):
        absorb(1, q)
    slot_notes = all_noted()
    for q in range(CHUNKS):
        for line, sigma in enumerate((1, -1)):
            came(-3 * sigma, q, 4 + line)
        came(4, q, 6)
        hand(3, q)
        absorb(2, q)

    def expert(q, gates, ups, common):
        at_rows = rows_of(q)
        weight, flag, scale = (v[at_rows] for v in slot_notes)
        hidden = (silu(gates * scale) * ups * (scale * weight)).astype(BF16)
        common = common * scale
        shared = (silu(common[:, :sf]) * common[:, sf:] * flag).astype(BF16)
        for g, group in enumerate((soon, rest)):
            for d in group:
                at = pl.ds(pl.multiple_of(along(d) * 2 * width, 2 * width), 2 * width)
                product = jnp.dot(hidden, vm["lower"][:, at], preferred_element_type=F32) + jnp.dot(
                    shared, vm["common_low"][:, at], preferred_element_type=F32
                )
                second_tp.put(d, at_rows, product)
            second_tp.near(q, g)

    second_tp = TpSum(part2, pair2, send2, recv2, near2_r, far2_r, gone2_s, piece_rows)
    for q in range(CHUNKS):
        expert(q, *absorb(3, q))
    for q in range(CHUNKS):
        second_tp.leg1(q)
    for q in range(CHUNKS):
        second_tp.neighbours(q)
    for q in range(CHUNKS):
        second_tp.leg2(q)
    for q in range(CHUNKS):
        value = second_tp.total(q)
        share_sp = n_sp // CHUNKS
        owners = slice(q * share_sp, (q + 1) * share_sp)
        spots = slice(q * share_sp * stride, (q + 1) * share_sp * stride)
        rsend[owners] = (
            mm(widen[spots, rows_of(q)], value)
            .astype(BF16)
            .reshape(share_sp, stride, rows)
        )
        for k in range(share_sp):
            to = q * share_sp + lax.rem(s + k, share_sp)

            @pl.when(to != s)
            def _(to=to):
                scattered(rsend, returned, ret_s, to).start()

    returned[s] = rsend[s]
    back = collected(returned, ret_s)
    mixture = mm(undo[...], back)
    second_sum = ALPHA * middle.astype(F32) + mixture
    sums = [jnp.sum(v, -1, keepdims=True) for v in (second_sum, second_sum * second_sum)]
    tell(stat2, sq2_s, jnp.concatenate([to_row(v) for v in sums], axis=0))
    totals = heard_all(stat2, sq2_s) / features
    mean2, square2 = totals[0:1, :], totals[1:2, :]
    scale2 = lax.rsqrt(square2 - mean2 * mean2 + 1e-05)
    out_ref[...] = (
        (second_sum - to_col(mean2)) * to_col(scale2) * vm["gain2"][...]
    ).astype(BF16)

    for copy in first:
        copy.wait_send()
    second.wait_send()
    def all_gone(there, sem):
        remote(there, there, sem, sem, at_tp(t)).wait_send()

    all_gone(pair2, gone_s.at[0])
    all_gone(pair2.at[1:ny], gone_s.at[1])
    first_tp.all_gone()
    second_tp.all_gone()


def dims_names():
    return (
        "probe", "address", "content", "storage", "fade", "extra", "label",
        "picks", "share", "exit", "incoming", "gain1", "gain2", "final",
        "valve", "raise", "lower", "common", "common_raise", "common_low", "channel",
    )


def shards(
    probe, address, content, storage, fade, channel, extra, label, exit_valve, final,
    incoming, gain1, picks, share, valve, raising, lowering, common_valve, common_raising,
    common_lowering, gain2,
):
    n_sp, n_tp = lax.axis_size("sp"), lax.axis_size("tp")
    ny = n_tp // 2
    rows, width = probe.shape
    experts = n_sp * valve.shape[0]
    cap = max(2, 9 * rows * picks.shape[1] // (8 * experts))
    stride = -(-(cap + 2) // 16) * 16
    slots = n_sp * cap
    ff, features = valve.shape[2], valve.shape[1]
    sf = common_valve.shape[1]
    dims = (n_sp, n_tp, rows, experts, cap, stride)
    args = {
        "probe": probe, "address": address, "content": content, "storage": storage,
        "fade": fade, "extra": extra, "label": label[None, :], "picks": picks.T,
        "share": share.T, "exit": exit_valve, "incoming": incoming, "gain1": gain1[None, :],
        "gain2": gain2[None, :], "final": final, "valve": valve[0], "raise": raising[0],
        "lower": lowering[0],
        "common": common_valve.T, "common_raise": common_raising.T,
        "common_low": common_lowering, "channel": channel[None, :],
    }
    names = dims_names()
    operands = [args[n] for n in names]
    dma = pltpu.SemaphoreType.DMA
    shapes = {n: a.shape for n, a in args.items()}
    shapes["common"] = (2 * sf, features)
    shapes["common_raise"] = (8, 128)
    own = [pltpu.VMEM(shapes[n], args[n].dtype) for n in names]

    def vmem(*shape, kind=BF16):
        return pltpu.VMEM(shape, kind)

    return pl.pallas_call(
        functools.partial(kernel, dims),
        out_shape=jax.ShapeDtypeStruct((rows, width), BF16),
        in_specs=[pl.BlockSpec(memory_space=pltpu.HBM)] * len(operands),
        out_specs=pl.BlockSpec(memory_space=pltpu.VMEM),
        scratch_shapes=own
        + [
            vmem(2 * width + 16, width), vmem(REACH, 2 * width + 16, width),
            vmem(width, width), vmem(width, width),
            vmem(ny, 2, rows, width), vmem(ny, rows, width), vmem(7, rows, width),
            vmem(7, rows, width),
            vmem(n_tp, 1, rows, kind=F32), vmem(n_tp, 1, rows, kind=F32),
            vmem(n_tp, 2, rows, kind=F32),
            vmem(n_sp, stride, width), vmem(n_sp, stride, width),
            vmem(n_sp, 8, width), vmem(n_sp, 8, width),
            vmem(ny, slots, 2 * width), vmem(2, slots, ff, kind=F32), vmem(slots, 2 * sf, kind=F32),
            vmem(ny, 2, slots, width), vmem(ny, slots, width), vmem(7, slots, width),
            vmem(7, slots, width),
            vmem(n_sp, stride, width), vmem(n_sp, stride, width),
            vmem(rows, n_sp * stride), vmem(n_sp * stride, slots),
            dma((len(operands),)), dma((REACH,)), dma((REACH,)), dma((2,)),
            dma((2 * CHUNKS,)), dma((7 * CHUNKS,)), dma((2,)), dma((2,)), dma((2,)), dma((2,)),
            dma((2,)), dma((2,)), dma((2,)), dma((7 * CHUNKS,)), dma((4 * CHUNKS,)), dma((2,)),
            dma((2 * CHUNKS,)), dma((7 * CHUNKS,)), dma((2,)),
        ],
        compiler_params=pltpu.CompilerParams(
            collective_id=0, has_side_effects=True, vmem_limit_bytes=60 * 1024 * 1024
        ),
        name="layer",
    )(*operands)


def solution(mesh):
    return jax.shard_map(
        shards,
        mesh=mesh,
        in_specs=(
            P("sp", "tp"), P("sp", "tp"), P("sp", "tp"), P("tp", "sp"), P("tp", "sp"), P("tp"),
            P("tp", "sp"), P("sp"), P("sp", "tp"), P("tp", None), P("sp", "tp"), P("tp"),
            P("sp", None), P("sp", None), P("sp", None, "tp"), P("sp", None, "tp"),
            P("sp", "tp", None), P(None, "tp"), P(None, "tp"), P("tp", None), P("tp"),
        ),
        out_specs=P("sp", "tp"),
        check_vma=False,
    )
```

```python
import functools

import jax
import jax.numpy as jnp
from jax import lax
from jax.experimental import pallas as pl
from jax.experimental.pallas import tpu as pltpu
from jax.sharding import PartitionSpec as P

BLOCK = 64
ALPHA = 2.0**0.25
F32 = jnp.float32
BF16 = jnp.bfloat16
MESH = pl.DeviceIdType.MESH
REACH = 3
CHUNKS = 2


def iota(shape, dim):
    return lax.broadcasted_iota(jnp.int32, shape, dim)


def mm(a, b):
    return jnp.dot(a.astype(BF16), b.astype(BF16), preferred_element_type=F32)


def mm_nt(a, b):
    return lax.dot_general(
        a.astype(BF16), b.astype(BF16), (((1,), (1,)), ((), ())), preferred_element_type=F32
    )


def mm_tn(a, b):
    return lax.dot_general(
        a.astype(BF16), b.astype(BF16), (((0,), (0,)), ((), ())), preferred_element_type=F32
    )


def silu(v):
    return v / (1.0 + jnp.exp(-v))


def kernel(dims, *refs):
    n_sp, n_tp, rows, experts, cap, stride = dims
    ny = n_tp // 2
    slots = n_sp * cap
    padded = n_sp * stride
    names = dims_names()
    hbm = dict(zip(names, refs[: len(names)]))
    out_ref = refs[len(names)]
    scratch = refs[len(names) + 1 :]
    vm = dict(zip(names, scratch[: len(names)]))
    (
        pay, pieces, carry_out, carry_in,
        part1, pair1, send1, recv1,
        stat0, stat1, stat2,
        sent, arrived, told, heard, gathered, acc_g, acc_s,
        part2, pair2, send2, recv2,
        rsend, returned, undo, widen,
        load_sem, pa_s, pa_r, pb_s,
        near1_r, far1_r, gone1_s, mean_s, sq1_s, sq2_s,
        dis_s, note_s, ret_s, wire_r, own_r, gone_s,
        near2_r, far2_r, gone2_s,
    ) = scratch[len(names) :]

    s = lax.axis_index("sp")
    t = lax.axis_index("tp")
    y = t // 2
    c = lax.rem(t, 2)
    other = 1 - c

    def at_sp(k):
        return {"sp": k, "tp": t}

    def at_tp(k):
        return {"sp": s, "tp": k}

    def remote(src, dst, send_sem, recv_sem, device):
        return pltpu.make_async_remote_copy(
            src_ref=src, dst_ref=dst, send_sem=send_sem, recv_sem=recv_sem,
            device_id=device, device_id_type=MESH,
        )

    barrier = pltpu.get_barrier_semaphore()

    nx = 4
    nz = n_sp // nx
    hops = sorted(
        ((dz, dx) for dz in range(nz) for dx in range(nx) if dz or dx),
        key=lambda d: -min(d[0], nz - d[0]) - min(d[1], nx - d[1]),
    )
    z, x = s // nx, lax.rem(s, nx)

    def beside(dz, dx):
        return lax.rem(z + dz, nz) * nx + lax.rem(x + dx, nx)

    for dz, dx in hops:
        pl.semaphore_signal(
            barrier, inc=1, device_id=at_sp(beside(dz, dx)), device_id_type=MESH
        )
    for k in sorted(range(1, n_tp), key=lambda k: -min(k, n_tp - k)):
        pl.semaphore_signal(
            barrier, inc=1, device_id=at_tp(lax.rem(t + k, n_tp)), device_id_type=MESH
        )
    sf = vm["common"].shape[0] // 2
    loads = {}
    for k, name in enumerate(names):
        into = vm[name]
        if name == "common":
            into = vm["common"].at[0:sf]
        if name == "common_raise":
            into = vm["common"].at[sf:]
        loads[name] = pltpu.make_async_copy(hbm[name], into, load_sem.at[k])
    early = ("probe", "address", "content", "storage", "fade", "extra", "channel", "label")
    for name in early:
        loads[name].start()
    for name in names:
        if name not in early:
            loads[name].start()
    for name in early:
        loads[name].wait()

    row_i, col_i = iota((rows, rows), 0), iota((rows, rows), 1)
    eye = row_i == col_i
    lower, strict = row_i >= col_i, row_i > col_i
    same_block = (row_i < BLOCK) == (col_i < BLOCK)

    def to_col(row):
        return jnp.sum(jnp.where(eye, row, 0.0), axis=1, keepdims=True)

    def to_row(col):
        return jnp.sum(jnp.where(eye, col, 0.0), axis=0, keepdims=True)

    queries = vm["probe"][...].astype(F32)
    keys = vm["address"][...].astype(F32)
    values = vm["content"][...].astype(F32)
    q_unit = queries * lax.rsqrt(
        jnp.sum(queries * queries, -1, keepdims=True) + 1e-06
    ) * queries.shape[-1] ** (-0.5)
    k_unit = keys * lax.rsqrt(jnp.sum(keys * keys, -1, keepdims=True) + 1e-06)
    gate = to_col(1.0 / (1.0 + jnp.exp(-vm["storage"][...])))
    fade = vm["fade"][...]
    softplus = jnp.maximum(fade, 0.0) + jnp.log(1.0 + jnp.exp(-jnp.abs(fade)))
    rate = jnp.exp(vm["channel"][...])
    decay = vm["extra"][...] - rate * softplus
    c_col = jnp.sum(jnp.where(lower, decay, 0.0), axis=1, keepdims=True)
    c_row = to_row(c_col)
    label_row = vm["label"][...].astype(F32)
    label_col = to_col(label_row)
    label_first, label_last = label_row[:, :1], label_row[:, rows - 1 :]
    c_last = c_row[:, rows - 1 :]
    reach = jnp.where(
        lower & (label_col == label_row), jnp.exp(jnp.where(lower, c_col - c_row, 0.0)), 0.0
    )
    weighted = k_unit * gate
    coupling = jnp.where(strict, mm_nt(weighted, k_unit) * reach, 0.0)
    power = jnp.where(same_block, coupling, 0.0)
    across = jnp.where(same_block, 0.0, coupling)
    inverse = jnp.where(eye, 1.0, 0.0) - power
    for _ in range(BLOCK.bit_length() - 2):
        power = mm(power, power)
        inverse = inverse + mm(inverse, power)
    inverse = inverse - mm(inverse, mm(across, inverse))
    growth = jnp.exp(c_col) * (label_col == label_first).astype(F32)
    both = mm(inverse, jnp.concatenate([weighted * growth, values * gate], axis=1))
    tail_keys = k_unit * (jnp.exp(c_last - c_col) * (label_col == label_last).astype(F32))
    ends = mm_tn(tail_keys, both)
    end_growth = jnp.exp(c_last) * (label_last == label_first).astype(F32)
    scores = mm_nt(q_unit, k_unit) * reach
    outs = mm(scores, both)
    width = q_unit.shape[-1]
    q_grown = q_unit * growth - outs[:, :width]
    own_mixed = outs[:, width:]
    state_map = (jnp.where(eye, end_growth, 0.0) - ends[:, :width]).astype(BF16)
    shift = ends[:, width:]
    marks_at = width + 16
    pay[0:width, :] = shift.astype(BF16)
    pay[width : width + 8, :] = jnp.broadcast_to(label_first, (8, width)).astype(BF16)
    pay[width + 8 : marks_at, :] = jnp.broadcast_to(label_last, (8, width)).astype(BF16)
    pay[marks_at:, :] = state_map
    pl.semaphore_wait(barrier, n_sp + n_tp - 2)
    tops = [pay.shape[0]] * (REACH - 1) + [marks_at]
    first = [
        remote(
            pay.at[0:top], pieces.at[k, 0:top], pa_s.at[k], pa_r.at[k],
            at_sp(lax.rem(s + k + 1, n_sp)),
        )
        for k, top in enumerate(tops)
    ]
    for k in reversed(range(REACH)):
        first[k].start()

    for name in names:
        if name not in early:
            loads[name].wait()
    pick0, pick1 = vm["picks"][0:1, :], vm["picks"][1:2, :]
    share = vm["share"][...].astype(F32)
    expert_i = iota((experts, rows), 0)
    to0, to1 = (expert_i == pick0).astype(F32), (expert_i == pick1).astype(F32)
    chosen = to0 + to1
    rank = mm(chosen, (row_i < col_i).astype(F32))
    coded = jnp.where(chosen > 0.0, rank + 1.0, 0.0)
    shares = to0 * share[0:1, :] + to1 * share[1:2, :]
    slot_i = iota((padded, experts), 0)
    from_e = iota((padded, experts), 1) * stride
    spread = ((slot_i >= from_e) & (slot_i < from_e + stride)).astype(F32)
    place = iota((n_sp, stride, rows), 1).reshape(padded, rows)
    wide = mm(spread, jnp.concatenate([coded, shares, to0], axis=1))
    hot = wide[:, :rows] == (place + 1).astype(F32)
    dispatch = hot.astype(BF16)
    undo[...] = hot.astype(F32).T.astype(BF16)
    slot_share = jnp.sum(jnp.where(hot, wide[:, rows : 2 * rows], 0.0), axis=1, keepdims=True)
    slot_first = jnp.sum(jnp.where(hot, wide[:, 2 * rows :], 0.0), axis=1, keepdims=True)
    here = (iota((padded, rows), 1) == place).astype(F32)

    def per_slot(column):
        return jnp.sum((here * column).reshape(n_sp, stride, rows), axis=1, keepdims=True)

    told[...] = jnp.zeros_like(told)
    told[:, 0:1, :] = per_slot(slot_share).astype(BF16)
    told[:, 1:2, :] = per_slot(slot_first).astype(BF16)
    compact_i = iota((slots, padded), 0).astype(F32)
    source = jnp.floor((compact_i + 0.5) * (1.0 / cap))
    within = compact_i - source * cap
    column = iota((slots, padded), 1).astype(F32)
    compact = (column == source * stride + within).astype(BF16)
    open_i = iota((padded, slots), 1).astype(F32)
    open_source = jnp.floor((open_i + 0.5) * (1.0 / cap))
    spread_out = (
        iota((padded, slots), 0).astype(F32) == open_source * (stride - cap) + open_i
    ).astype(BF16)
    widen[...] = spread_out
    slot_lane = iota((slots, rows), 1).astype(F32) == within[:, :rows]
    valve = silu(vm["exit"][...].astype(F32))

    for k in range(REACH):
        first[k].wait_recv()

    def piece(k):
        label = pieces[k, width:marks_at, :].astype(F32)
        return pieces[k, 0:width, :], label[0:1, :], label[8:9, :]

    shift1, first1, last1 = piece(0)
    shift2, first2, last2 = piece(1)
    shift3, _, last3 = piece(2)
    map1 = pieces[0, marks_at:, :] * (first1 == last2).astype(BF16)
    map2 = pieces[1, marks_at:, :] * (first2 == last3).astype(BF16)
    joined = (label_first == last1).astype(F32)
    shift12 = shift1.astype(F32) + mm(map1, shift2)
    map12 = mm(map1, map2).astype(BF16)
    entering = (shift12 + mm(map12, shift3)) * joined
    carry_out[...] = (shift + mm(state_map, entering)).astype(BF16)
    second = remote(
        carry_out, carry_in, pb_s.at[0], pb_s.at[1], at_sp(lax.rem(s + REACH, n_sp))
    )
    second.start()
    from_carry = mm(q_grown, map12).astype(BF16)
    known = own_mixed + mm(q_grown, shift12) * joined
    second.wait_recv()
    mixed = known + mm(from_carry, carry_in[...]) * joined
    scaled = mixed * lax.rsqrt(jnp.mean(mixed * mixed, -1, keepdims=True) + 1e-06)
    heads_out = (scaled * valve).astype(BF16)

    def along(d):
        return lax.rem(y + d + 2 * ny, ny)

    def sigma_of(q):
        return 1 if q % 2 == 0 else -1

    soon, rest = (3, -3, 4), (1, -1, 2, -2, 0)

    class TpSum:
        def __init__(self, part, pair, send, recv, near_r, far_r, gone, chunk_rows):
            self.part, self.pair, self.send, self.recv = part, pair, send, recv
            self.near_r, self.far_r, self.gone, self.rows = near_r, far_r, gone, chunk_rows

        def at(self, q):
            return slice(q * self.rows, (q + 1) * self.rows)

        def put(self, d, at_rows, product):
            chip = along(d)
            self.part[chip, 0, at_rows] = product[:, :width].astype(BF16)
            self.part[chip, 1, at_rows] = product[:, width:].astype(BF16)

        def near(self, q, g):
            for d in (soon, rest)[g]:
                chip = along(d)
                remote(
                    self.part.at[chip, other, self.at(q)], self.pair.at[chip, self.at(q)],
                    self.gone.at[0], self.near_r.at[2 * q + g], at_tp(2 * y + other),
                ).start()

        def near_wait(self, q, g):
            there = self.pair.at[0 : len((soon, rest)[g]), self.at(q)]
            sem = self.near_r.at[2 * q + g]
            remote(there, there, sem, sem, at_tp(t)).wait_recv()

        def chip_sum(self, d, q):
            chip = along(d)
            mine = self.part[chip, c, self.at(q)].astype(F32)
            return mine + self.pair[chip, self.at(q)].astype(F32)

        def copy(self, line, q, to):
            return remote(
                self.send.at[line, self.at(q)], self.recv.at[line, self.at(q)], self.gone.at[1],
                self.far_r.at[(line > 2) * CHUNKS + q], at_tp(2 * along(to) + c),
            )

        def go(self, line, q, to, value):
            self.send[line, self.at(q)] = value.astype(BF16)
            self.copy(line, q, to).start()

        def got_all(self, first, last, q):
            there = self.recv.at[first:last, self.at(q)]
            sem = self.far_r.at[(first > 2) * CHUNKS + q]
            remote(there, there, sem, sem, at_tp(t)).wait_recv()

        def got(self, line, q):
            return self.recv[line, self.at(q)].astype(F32)

        def leg1(self, q):
            self.near_wait(q, 0)
            self.go(2, q, -2 * sigma_of(q), self.chip_sum(4, q))
            for i, sigma in enumerate((1, -1)):
                self.go(i, q, -sigma, self.chip_sum(-3 * sigma, q))

        def neighbours(self, q):
            self.near_wait(q, 1)
            for i, sigma in enumerate((1, -1)):
                self.go(3 + i, q, sigma, self.chip_sum(sigma, q))

        def leg2(self, q):
            self.got_all(0, 3, q)
            for i, sigma in enumerate((1, -1)):
                value = self.chip_sum(-2 * sigma, q) + self.got(i, q)
                if sigma == sigma_of(q):
                    value = value + self.got(2, q)
                self.go(5 + i, q, -2 * sigma, value)

        def total(self, q):
            value = self.chip_sum(0, q)
            self.got_all(3, 7, q)
            for line in (3, 4, 5, 6):
                value = value + self.got(line, q)
            return value

        def all_gone(self):
            there = self.part.at[:, 0]
            remote(there, there, self.gone.at[0], self.gone.at[0], at_tp(t)).wait_send()
            remote(
                self.send, self.send, self.gone.at[1], self.gone.at[1], at_tp(t)
            ).wait_send()

    def tell(stat, sems, line):
        stat[t] = line
        for k in sorted(range(1, n_tp), key=lambda k: -min(k, n_tp - k)):
            to = lax.rem(t + k, n_tp)
            remote(stat.at[t], stat.at[t], sems.at[0], sems.at[1], at_tp(to)).start()

    def heard_all(stat, sems):
        there = stat.at[1:n_tp]
        remote(there, there, sems.at[0], sems.at[1], at_tp(t)).wait()
        return jnp.sum(stat[...], axis=0)

    scaled_in = ALPHA * vm["incoming"][...].astype(F32)
    row_sum = jnp.sum(scaled_in, -1, keepdims=True)
    first_tp = TpSum(part1, pair1, send1, recv1, near1_r, far1_r, gone1_s, rows // CHUNKS)
    for g, group in enumerate((soon, rest)):
        for d in group:
            at = pl.ds(pl.multiple_of(along(d) * 2 * width, 2 * width), 2 * width)
            product = mm(heads_out, vm["final"][:, at])
            first_tp.put(d, slice(0, rows), product)
            row_sum = row_sum + jnp.sum(product, -1, keepdims=True)
        for q in range(CHUNKS):
            first_tp.near(q, g)
    for q in range(CHUNKS):
        first_tp.leg1(q)
    tell(stat0, mean_s, to_row(row_sum))
    for q in range(CHUNKS):
        first_tp.neighbours(q)
    for q in range(CHUNKS):
        first_tp.leg2(q)
    projected = jnp.concatenate([first_tp.total(q) for q in range(CHUNKS)], axis=0)
    features = width * n_tp
    mean = to_col(heard_all(stat0, mean_s) / features)
    centred = scaled_in + projected - mean

    sent_rows = -(-cap // 2) * 2

    def scattered(src, dst, sems, to):
        top = min(src.shape[1], sent_rows)
        return remote(
            src.at[to, 0:top], dst.at[s, 0:top], sems.at[0], sems.at[1], at_sp(to)
        )

    def scatter(src, dst, sems):
        for dz, dx in hops:
            scattered(src, dst, sems, beside(dz, dx)).start()
        dst[s] = src[s]

    def collected(dst, sems):
        top = min(dst.shape[1], sent_rows)
        there = dst.at[1:n_sp, 0:top]
        remote(there, there, sems.at[0], sems.at[1], at_sp(s)).wait()
        return as_rows(dst[...], top)

    def as_rows(came, top):
        shape = came.shape
        came = jnp.where(iota(shape, 1) < top, came.astype(F32), 0.0).astype(BF16)
        return came.reshape(shape[0] * shape[1], shape[2])

    gained = (centred * vm["gain1"][...]).astype(BF16)
    payload = jnp.dot(dispatch, gained, preferred_element_type=F32)
    sent[...] = payload.astype(BF16).reshape(n_sp, stride, rows)
    scatter(sent, arrived, dis_s)
    tell(stat1, sq1_s, to_row(jnp.sum(centred * centred, -1, keepdims=True)))
    came = collected(arrived, dis_s)
    lanes = pl.ds(pl.multiple_of(c * width, width), width)
    piece_rows = slots // CHUNKS

    def rows_of(q):
        return slice(q * piece_rows, (q + 1) * piece_rows)

    def block(chip, q):
        return gathered.at[chip, rows_of(q), lanes]

    chips_of = ((0,), (2, -2), (1, -1), (3, -3, 4))

    def passed(d, q, to, late):
        there = block(along(d), q)
        sem = wire_r.at[late * CHUNKS + q]
        remote(there, there, gone_s.at[1], sem, at_tp(2 * along(to) + c)).start()

    def hand(k, q):
        for d in chips_of[k]:
            there = block(along(d), q)
            remote(
                there, there, gone_s.at[0], own_r.at[k * CHUNKS + q], at_tp(2 * y + other)
            ).start()

    def wait_bytes(count, sem):
        there = pair2.at[0:count, 0:piece_rows]
        remote(there, there, sem, sem, at_tp(t)).wait_recv()

    def absorb(k, q):
        chips, at_rows = [along(d) for d in chips_of[k]], rows_of(q)
        wait_bytes(len(chips), own_r.at[k * CHUNKS + q])
        gates = ups = common = 0.0
        for chip in chips:
            block_in = gathered[chip, at_rows, :]
            at = pl.ds(pl.multiple_of(chip * 2 * width, 2 * width), 2 * width)
            gates += jnp.dot(block_in, vm["valve"][at, :], preferred_element_type=F32)
            ups += jnp.dot(block_in, vm["raise"][at, :], preferred_element_type=F32)
            common += lax.dot_general(
                block_in, vm["common"][:, at], (((1,), (1,)), ((), ())), preferred_element_type=F32
            )
        if k:
            gates, ups = gates + acc_g[0, at_rows], ups + acc_g[1, at_rows]
            common = common + acc_s[at_rows]
        if k < 3:
            acc_g[0, at_rows], acc_g[1, at_rows], acc_s[at_rows] = gates, ups, common
        return gates, ups, common

    def all_noted():
        notes = collected(heard, note_s)
        note_column = iota((slots, notes.shape[0]), 1).astype(F32)
        note_source = source[:, :1] * told.shape[1]

        def noted(j):
            line = (note_column == note_source + j).astype(BF16)
            found = jnp.dot(line, notes, preferred_element_type=F32)
            return jnp.sum(jnp.where(slot_lane, found, 0.0), axis=1, keepdims=True)

        return noted(0), noted(1), noted(2) + noted(3)

    for q in range(CHUNKS):
        found = jnp.dot(compact[rows_of(q)], came, preferred_element_type=F32)
        gathered[y, rows_of(q), lanes] = found.astype(BF16)
        for sigma in (1, -1):
            passed(0, q, 2 * sigma, 0)
    for q in range(CHUNKS):
        for sigma in (1, -1):
            passed(0, q, sigma, 1)
    for q in range(CHUNKS):
        hand(0, q)
    row_scale = lax.rsqrt(heard_all(stat1, sq1_s) / features + 1e-05)
    slot_scale = jnp.sum(jnp.where(hot, row_scale, 0.0), axis=1, keepdims=True)
    scales = per_slot(slot_scale)
    coarse = scales.astype(BF16)
    told[:, 2:3, :] = coarse
    told[:, 3:4, :] = (scales - coarse.astype(F32)).astype(BF16)
    scatter(told, heard, note_s)
    middle = (centred * to_col(row_scale) * vm["gain1"][...]).astype(BF16)
    for q in range(CHUNKS):
        wait_bytes(2, wire_r.at[q])
        for sigma in (1, -1):
            if sigma == sigma_of(q):
                passed(-2 * sigma, q, 2 * sigma, 2)
            passed(-2 * sigma, q, sigma, 2)
        hand(1, q)
    for q in range(CHUNKS):
        absorb(0, q)
    for q in range(CHUNKS):
        wait_bytes(2, wire_r.at[CHUNKS + q])
        hand(2, q)
    for q in range(CHUNKS):
        absorb(1, q)
    slot_notes = all_noted()
    for q in range(CHUNKS):
        wait_bytes(3, wire_r.at[2 * CHUNKS + q])
        hand(3, q)
        if q == 0:
            for k in range(CHUNKS):
                absorb(2, k)

    def expert(q, gates, ups, common):
        at_rows = rows_of(q)
        weight, flag, scale = (v[at_rows] for v in slot_notes)
        hidden = (silu(gates * scale) * ups * (scale * weight)).astype(BF16)
        common = common * scale
        shared = (silu(common[:, :sf]) * common[:, sf:] * flag).astype(BF16)
        for g, group in enumerate((soon, rest)):
            for d in group:
                at = pl.ds(pl.multiple_of(along(d) * 2 * width, 2 * width), 2 * width)
                product = jnp.dot(hidden, vm["lower"][:, at], preferred_element_type=F32) + jnp.dot(
                    shared, vm["common_low"][:, at], preferred_element_type=F32
                )
                second_tp.put(d, at_rows, product)
            second_tp.near(q, g)

    second_tp = TpSum(part2, pair2, send2, recv2, near2_r, far2_r, gone2_s, piece_rows)
    expert(0, *absorb(3, 0))
    for q in range(1, CHUNKS):
        ready = absorb(3, q)
        second_tp.leg1(q - 1)
        expert(q, *ready)
    second_tp.leg1(CHUNKS - 1)
    for q in range(CHUNKS):
        second_tp.neighbours(q)
    for q in range(CHUNKS):
        second_tp.leg2(q)
    for q in range(CHUNKS):
        value = second_tp.total(q)
        share_sp = n_sp // CHUNKS
        owners = slice(q * share_sp, (q + 1) * share_sp)
        spots = slice(q * share_sp * stride, (q + 1) * share_sp * stride)
        rsend[owners] = (
            mm(widen[spots, rows_of(q)], value)
            .astype(BF16)
            .reshape(share_sp, stride, rows)
        )
        for k in range(share_sp):
            to = q * share_sp + lax.rem(s + k, share_sp)

            @pl.when(to != s)
            def _(to=to):
                scattered(rsend, returned, ret_s, to).start()

    returned[s] = rsend[s]
    back = collected(returned, ret_s)
    mixture = mm(undo[...], back)
    second_sum = ALPHA * middle.astype(F32) + mixture
    sums = [jnp.sum(v, -1, keepdims=True) for v in (second_sum, second_sum * second_sum)]
    tell(stat2, sq2_s, jnp.concatenate([to_row(v) for v in sums], axis=0))
    totals = heard_all(stat2, sq2_s) / features
    mean2, square2 = totals[0:1, :], totals[1:2, :]
    scale2 = lax.rsqrt(square2 - mean2 * mean2 + 1e-05)
    out_ref[...] = (
        (second_sum - to_col(mean2)) * to_col(scale2) * vm["gain2"][...]
    ).astype(BF16)

    for copy in first:
        copy.wait_send()
    second.wait_send()
    def all_gone(there, sem):
        remote(there, there, sem, sem, at_tp(t)).wait_send()

    all_gone(pair2, gone_s.at[0])
    all_gone(pair2.at[1:ny], gone_s.at[1])
    first_tp.all_gone()
    second_tp.all_gone()


def dims_names():
    return (
        "probe", "address", "content", "storage", "fade", "extra", "label",
        "picks", "share", "exit", "incoming", "gain1", "gain2", "final",
        "valve", "raise", "lower", "common", "common_raise", "common_low", "channel",
    )


def shards(
    probe, address, content, storage, fade, channel, extra, label, exit_valve, final,
    incoming, gain1, picks, share, valve, raising, lowering, common_valve, common_raising,
    common_lowering, gain2,
):
    n_sp, n_tp = lax.axis_size("sp"), lax.axis_size("tp")
    ny = n_tp // 2
    rows, width = probe.shape
    experts = n_sp * valve.shape[0]
    cap = max(2, 9 * rows * picks.shape[1] // (8 * experts))
    stride = -(-(cap + 2) // 16) * 16
    slots = n_sp * cap
    ff, features = valve.shape[2], valve.shape[1]
    sf = common_valve.shape[1]
    dims = (n_sp, n_tp, rows, experts, cap, stride)
    args = {
        "probe": probe, "address": address, "content": content, "storage": storage,
        "fade": fade, "extra": extra, "label": label[None, :], "picks": picks.T,
        "share": share.T, "exit": exit_valve, "incoming": incoming, "gain1": gain1[None, :],
        "gain2": gain2[None, :], "final": final, "valve": valve[0], "raise": raising[0],
        "lower": lowering[0],
        "common": common_valve.T, "common_raise": common_raising.T,
        "common_low": common_lowering, "channel": channel[None, :],
    }
    names = dims_names()
    operands = [
        args[n] if n == "channel" else pltpu.with_memory_space_constraint(args[n], pltpu.HBM)
        for n in names
    ]
    dma = pltpu.SemaphoreType.DMA
    shapes = {n: a.shape for n, a in args.items()}
    shapes["common"] = (2 * sf, features)
    shapes["common_raise"] = (8, 128)
    own = [pltpu.VMEM(shapes[n], args[n].dtype) for n in names]

    def vmem(*shape, kind=BF16):
        return pltpu.VMEM(shape, kind)

    return pl.pallas_call(
        functools.partial(kernel, dims),
        out_shape=jax.ShapeDtypeStruct((rows, width), BF16),
        in_specs=[pl.BlockSpec(memory_space=pltpu.HBM)] * len(operands),
        out_specs=pl.BlockSpec(memory_space=pltpu.VMEM),
        scratch_shapes=own
        + [
            vmem(2 * width + 16, width), vmem(REACH, 2 * width + 16, width),
            vmem(width, width), vmem(width, width),
            vmem(ny, 2, rows, width), vmem(ny, rows, width), vmem(7, rows, width),
            vmem(7, rows, width),
            vmem(n_tp, 1, rows, kind=F32), vmem(n_tp, 1, rows, kind=F32),
            vmem(n_tp, 2, rows, kind=F32),
            vmem(n_sp, stride, width), vmem(n_sp, stride, width),
            vmem(n_sp, 8, width), vmem(n_sp, 8, width),
            vmem(ny, slots, 2 * width), vmem(2, slots, ff, kind=F32), vmem(slots, 2 * sf, kind=F32),
            vmem(ny, 2, slots, width), vmem(ny, slots, width), vmem(7, slots, width),
            vmem(7, slots, width),
            vmem(n_sp, stride, width), vmem(n_sp, stride, width),
            vmem(rows, n_sp * stride), vmem(n_sp * stride, slots),
            dma((len(operands),)), dma((REACH,)), dma((REACH,)), dma((2,)),
            dma((2 * CHUNKS,)), dma((2 * CHUNKS,)), dma((2,)), dma((2,)), dma((2,)), dma((2,)),
            dma((2,)), dma((2,)), dma((2,)), dma((3 * CHUNKS,)), dma((4 * CHUNKS,)),
            dma((2,)), dma((2 * CHUNKS,)), dma((2 * CHUNKS,)), dma((2,)),
        ],
        compiler_params=pltpu.CompilerParams(
            collective_id=0, has_side_effects=True, vmem_limit_bytes=48 * 1024 * 1024
        ),
        name="layer",
    )(*operands)


def solution(mesh):
    return jax.shard_map(
        shards,
        mesh=mesh,
        in_specs=(
            P("sp", "tp"), P("sp", "tp"), P("sp", "tp"), P("tp", "sp"), P("tp", "sp"), P("tp"),
            P("tp", "sp"), P("sp"), P("sp", "tp"), P("tp", None), P("sp", "tp"), P("tp"),
            P("sp", None), P("sp", None), P("sp", None, "tp"), P("sp", None, "tp"),
            P("sp", "tp", None), P(None, "tp"), P(None, "tp"), P("tp", None), P("tp"),
        ),
        out_specs=P("sp", "tp"),
        check_vma=False,
    )
```

```python
import functools

import jax
import jax.numpy as jnp
from jax import lax
from jax.experimental import pallas as pl
from jax.experimental.pallas import tpu as pltpu
from jax.sharding import PartitionSpec as P

BLOCK = 64
ALPHA = 2.0**0.25
F32 = jnp.float32
BF16 = jnp.bfloat16
MESH = pl.DeviceIdType.MESH
REACH = 3
CHUNKS = 2


def iota(shape, dim):
    return lax.broadcasted_iota(jnp.int32, shape, dim)


def mm(a, b):
    return jnp.dot(a.astype(BF16), b.astype(BF16), preferred_element_type=F32)


def mm_nt(a, b):
    return lax.dot_general(
        a.astype(BF16), b.astype(BF16), (((1,), (1,)), ((), ())), preferred_element_type=F32
    )


def mm_tn(a, b):
    return lax.dot_general(
        a.astype(BF16), b.astype(BF16), (((0,), (0,)), ((), ())), preferred_element_type=F32
    )


def silu(v):
    return v / (1.0 + jnp.exp(-v))


def kernel(dims, *refs):
    n_sp, n_tp, rows, experts, cap, stride = dims
    ny = n_tp // 2
    slots = n_sp * cap
    padded = n_sp * stride
    names = dims_names()
    hbm = dict(zip(names, refs[: len(names)]))
    out_ref = refs[len(names)]
    scratch = refs[len(names) + 1 :]
    vm = dict(zip(names, scratch[: len(names)]))
    (
        pay, pieces, carry_out, carry_in,
        part1, pair1, send1, recv1,
        stat0, stat1, stat2,
        sent, arrived, told, heard, gathered, acc_g, acc_s,
        part2, pair2, send2, recv2,
        rsend, returned, undo, widen,
        load_sem, pa_s, pa_r, pb_s,
        near1_r, far1_r, gone1_s, mean_s, sq1_s, sq2_s,
        dis_s, note_s, ret_s, wire_r, own_r, gone_s,
        near2_r, far2_r, gone2_s,
    ) = scratch[len(names) :]

    s = lax.axis_index("sp")
    t = lax.axis_index("tp")
    y = t // 2
    c = lax.rem(t, 2)
    other = 1 - c

    def at_sp(k):
        return {"sp": k, "tp": t}

    def at_tp(k):
        return {"sp": s, "tp": k}

    def remote(src, dst, send_sem, recv_sem, device):
        return pltpu.make_async_remote_copy(
            src_ref=src, dst_ref=dst, send_sem=send_sem, recv_sem=recv_sem,
            device_id=device, device_id_type=MESH,
        )

    barrier = pltpu.get_barrier_semaphore()

    nx = 4
    nz = n_sp // nx
    hops = sorted(
        ((dz, dx) for dz in range(nz) for dx in range(nx) if dz or dx),
        key=lambda d: -min(d[0], nz - d[0]) - min(d[1], nx - d[1]),
    )
    z, x = s // nx, lax.rem(s, nx)

    def beside(dz, dx):
        return lax.rem(z + dz, nz) * nx + lax.rem(x + dx, nx)

    sf = vm["common"].shape[0] // 2
    loads = {}
    for k, name in enumerate(names):
        into = vm[name]
        if name == "common":
            into = vm["common"].at[0:sf]
        if name == "common_raise":
            into = vm["common"].at[sf:]
        loads[name] = pltpu.make_async_copy(hbm[name], into, load_sem.at[k])
    early = ("probe", "address", "content", "storage", "fade", "extra", "channel", "label")
    for name in early:
        loads[name].start()
    for dz, dx in hops:
        pl.semaphore_signal(
            barrier, inc=1, device_id=at_sp(beside(dz, dx)), device_id_type=MESH
        )
    for k in sorted(range(1, n_tp), key=lambda k: -min(k, n_tp - k)):
        pl.semaphore_signal(
            barrier, inc=1, device_id=at_tp(lax.rem(t + k, n_tp)), device_id_type=MESH
        )
    for name in names:
        if name not in early:
            loads[name].start()
    for name in early:
        loads[name].wait()

    row_i, col_i = iota((rows, rows), 0), iota((rows, rows), 1)
    eye = row_i == col_i
    lower, strict = row_i >= col_i, row_i > col_i
    same_block = (row_i < BLOCK) == (col_i < BLOCK)

    def to_col(row):
        return jnp.sum(jnp.where(eye, row, 0.0), axis=1, keepdims=True)

    def to_row(col):
        return jnp.sum(jnp.where(eye, col, 0.0), axis=0, keepdims=True)

    queries = vm["probe"][...].astype(F32)
    keys = vm["address"][...].astype(F32)
    values = vm["content"][...].astype(F32)
    q_unit = queries * lax.rsqrt(
        jnp.sum(queries * queries, -1, keepdims=True) + 1e-06
    ) * queries.shape[-1] ** (-0.5)
    k_unit = keys * lax.rsqrt(jnp.sum(keys * keys, -1, keepdims=True) + 1e-06)
    gate = to_col(1.0 / (1.0 + jnp.exp(-vm["storage"][...])))
    fade = vm["fade"][...]
    softplus = jnp.maximum(fade, 0.0) + jnp.log(1.0 + jnp.exp(-jnp.abs(fade)))
    rate = jnp.exp(vm["channel"][...])
    decay = vm["extra"][...] - rate * softplus
    c_col = jnp.sum(jnp.where(lower, decay, 0.0), axis=1, keepdims=True)
    c_row = to_row(c_col)
    label_row = vm["label"][...].astype(F32)
    label_col = to_col(label_row)
    label_first, label_last = label_row[:, :1], label_row[:, rows - 1 :]
    c_last = c_row[:, rows - 1 :]
    reach = jnp.where(
        lower & (label_col == label_row), jnp.exp(jnp.where(lower, c_col - c_row, 0.0)), 0.0
    )
    weighted = k_unit * gate
    coupling = jnp.where(strict, mm_nt(weighted, k_unit) * reach, 0.0)
    power = jnp.where(same_block, coupling, 0.0)
    across = jnp.where(same_block, 0.0, coupling)
    inverse = jnp.where(eye, 1.0, 0.0) - power
    for _ in range(BLOCK.bit_length() - 2):
        power = mm(power, power)
        inverse = inverse + mm(inverse, power)
    inverse = inverse - mm(inverse, mm(across, inverse))
    growth = jnp.exp(c_col) * (label_col == label_first).astype(F32)
    both = mm(inverse, jnp.concatenate([weighted * growth, values * gate], axis=1))
    tail_keys = k_unit * (jnp.exp(c_last - c_col) * (label_col == label_last).astype(F32))
    ends = mm_tn(tail_keys, both)
    end_growth = jnp.exp(c_last) * (label_last == label_first).astype(F32)
    scores = mm_nt(q_unit, k_unit) * reach
    outs = mm(scores, both)
    width = q_unit.shape[-1]
    q_grown = q_unit * growth - outs[:, :width]
    own_mixed = outs[:, width:]
    state_map = (jnp.where(eye, end_growth, 0.0) - ends[:, :width]).astype(BF16)
    shift = ends[:, width:]
    marks_at = width + 16
    pay[0:width, :] = shift.astype(BF16)
    pay[width : width + 8, :] = jnp.broadcast_to(label_first, (8, width)).astype(BF16)
    pay[width + 8 : marks_at, :] = jnp.broadcast_to(label_last, (8, width)).astype(BF16)
    pay[marks_at:, :] = state_map
    pl.semaphore_wait(barrier, n_sp + n_tp - 2)
    tops = [pay.shape[0]] * (REACH - 1) + [marks_at]
    first = [
        remote(
            pay.at[0:top], pieces.at[k, 0:top], pa_s.at[k], pa_r.at[k],
            at_sp(lax.rem(s + k + 1, n_sp)),
        )
        for k, top in enumerate(tops)
    ]
    for k in (1, 2, 0):
        first[k].start()

    for name in names:
        if name not in early:
            loads[name].wait()
    pick0, pick1 = vm["picks"][0:1, :], vm["picks"][1:2, :]
    share = vm["share"][...].astype(F32)
    expert_i = iota((experts, rows), 0)
    to0, to1 = (expert_i == pick0).astype(F32), (expert_i == pick1).astype(F32)
    chosen = to0 + to1
    rank = mm(chosen, (row_i < col_i).astype(F32))
    coded = jnp.where(chosen > 0.0, rank + 1.0, 0.0)
    shares = to0 * share[0:1, :] + to1 * share[1:2, :]
    slot_i = iota((padded, experts), 0)
    from_e = iota((padded, experts), 1) * stride
    spread = ((slot_i >= from_e) & (slot_i < from_e + stride)).astype(F32)
    place = iota((n_sp, stride, rows), 1).reshape(padded, rows)
    wide = mm(spread, jnp.concatenate([coded, shares, to0], axis=1))
    hot = wide[:, :rows] == (place + 1).astype(F32)
    dispatch = hot.astype(BF16)
    undo[...] = hot.astype(F32).T.astype(BF16)
    slot_share = jnp.sum(jnp.where(hot, wide[:, rows : 2 * rows], 0.0), axis=1, keepdims=True)
    slot_first = jnp.sum(jnp.where(hot, wide[:, 2 * rows :], 0.0), axis=1, keepdims=True)
    here = (iota((padded, rows), 1) == place).astype(F32)

    def per_slot(column):
        return jnp.sum((here * column).reshape(n_sp, stride, rows), axis=1, keepdims=True)

    told[...] = jnp.zeros_like(told)
    told[:, 0:1, :] = per_slot(slot_share).astype(BF16)
    told[:, 1:2, :] = per_slot(slot_first).astype(BF16)
    compact_i = iota((slots, padded), 0).astype(F32)
    source = jnp.floor((compact_i + 0.5) * (1.0 / cap))
    within = compact_i - source * cap
    column = iota((slots, padded), 1).astype(F32)
    compact = (column == source * stride + within).astype(BF16)
    open_i = iota((padded, slots), 1).astype(F32)
    open_source = jnp.floor((open_i + 0.5) * (1.0 / cap))
    spread_out = (
        iota((padded, slots), 0).astype(F32) == open_source * (stride - cap) + open_i
    ).astype(BF16)
    widen[...] = spread_out
    slot_lane = iota((slots, rows), 1).astype(F32) == within[:, :rows]
    valve = silu(vm["exit"][...].astype(F32))

    for k in range(REACH):
        first[k].wait_recv()

    def piece(k):
        label = pieces[k, width:marks_at, :].astype(F32)
        return pieces[k, 0:width, :], label[0:1, :], label[8:9, :]

    shift1, first1, last1 = piece(0)
    shift2, first2, last2 = piece(1)
    shift3, _, last3 = piece(2)
    map1 = pieces[0, marks_at:, :] * (first1 == last2).astype(BF16)
    map2 = pieces[1, marks_at:, :] * (first2 == last3).astype(BF16)
    joined = (label_first == last1).astype(F32)
    shift12 = shift1.astype(F32) + mm(map1, shift2)
    map12 = mm(map1, map2).astype(BF16)
    entering = (shift12 + mm(map12, shift3)) * joined
    carry_out[...] = (shift + mm(state_map, entering)).astype(BF16)
    second = remote(
        carry_out, carry_in, pb_s.at[0], pb_s.at[1], at_sp(lax.rem(s + REACH, n_sp))
    )
    second.start()
    from_carry = mm(q_grown, map12).astype(BF16)
    known = own_mixed + mm(q_grown, shift12) * joined
    second.wait_recv()
    mixed = known + mm(from_carry, carry_in[...]) * joined
    scaled = mixed * lax.rsqrt(jnp.mean(mixed * mixed, -1, keepdims=True) + 1e-06)
    heads_out = (scaled * valve).astype(BF16)

    def along(d):
        return lax.rem(y + d + 2 * ny, ny)

    def sigma_of(q):
        return 1 if q % 2 == 0 else -1

    soon, rest = (3, -3, 4), (1, -1, 2, -2, 0)

    class TpSum:
        def __init__(self, part, pair, send, recv, near_r, far_r, gone, chunk_rows):
            self.part, self.pair, self.send, self.recv = part, pair, send, recv
            self.near_r, self.far_r, self.gone, self.rows = near_r, far_r, gone, chunk_rows

        def at(self, q):
            return slice(q * self.rows, (q + 1) * self.rows)

        def put(self, d, at_rows, product):
            chip = along(d)
            self.part[chip, 0, at_rows] = product[:, :width].astype(BF16)
            self.part[chip, 1, at_rows] = product[:, width:].astype(BF16)

        def near(self, q, g):
            for d in (soon, rest)[g]:
                chip = along(d)
                remote(
                    self.part.at[chip, other, self.at(q)], self.pair.at[chip, self.at(q)],
                    self.gone.at[0], self.near_r.at[2 * q + g], at_tp(2 * y + other),
                ).start()

        def near_wait(self, q, g):
            there = self.pair.at[0 : len((soon, rest)[g]), self.at(q)]
            sem = self.near_r.at[2 * q + g]
            remote(there, there, sem, sem, at_tp(t)).wait_recv()

        def chip_sum(self, d, q):
            chip = along(d)
            mine = self.part[chip, c, self.at(q)].astype(F32)
            return mine + self.pair[chip, self.at(q)].astype(F32)

        def copy(self, line, q, to):
            return remote(
                self.send.at[line, self.at(q)], self.recv.at[line, self.at(q)], self.gone.at[1],
                self.far_r.at[(line > 2) * CHUNKS + q], at_tp(2 * along(to) + c),
            )

        def go(self, line, q, to, value):
            self.send[line, self.at(q)] = value.astype(BF16)
            self.copy(line, q, to).start()

        def got_all(self, first, last, q):
            there = self.recv.at[first:last, self.at(q)]
            sem = self.far_r.at[(first > 2) * CHUNKS + q]
            remote(there, there, sem, sem, at_tp(t)).wait_recv()

        def got(self, line, q):
            return self.recv[line, self.at(q)].astype(F32)

        def leg1(self, q):
            self.near_wait(q, 0)
            self.go(2, q, -2 * sigma_of(q), self.chip_sum(4, q))
            for i, sigma in enumerate((1, -1)):
                self.go(i, q, -sigma, self.chip_sum(-3 * sigma, q))

        def neighbours(self, q):
            self.near_wait(q, 1)
            for i, sigma in enumerate((1, -1)):
                self.go(3 + i, q, sigma, self.chip_sum(sigma, q))

        def leg2(self, q):
            self.got_all(0, 3, q)
            for i, sigma in enumerate((1, -1)):
                value = self.chip_sum(-2 * sigma, q) + self.got(i, q)
                if sigma == sigma_of(q):
                    value = value + self.got(2, q)
                self.go(5 + i, q, -2 * sigma, value)

        def total(self, q):
            value = self.chip_sum(0, q)
            self.got_all(3, 7, q)
            for line in (3, 4, 5, 6):
                value = value + self.got(line, q)
            return value

        def all_gone(self):
            there = self.part.at[:, 0]
            remote(there, there, self.gone.at[0], self.gone.at[0], at_tp(t)).wait_send()
            remote(
                self.send, self.send, self.gone.at[1], self.gone.at[1], at_tp(t)
            ).wait_send()

    def tell(stat, sems, line):
        stat[t] = line
        for k in sorted(range(1, n_tp), key=lambda k: -min(k, n_tp - k)):
            to = lax.rem(t + k, n_tp)
            remote(stat.at[t], stat.at[t], sems.at[0], sems.at[1], at_tp(to)).start()

    def heard_all(stat, sems):
        there = stat.at[1:n_tp]
        remote(there, there, sems.at[0], sems.at[1], at_tp(t)).wait()
        return jnp.sum(stat[...], axis=0)

    scaled_in = ALPHA * vm["incoming"][...].astype(F32)
    row_sum = jnp.sum(scaled_in, -1, keepdims=True)
    first_tp = TpSum(part1, pair1, send1, recv1, near1_r, far1_r, gone1_s, rows // CHUNKS)
    for g, group in enumerate((soon, rest)):
        for d in group:
            at = pl.ds(pl.multiple_of(along(d) * 2 * width, 2 * width), 2 * width)
            product = mm(heads_out, vm["final"][:, at])
            first_tp.put(d, slice(0, rows), product)
            row_sum = row_sum + jnp.sum(product, -1, keepdims=True)
        for q in range(CHUNKS):
            first_tp.near(q, g)
    for q in range(CHUNKS):
        first_tp.leg1(q)
    tell(stat0, mean_s, to_row(row_sum))
    for q in range(CHUNKS):
        first_tp.neighbours(q)
    for q in range(CHUNKS):
        first_tp.leg2(q)
    projected = jnp.concatenate([first_tp.total(q) for q in range(CHUNKS)], axis=0)
    features = width * n_tp
    mean = to_col(heard_all(stat0, mean_s) / features)
    centred = scaled_in + projected - mean

    sent_rows = -(-cap // 2) * 2

    def scattered(src, dst, sems, to):
        top = min(src.shape[1], sent_rows)
        return remote(
            src.at[to, 0:top], dst.at[s, 0:top], sems.at[0], sems.at[1], at_sp(to)
        )

    def scatter(src, dst, sems):
        for dz, dx in hops:
            scattered(src, dst, sems, beside(dz, dx)).start()
        dst[s] = src[s]

    def collected(dst, sems):
        top = min(dst.shape[1], sent_rows)
        there = dst.at[1:n_sp, 0:top]
        remote(there, there, sems.at[0], sems.at[1], at_sp(s)).wait()
        return as_rows(dst[...], top)

    def as_rows(came, top):
        shape = came.shape
        came = jnp.where(iota(shape, 1) < top, came.astype(F32), 0.0).astype(BF16)
        return came.reshape(shape[0] * shape[1], shape[2])

    gained = (centred * vm["gain1"][...]).astype(BF16)
    payload = jnp.dot(dispatch, gained, preferred_element_type=F32)
    sent[...] = payload.astype(BF16).reshape(n_sp, stride, rows)
    scatter(sent, arrived, dis_s)
    tell(stat1, sq1_s, to_row(jnp.sum(centred * centred, -1, keepdims=True)))
    came = collected(arrived, dis_s)
    lanes = pl.ds(pl.multiple_of(c * width, width), width)
    piece_rows = slots // CHUNKS

    def rows_of(q):
        return slice(q * piece_rows, (q + 1) * piece_rows)

    def block(chip, q):
        return gathered.at[chip, rows_of(q), lanes]

    chips_of = ((0,), (2, -2), (1, -1), (3, -3, 4))

    def passed(d, q, to, late):
        there = block(along(d), q)
        sem = wire_r.at[late * CHUNKS + q]
        remote(there, there, gone_s.at[1], sem, at_tp(2 * along(to) + c)).start()

    def hand(k, q):
        for d in chips_of[k]:
            there = block(along(d), q)
            remote(
                there, there, gone_s.at[0], own_r.at[k * CHUNKS + q], at_tp(2 * y + other)
            ).start()

    def wait_bytes(count, sem):
        there = pair2.at[0:count, 0:piece_rows]
        remote(there, there, sem, sem, at_tp(t)).wait_recv()

    def absorb(k, q):
        chips, at_rows = [along(d) for d in chips_of[k]], rows_of(q)
        wait_bytes(len(chips), own_r.at[k * CHUNKS + q])
        gates = ups = common = 0.0
        for chip in chips:
            block_in = gathered[chip, at_rows, :]
            at = pl.ds(pl.multiple_of(chip * 2 * width, 2 * width), 2 * width)
            gates += jnp.dot(block_in, vm["valve"][at, :], preferred_element_type=F32)
            ups += jnp.dot(block_in, vm["raise"][at, :], preferred_element_type=F32)
            common += lax.dot_general(
                block_in, vm["common"][:, at], (((1,), (1,)), ((), ())), preferred_element_type=F32
            )
        if k:
            gates, ups = gates + acc_g[0, at_rows], ups + acc_g[1, at_rows]
            common = common + acc_s[at_rows]
        if k < 3:
            acc_g[0, at_rows], acc_g[1, at_rows], acc_s[at_rows] = gates, ups, common
        return gates, ups, common

    def all_noted():
        notes = collected(heard, note_s)
        note_column = iota((slots, notes.shape[0]), 1).astype(F32)
        note_source = source[:, :1] * told.shape[1]

        def noted(j):
            line = (note_column == note_source + j).astype(BF16)
            found = jnp.dot(line, notes, preferred_element_type=F32)
            return jnp.sum(jnp.where(slot_lane, found, 0.0), axis=1, keepdims=True)

        return noted(0), noted(1), noted(2) + noted(3)

    for q in range(CHUNKS):
        found = jnp.dot(compact[rows_of(q)], came, preferred_element_type=F32)
        gathered[y, rows_of(q), lanes] = found.astype(BF16)
        for sigma in (1, -1):
            passed(0, q, 2 * sigma, 0)
    for q in range(CHUNKS):
        for sigma in (1, -1):
            passed(0, q, sigma, 1)
    for q in range(CHUNKS):
        hand(0, q)
    row_scale = lax.rsqrt(heard_all(stat1, sq1_s) / features + 1e-05)
    slot_scale = jnp.sum(jnp.where(hot, row_scale, 0.0), axis=1, keepdims=True)
    scales = per_slot(slot_scale)
    coarse = scales.astype(BF16)
    told[:, 2:3, :] = coarse
    told[:, 3:4, :] = (scales - coarse.astype(F32)).astype(BF16)
    scatter(told, heard, note_s)
    middle = (centred * to_col(row_scale) * vm["gain1"][...]).astype(BF16)
    for q in range(CHUNKS):
        wait_bytes(2, wire_r.at[q])
        for sigma in (1, -1):
            if sigma == sigma_of(q):
                passed(-2 * sigma, q, 2 * sigma, 2)
            passed(-2 * sigma, q, sigma, 2)
        hand(1, q)
    for q in range(CHUNKS):
        absorb(0, q)
    for q in range(CHUNKS):
        wait_bytes(2, wire_r.at[CHUNKS + q])
        hand(2, q)
    for q in range(CHUNKS):
        absorb(1, q)
    slot_notes = all_noted()
    for q in range(CHUNKS):
        wait_bytes(3, wire_r.at[2 * CHUNKS + q])
        hand(3, q)
        if q == 0:
            for k in range(CHUNKS):
                absorb(2, k)

    def expert(q, gates, ups, common):
        at_rows = rows_of(q)
        weight, flag, scale = (v[at_rows] for v in slot_notes)
        hidden = (silu(gates * scale) * ups * (scale * weight)).astype(BF16)
        common = common * scale
        shared = (silu(common[:, :sf]) * common[:, sf:] * flag).astype(BF16)
        for g, group in enumerate((soon, rest)):
            for d in group:
                at = pl.ds(pl.multiple_of(along(d) * 2 * width, 2 * width), 2 * width)
                product = jnp.dot(hidden, vm["lower"][:, at], preferred_element_type=F32) + jnp.dot(
                    shared, vm["common_low"][:, at], preferred_element_type=F32
                )
                second_tp.put(d, at_rows, product)
            second_tp.near(q, g)

    second_tp = TpSum(part2, pair2, send2, recv2, near2_r, far2_r, gone2_s, piece_rows)
    expert(0, *absorb(3, 0))
    for q in range(1, CHUNKS):
        ready = absorb(3, q)
        second_tp.leg1(q - 1)
        expert(q, *ready)
    second_tp.leg1(CHUNKS - 1)
    for q in range(CHUNKS):
        second_tp.neighbours(q)
    for q in range(CHUNKS):
        second_tp.leg2(q)
    for q in range(CHUNKS):
        value = second_tp.total(q)
        share_sp = n_sp // CHUNKS
        owners = slice(q * share_sp, (q + 1) * share_sp)
        spots = slice(q * share_sp * stride, (q + 1) * share_sp * stride)
        rsend[owners] = (
            mm(widen[spots, rows_of(q)], value)
            .astype(BF16)
            .reshape(share_sp, stride, rows)
        )
        for k in range(share_sp):
            to = q * share_sp + lax.rem(s + k, share_sp)

            @pl.when(to != s)
            def _(to=to):
                scattered(rsend, returned, ret_s, to).start()

    returned[s] = rsend[s]
    back = collected(returned, ret_s)
    mixture = mm(undo[...], back)
    second_sum = ALPHA * middle.astype(F32) + mixture
    sums = [jnp.sum(v, -1, keepdims=True) for v in (second_sum, second_sum * second_sum)]
    tell(stat2, sq2_s, jnp.concatenate([to_row(v) for v in sums], axis=0))
    totals = heard_all(stat2, sq2_s) / features
    mean2, square2 = totals[0:1, :], totals[1:2, :]
    scale2 = lax.rsqrt(square2 - mean2 * mean2 + 1e-05)
    out_ref[...] = (
        (second_sum - to_col(mean2)) * to_col(scale2) * vm["gain2"][...]
    ).astype(BF16)

    for copy in first:
        copy.wait_send()
    second.wait_send()
    def all_gone(there, sem):
        remote(there, there, sem, sem, at_tp(t)).wait_send()

    all_gone(pair2, gone_s.at[0])
    all_gone(pair2.at[1:ny], gone_s.at[1])
    first_tp.all_gone()
    second_tp.all_gone()


def dims_names():
    return (
        "probe", "address", "content", "storage", "fade", "extra", "label",
        "picks", "share", "exit", "incoming", "gain1", "gain2", "final",
        "valve", "raise", "lower", "common", "common_raise", "common_low", "channel",
    )


def shards(
    probe, address, content, storage, fade, channel, extra, label, exit_valve, final,
    incoming, gain1, picks, share, valve, raising, lowering, common_valve, common_raising,
    common_lowering, gain2,
):
    n_sp, n_tp = lax.axis_size("sp"), lax.axis_size("tp")
    ny = n_tp // 2
    rows, width = probe.shape
    experts = n_sp * valve.shape[0]
    cap = max(2, 9 * rows * picks.shape[1] // (8 * experts))
    stride = -(-(cap + 2) // 16) * 16
    slots = n_sp * cap
    ff, features = valve.shape[2], valve.shape[1]
    sf = common_valve.shape[1]
    dims = (n_sp, n_tp, rows, experts, cap, stride)
    args = {
        "probe": probe, "address": address, "content": content, "storage": storage,
        "fade": fade, "extra": extra, "label": label[None, :], "picks": picks.T,
        "share": share.T, "exit": exit_valve, "incoming": incoming, "gain1": gain1[None, :],
        "gain2": gain2[None, :], "final": final, "valve": valve[0], "raise": raising[0],
        "lower": lowering[0],
        "common": common_valve.T, "common_raise": common_raising.T,
        "common_low": common_lowering, "channel": channel[None, :],
    }
    names = dims_names()
    operands = [
        args[n] if n == "channel" else pltpu.with_memory_space_constraint(args[n], pltpu.HBM)
        for n in names
    ]
    dma = pltpu.SemaphoreType.DMA
    shapes = {n: a.shape for n, a in args.items()}
    shapes["common"] = (2 * sf, features)
    shapes["common_raise"] = (8, 128)
    own = [pltpu.VMEM(shapes[n], args[n].dtype) for n in names]

    def vmem(*shape, kind=BF16):
        return pltpu.VMEM(shape, kind)

    return pl.pallas_call(
        functools.partial(kernel, dims),
        out_shape=jax.ShapeDtypeStruct((rows, width), BF16),
        in_specs=[pl.BlockSpec(memory_space=pltpu.HBM)] * len(operands),
        out_specs=pl.BlockSpec(memory_space=pltpu.VMEM),
        scratch_shapes=own
        + [
            vmem(2 * width + 16, width), vmem(REACH, 2 * width + 16, width),
            vmem(width, width), vmem(width, width),
            vmem(ny, 2, rows, width), vmem(ny, rows, width), vmem(7, rows, width),
            vmem(7, rows, width),
            vmem(n_tp, 1, rows, kind=F32), vmem(n_tp, 1, rows, kind=F32),
            vmem(n_tp, 2, rows, kind=F32),
            vmem(n_sp, stride, width), vmem(n_sp, stride, width),
            vmem(n_sp, 8, width), vmem(n_sp, 8, width),
            vmem(ny, slots, 2 * width), vmem(2, slots, ff, kind=F32), vmem(slots, 2 * sf, kind=F32),
            vmem(ny, 2, slots, width), vmem(ny, slots, width), vmem(7, slots, width),
            vmem(7, slots, width),
            vmem(n_sp, stride, width), vmem(n_sp, stride, width),
            vmem(rows, n_sp * stride), vmem(n_sp * stride, slots),
            dma((len(operands),)), dma((REACH,)), dma((REACH,)), dma((2,)),
            dma((2 * CHUNKS,)), dma((2 * CHUNKS,)), dma((2,)), dma((2,)), dma((2,)), dma((2,)),
            dma((2,)), dma((2,)), dma((2,)), dma((3 * CHUNKS,)), dma((4 * CHUNKS,)),
            dma((2,)), dma((2 * CHUNKS,)), dma((2 * CHUNKS,)), dma((2,)),
        ],
        compiler_params=pltpu.CompilerParams(
            collective_id=0, has_side_effects=True, vmem_limit_bytes=48 * 1024 * 1024
        ),
        name="layer",
    )(*operands)


def solution(mesh):
    return jax.shard_map(
        shards,
        mesh=mesh,
        in_specs=(
            P("sp", "tp"), P("sp", "tp"), P("sp", "tp"), P("tp", "sp"), P("tp", "sp"), P("tp"),
            P("tp", "sp"), P("sp"), P("sp", "tp"), P("tp", None), P("sp", "tp"), P("tp"),
            P("sp", None), P("sp", None), P("sp", None, "tp"), P("sp", None, "tp"),
            P("sp", "tp", None), P(None, "tp"), P(None, "tp"), P("tp", None), P("tp"),
        ),
        out_specs=P("sp", "tp"),
        check_vma=False,
    )
```

```python
import functools

import jax
import jax.numpy as jnp
from jax import lax
from jax.experimental import pallas as pl
from jax.experimental.pallas import tpu as pltpu
from jax.sharding import PartitionSpec as P

BLOCK = 64
ALPHA = 2.0**0.25
F32 = jnp.float32
BF16 = jnp.bfloat16
MESH = pl.DeviceIdType.MESH
REACH = 3
CHUNKS = 2


def iota(shape, dim):
    return lax.broadcasted_iota(jnp.int32, shape, dim)


def mm(a, b):
    return jnp.dot(a.astype(BF16), b.astype(BF16), preferred_element_type=F32)


def mm_nt(a, b):
    return lax.dot_general(
        a.astype(BF16), b.astype(BF16), (((1,), (1,)), ((), ())), preferred_element_type=F32
    )


def mm_tn(a, b):
    return lax.dot_general(
        a.astype(BF16), b.astype(BF16), (((0,), (0,)), ((), ())), preferred_element_type=F32
    )


def silu(v):
    return v / (1.0 + jnp.exp(-v))


def kernel(dims, *refs):
    n_sp, n_tp, rows, experts, cap, stride = dims
    ny = n_tp // 2
    slots = n_sp * cap
    padded = n_sp * stride
    names = dims_names()
    hbm = dict(zip(names, refs[: len(names)]))
    out_ref = refs[len(names)]
    scratch = refs[len(names) + 1 :]
    vm = dict(zip(names, scratch[: len(names)]))
    (
        pay, pieces, carry_out, carry_in,
        part1, pair1, send1, recv1,
        stat0, stat1, stat2,
        sent, arrived, told, heard, gathered, acc_g, acc_s,
        part2, pair2, send2, recv2,
        rsend, returned, undo, widen,
        met, load_sem, pa_s, pa_r, pb_s,
        near1_r, far1_r, gone1_s, mean_s, sq1_s, sq2_s,
        dis_s, note_s, ret_s, wire_r, own_r, gone_s,
        near2_r, far2_r, gone2_s,
    ) = scratch[len(names) :]

    s = lax.axis_index("sp")
    t = lax.axis_index("tp")
    y = t // 2
    c = lax.rem(t, 2)
    other = 1 - c

    def at_sp(k):
        return {"sp": k, "tp": t}

    def at_tp(k):
        return {"sp": s, "tp": k}

    def remote(src, dst, send_sem, recv_sem, device):
        return pltpu.make_async_remote_copy(
            src_ref=src, dst_ref=dst, send_sem=send_sem, recv_sem=recv_sem,
            device_id=device, device_id_type=MESH,
        )

    barrier = pltpu.get_barrier_semaphore()

    nx = 4
    nz = n_sp // nx
    hops = sorted(
        ((dz, dx) for dz in range(nz) for dx in range(nx) if dz or dx),
        key=lambda d: -min(d[0], nz - d[0]) - min(d[1], nx - d[1]),
    )
    z, x = s // nx, lax.rem(s, nx)

    def beside(dz, dx):
        return lax.rem(z + dz, nz) * nx + lax.rem(x + dx, nx)

    lines = [d for d in hops if not (d[0] and d[1])]
    for dz, dx in lines:
        pl.semaphore_signal(
            barrier, inc=1, device_id=at_sp(beside(dz, dx)), device_id_type=MESH
        )
    for k in range(1, REACH + 1):
        for to in (s + k, s - k + n_sp):
            pl.semaphore_signal(
                barrier, inc=1, device_id=at_sp(lax.rem(to, n_sp)), device_id_type=MESH
            )
    for k in sorted(range(1, n_tp), key=lambda k: -min(k, n_tp - k)):
        pl.semaphore_signal(
            barrier, inc=1, device_id=at_tp(lax.rem(t + k, n_tp)), device_id_type=MESH
        )
    sf = vm["common"].shape[0] // 2
    loads = {}
    for k, name in enumerate(names):
        into = vm[name]
        if name == "common":
            into = vm["common"].at[0:sf]
        if name == "common_raise":
            into = vm["common"].at[sf:]
        loads[name] = pltpu.make_async_copy(hbm[name], into, load_sem.at[k])
    early = ("probe", "address", "content", "storage", "fade", "extra", "channel", "label")
    for name in early:
        loads[name].start()
    for name in names:
        if name not in early:
            loads[name].start()
    for name in early:
        loads[name].wait()

    row_i, col_i = iota((rows, rows), 0), iota((rows, rows), 1)
    eye = row_i == col_i
    lower, strict = row_i >= col_i, row_i > col_i
    same_block = (row_i < BLOCK) == (col_i < BLOCK)

    def to_col(row):
        return jnp.sum(jnp.where(eye, row, 0.0), axis=1, keepdims=True)

    def to_row(col):
        return jnp.sum(jnp.where(eye, col, 0.0), axis=0, keepdims=True)

    queries = vm["probe"][...].astype(F32)
    keys = vm["address"][...].astype(F32)
    values = vm["content"][...].astype(F32)
    q_unit = queries * lax.rsqrt(
        jnp.sum(queries * queries, -1, keepdims=True) + 1e-06
    ) * queries.shape[-1] ** (-0.5)
    k_unit = keys * lax.rsqrt(jnp.sum(keys * keys, -1, keepdims=True) + 1e-06)
    gate = to_col(1.0 / (1.0 + jnp.exp(-vm["storage"][...])))
    fade = vm["fade"][...]
    softplus = jnp.maximum(fade, 0.0) + jnp.log(1.0 + jnp.exp(-jnp.abs(fade)))
    rate = jnp.exp(vm["channel"][...])
    decay = vm["extra"][...] - rate * softplus
    c_col = jnp.sum(jnp.where(lower, decay, 0.0), axis=1, keepdims=True)
    c_row = to_row(c_col)
    label_row = vm["label"][...].astype(F32)
    label_col = to_col(label_row)
    label_first, label_last = label_row[:, :1], label_row[:, rows - 1 :]
    c_last = c_row[:, rows - 1 :]
    reach = jnp.where(
        lower & (label_col == label_row), jnp.exp(jnp.where(lower, c_col - c_row, 0.0)), 0.0
    )
    weighted = k_unit * gate
    coupling = jnp.where(strict, mm_nt(weighted, k_unit) * reach, 0.0)
    power = jnp.where(same_block, coupling, 0.0)
    across = jnp.where(same_block, 0.0, coupling)
    inverse = jnp.where(eye, 1.0, 0.0) - power
    for _ in range(BLOCK.bit_length() - 2):
        power = mm(power, power)
        inverse = inverse + mm(inverse, power)
    inverse = inverse - mm(inverse, mm(across, inverse))
    growth = jnp.exp(c_col) * (label_col == label_first).astype(F32)
    both = mm(inverse, jnp.concatenate([weighted * growth, values * gate], axis=1))
    tail_keys = k_unit * (jnp.exp(c_last - c_col) * (label_col == label_last).astype(F32))
    ends = mm_tn(tail_keys, both)
    end_growth = jnp.exp(c_last) * (label_last == label_first).astype(F32)
    scores = mm_nt(q_unit, k_unit) * reach
    outs = mm(scores, both)
    width = q_unit.shape[-1]
    q_grown = q_unit * growth - outs[:, :width]
    own_mixed = outs[:, width:]
    state_map = (jnp.where(eye, end_growth, 0.0) - ends[:, :width]).astype(BF16)
    shift = ends[:, width:]
    marks_at = width + 16
    pay[0:width, :] = shift.astype(BF16)
    pay[width : width + 8, :] = jnp.broadcast_to(label_first, (8, width)).astype(BF16)
    pay[width + 8 : marks_at, :] = jnp.broadcast_to(label_last, (8, width)).astype(BF16)
    pay[marks_at:, :] = state_map
    pl.semaphore_wait(barrier, len(lines) + 2 * REACH + n_tp - 1)
    tops = [pay.shape[0]] * (REACH - 1) + [marks_at]
    first = [
        remote(
            pay.at[0:top], pieces.at[k, 0:top], pa_s.at[k], pa_r.at[k],
            at_sp(lax.rem(s + k + 1, n_sp)),
        )
        for k, top in enumerate(tops)
    ]
    for k in (1, 2, 0):
        first[k].start()

    for dz in range(1, nz):
        pl.semaphore_signal(met, inc=1, device_id=at_sp(beside(dz, 0)), device_id_type=MESH)

    for name in names:
        if name not in early:
            loads[name].wait()
    pick0, pick1 = vm["picks"][0:1, :], vm["picks"][1:2, :]
    share = vm["share"][...].astype(F32)
    expert_i = iota((experts, rows), 0)
    to0, to1 = (expert_i == pick0).astype(F32), (expert_i == pick1).astype(F32)
    chosen = to0 + to1
    rank = mm(chosen, (row_i < col_i).astype(F32))
    coded = jnp.where(chosen > 0.0, rank + 1.0, 0.0)
    shares = to0 * share[0:1, :] + to1 * share[1:2, :]
    slot_i = iota((padded, experts), 0)
    from_e = iota((padded, experts), 1) * stride
    spread = ((slot_i >= from_e) & (slot_i < from_e + stride)).astype(F32)
    place = iota((n_sp, stride, rows), 1).reshape(padded, rows)
    wide = mm(spread, jnp.concatenate([coded, shares, to0], axis=1))
    hot = wide[:, :rows] == (place + 1).astype(F32)
    dispatch = hot.astype(BF16)
    undo[...] = hot.astype(F32).T.astype(BF16)
    slot_share = jnp.sum(jnp.where(hot, wide[:, rows : 2 * rows], 0.0), axis=1, keepdims=True)
    slot_first = jnp.sum(jnp.where(hot, wide[:, 2 * rows :], 0.0), axis=1, keepdims=True)
    here = (iota((padded, rows), 1) == place).astype(F32)

    def per_slot(column):
        return jnp.sum((here * column).reshape(n_sp, stride, rows), axis=1, keepdims=True)

    told[...] = jnp.zeros_like(told)
    told[:, 0:1, :] = per_slot(slot_share).astype(BF16)
    told[:, 1:2, :] = per_slot(slot_first).astype(BF16)
    compact_i = iota((slots, padded), 0).astype(F32)
    source = jnp.floor((compact_i + 0.5) * (1.0 / cap))
    within = compact_i - source * cap
    column = iota((slots, padded), 1).astype(F32)
    compact = (column == source * stride + within).astype(BF16)
    open_i = iota((padded, slots), 1).astype(F32)
    open_source = jnp.floor((open_i + 0.5) * (1.0 / cap))
    spread_out = (
        iota((padded, slots), 0).astype(F32) == open_source * (stride - cap) + open_i
    ).astype(BF16)
    widen[...] = spread_out
    slot_lane = iota((slots, rows), 1).astype(F32) == within[:, :rows]
    valve = silu(vm["exit"][...].astype(F32))

    for k in range(REACH):
        first[k].wait_recv()

    def piece(k):
        label = pieces[k, width:marks_at, :].astype(F32)
        return pieces[k, 0:width, :], label[0:1, :], label[8:9, :]

    shift1, first1, last1 = piece(0)
    shift2, first2, last2 = piece(1)
    shift3, _, last3 = piece(2)
    map1 = pieces[0, marks_at:, :] * (first1 == last2).astype(BF16)
    map2 = pieces[1, marks_at:, :] * (first2 == last3).astype(BF16)
    joined = (label_first == last1).astype(F32)
    shift12 = shift1.astype(F32) + mm(map1, shift2)
    map12 = mm(map1, map2).astype(BF16)
    entering = (shift12 + mm(map12, shift3)) * joined
    carry_out[...] = (shift + mm(state_map, entering)).astype(BF16)
    second = remote(
        carry_out, carry_in, pb_s.at[0], pb_s.at[1], at_sp(lax.rem(s + REACH, n_sp))
    )
    second.start()
    from_carry = mm(q_grown, map12).astype(BF16)
    known = own_mixed + mm(q_grown, shift12) * joined
    second.wait_recv()
    mixed = known + mm(from_carry, carry_in[...]) * joined
    scaled = mixed * lax.rsqrt(jnp.mean(mixed * mixed, -1, keepdims=True) + 1e-06)
    heads_out = (scaled * valve).astype(BF16)

    def along(d):
        return lax.rem(y + d + 2 * ny, ny)

    def sigma_of(q):
        return 1 if q % 2 == 0 else -1

    soon, rest = (3, -3, 4), (1, -1, 2, -2, 0)

    class TpSum:
        def __init__(self, part, pair, send, recv, near_r, far_r, gone, chunk_rows):
            self.part, self.pair, self.send, self.recv = part, pair, send, recv
            self.near_r, self.far_r, self.gone, self.rows = near_r, far_r, gone, chunk_rows

        def at(self, q):
            return slice(q * self.rows, (q + 1) * self.rows)

        def put(self, d, at_rows, product):
            chip = along(d)
            self.part[chip, 0, at_rows] = product[:, :width].astype(BF16)
            self.part[chip, 1, at_rows] = product[:, width:].astype(BF16)

        def near(self, q, g):
            for d in (soon, rest)[g]:
                chip = along(d)
                remote(
                    self.part.at[chip, other, self.at(q)], self.pair.at[chip, self.at(q)],
                    self.gone.at[0], self.near_r.at[2 * q + g], at_tp(2 * y + other),
                ).start()

        def near_wait(self, q, g):
            there = self.pair.at[0 : len((soon, rest)[g]), self.at(q)]
            sem = self.near_r.at[2 * q + g]
            remote(there, there, sem, sem, at_tp(t)).wait_recv()

        def chip_sum(self, d, q):
            chip = along(d)
            mine = self.part[chip, c, self.at(q)].astype(F32)
            return mine + self.pair[chip, self.at(q)].astype(F32)

        def copy(self, line, q, to):
            return remote(
                self.send.at[line, self.at(q)], self.recv.at[line, self.at(q)], self.gone.at[1],
                self.far_r.at[(line > 2) * CHUNKS + q], at_tp(2 * along(to) + c),
            )

        def go(self, line, q, to, value):
            self.send[line, self.at(q)] = value.astype(BF16)
            self.copy(line, q, to).start()

        def got_all(self, first, last, q):
            there = self.recv.at[first:last, self.at(q)]
            sem = self.far_r.at[(first > 2) * CHUNKS + q]
            remote(there, there, sem, sem, at_tp(t)).wait_recv()

        def got(self, line, q):
            return self.recv[line, self.at(q)].astype(F32)

        def leg1(self, q):
            self.near_wait(q, 0)
            self.go(2, q, -2 * sigma_of(q), self.chip_sum(4, q))
            for i, sigma in enumerate((1, -1)):
                self.go(i, q, -sigma, self.chip_sum(-3 * sigma, q))

        def neighbours(self, q):
            self.near_wait(q, 1)
            for i, sigma in enumerate((1, -1)):
                self.go(3 + i, q, sigma, self.chip_sum(sigma, q))

        def leg2(self, q):
            self.got_all(0, 3, q)
            for i, sigma in enumerate((1, -1)):
                value = self.chip_sum(-2 * sigma, q) + self.got(i, q)
                if sigma == sigma_of(q):
                    value = value + self.got(2, q)
                self.go(5 + i, q, -2 * sigma, value)

        def total(self, q):
            value = self.chip_sum(0, q)
            self.got_all(3, 7, q)
            for line in (3, 4, 5, 6):
                value = value + self.got(line, q)
            return value

        def all_gone(self):
            there = self.part.at[:, 0]
            remote(there, there, self.gone.at[0], self.gone.at[0], at_tp(t)).wait_send()
            remote(
                self.send, self.send, self.gone.at[1], self.gone.at[1], at_tp(t)
            ).wait_send()

    def tell(stat, sems, line):
        stat[t] = line
        for k in sorted(range(1, n_tp), key=lambda k: -min(k, n_tp - k)):
            to = lax.rem(t + k, n_tp)
            remote(stat.at[t], stat.at[t], sems.at[0], sems.at[1], at_tp(to)).start()

    def heard_all(stat, sems):
        there = stat.at[1:n_tp]
        remote(there, there, sems.at[0], sems.at[1], at_tp(t)).wait()
        return jnp.sum(stat[...], axis=0)

    scaled_in = ALPHA * vm["incoming"][...].astype(F32)
    row_sum = jnp.sum(scaled_in, -1, keepdims=True)
    first_tp = TpSum(part1, pair1, send1, recv1, near1_r, far1_r, gone1_s, rows // CHUNKS)
    for g, group in enumerate((soon, rest)):
        for d in group:
            at = pl.ds(pl.multiple_of(along(d) * 2 * width, 2 * width), 2 * width)
            product = mm(heads_out, vm["final"][:, at])
            first_tp.put(d, slice(0, rows), product)
            row_sum = row_sum + jnp.sum(product, -1, keepdims=True)
        for q in range(CHUNKS):
            first_tp.near(q, g)
    for q in range(CHUNKS):
        first_tp.leg1(q)
    tell(stat0, mean_s, to_row(row_sum))
    for q in range(CHUNKS):
        first_tp.neighbours(q)
    for q in range(CHUNKS):
        first_tp.leg2(q)
    projected = jnp.concatenate([first_tp.total(q) for q in range(CHUNKS)], axis=0)
    features = width * n_tp
    mean = to_col(heard_all(stat0, mean_s) / features)
    centred = scaled_in + projected - mean

    sent_rows = -(-cap // 2) * 2

    def scattered(src, dst, sems, to):
        top = min(src.shape[1], sent_rows)
        return remote(
            src.at[to, 0:top], dst.at[s, 0:top], sems.at[0], sems.at[1], at_sp(to)
        )

    def scatter(src, dst, sems):
        for dz, dx in hops:
            scattered(src, dst, sems, beside(dz, dx)).start()
        dst[s] = src[s]

    def collected(dst, sems):
        top = min(dst.shape[1], sent_rows)
        there = dst.at[1:n_sp, 0:top]
        remote(there, there, sems.at[0], sems.at[1], at_sp(s)).wait()
        return as_rows(dst[...], top)

    def as_rows(came, top):
        shape = came.shape
        came = jnp.where(iota(shape, 1) < top, came.astype(F32), 0.0).astype(BF16)
        return came.reshape(shape[0] * shape[1], shape[2])

    gained = (centred * vm["gain1"][...]).astype(BF16)
    payload = jnp.dot(dispatch, gained, preferred_element_type=F32)
    sent[...] = payload.astype(BF16).reshape(n_sp, stride, rows)
    if nz > 1:
        pl.semaphore_wait(met, nz - 1)
    scatter(sent, arrived, dis_s)
    tell(stat1, sq1_s, to_row(jnp.sum(centred * centred, -1, keepdims=True)))
    came = collected(arrived, dis_s)
    lanes = pl.ds(pl.multiple_of(c * width, width), width)
    piece_rows = slots // CHUNKS

    def rows_of(q):
        return slice(q * piece_rows, (q + 1) * piece_rows)

    def block(chip, q):
        return gathered.at[chip, rows_of(q), lanes]

    chips_of = ((0,), (2, -2), (1, -1), (3, -3, 4))

    def passed(d, q, to, late):
        there = block(along(d), q)
        sem = wire_r.at[late * CHUNKS + q]
        remote(there, there, gone_s.at[1], sem, at_tp(2 * along(to) + c)).start()

    def hand(k, q):
        for d in chips_of[k]:
            there = block(along(d), q)
            remote(
                there, there, gone_s.at[0], own_r.at[k * CHUNKS + q], at_tp(2 * y + other)
            ).start()

    def wait_bytes(count, sem):
        there = pair2.at[0:count, 0:piece_rows]
        remote(there, there, sem, sem, at_tp(t)).wait_recv()

    def absorb(k, q):
        chips, at_rows = [along(d) for d in chips_of[k]], rows_of(q)
        wait_bytes(len(chips), own_r.at[k * CHUNKS + q])
        gates = ups = common = 0.0
        for chip in chips:
            block_in = gathered[chip, at_rows, :]
            at = pl.ds(pl.multiple_of(chip * 2 * width, 2 * width), 2 * width)
            gates += jnp.dot(block_in, vm["valve"][at, :], preferred_element_type=F32)
            ups += jnp.dot(block_in, vm["raise"][at, :], preferred_element_type=F32)
            common += lax.dot_general(
                block_in, vm["common"][:, at], (((1,), (1,)), ((), ())), preferred_element_type=F32
            )
        if k:
            gates, ups = gates + acc_g[0, at_rows], ups + acc_g[1, at_rows]
            common = common + acc_s[at_rows]
        if k < 3:
            acc_g[0, at_rows], acc_g[1, at_rows], acc_s[at_rows] = gates, ups, common
        return gates, ups, common

    def all_noted():
        notes = collected(heard, note_s)
        note_column = iota((slots, notes.shape[0]), 1).astype(F32)
        note_source = source[:, :1] * told.shape[1]

        def noted(j):
            line = (note_column == note_source + j).astype(BF16)
            found = jnp.dot(line, notes, preferred_element_type=F32)
            return jnp.sum(jnp.where(slot_lane, found, 0.0), axis=1, keepdims=True)

        return noted(0), noted(1), noted(2) + noted(3)

    for q in range(CHUNKS):
        found = jnp.dot(compact[rows_of(q)], came, preferred_element_type=F32)
        gathered[y, rows_of(q), lanes] = found.astype(BF16)
        for sigma in (1, -1):
            passed(0, q, 2 * sigma, 0)
    for q in range(CHUNKS):
        for sigma in (1, -1):
            passed(0, q, sigma, 1)
    for q in range(CHUNKS):
        hand(0, q)
    row_scale = lax.rsqrt(heard_all(stat1, sq1_s) / features + 1e-05)
    slot_scale = jnp.sum(jnp.where(hot, row_scale, 0.0), axis=1, keepdims=True)
    scales = per_slot(slot_scale)
    coarse = scales.astype(BF16)
    told[:, 2:3, :] = coarse
    told[:, 3:4, :] = (scales - coarse.astype(F32)).astype(BF16)
    scatter(told, heard, note_s)
    middle = (centred * to_col(row_scale) * vm["gain1"][...]).astype(BF16)
    for q in range(CHUNKS):
        wait_bytes(2, wire_r.at[q])
        for sigma in (1, -1):
            if sigma == sigma_of(q):
                passed(-2 * sigma, q, 2 * sigma, 2)
            passed(-2 * sigma, q, sigma, 2)
        hand(1, q)
    for q in range(CHUNKS):
        absorb(0, q)
    for q in range(CHUNKS):
        wait_bytes(2, wire_r.at[CHUNKS + q])
        hand(2, q)
    for q in range(CHUNKS):
        absorb(1, q)
    slot_notes = all_noted()
    for q in range(CHUNKS):
        wait_bytes(3, wire_r.at[2 * CHUNKS + q])
        hand(3, q)
        if q == 0:
            for k in range(CHUNKS):
                absorb(2, k)

    def expert(q, gates, ups, common):
        at_rows = rows_of(q)
        weight, flag, scale = (v[at_rows] for v in slot_notes)
        hidden = (silu(gates * scale) * ups * (scale * weight)).astype(BF16)
        common = common * scale
        shared = (silu(common[:, :sf]) * common[:, sf:] * flag).astype(BF16)
        for g, group in enumerate((soon, rest)):
            for d in group:
                at = pl.ds(pl.multiple_of(along(d) * 2 * width, 2 * width), 2 * width)
                product = jnp.dot(hidden, vm["lower"][:, at], preferred_element_type=F32) + jnp.dot(
                    shared, vm["common_low"][:, at], preferred_element_type=F32
                )
                second_tp.put(d, at_rows, product)
            second_tp.near(q, g)

    second_tp = TpSum(part2, pair2, send2, recv2, near2_r, far2_r, gone2_s, piece_rows)
    expert(0, *absorb(3, 0))
    for q in range(1, CHUNKS):
        ready = absorb(3, q)
        second_tp.leg1(q - 1)
        expert(q, *ready)
    second_tp.leg1(CHUNKS - 1)
    for q in range(CHUNKS):
        second_tp.neighbours(q)
    for q in range(CHUNKS):
        second_tp.leg2(q)
    for q in range(CHUNKS):
        value = second_tp.total(q)
        share_sp = n_sp // CHUNKS
        owners = slice(q * share_sp, (q + 1) * share_sp)
        spots = slice(q * share_sp * stride, (q + 1) * share_sp * stride)
        rsend[owners] = (
            mm(widen[spots, rows_of(q)], value)
            .astype(BF16)
            .reshape(share_sp, stride, rows)
        )
        for k in range(share_sp):
            to = q * share_sp + lax.rem(s + k, share_sp)

            @pl.when(to != s)
            def _(to=to):
                scattered(rsend, returned, ret_s, to).start()

    returned[s] = rsend[s]
    back = collected(returned, ret_s)
    mixture = mm(undo[...], back)
    second_sum = ALPHA * middle.astype(F32) + mixture
    sums = [jnp.sum(v, -1, keepdims=True) for v in (second_sum, second_sum * second_sum)]
    tell(stat2, sq2_s, jnp.concatenate([to_row(v) for v in sums], axis=0))
    totals = heard_all(stat2, sq2_s) / features
    mean2, square2 = totals[0:1, :], totals[1:2, :]
    scale2 = lax.rsqrt(square2 - mean2 * mean2 + 1e-05)
    out_ref[...] = (
        (second_sum - to_col(mean2)) * to_col(scale2) * vm["gain2"][...]
    ).astype(BF16)

    for copy in first:
        copy.wait_send()
    second.wait_send()
    def all_gone(there, sem):
        remote(there, there, sem, sem, at_tp(t)).wait_send()

    all_gone(pair2, gone_s.at[0])
    all_gone(pair2.at[1:ny], gone_s.at[1])
    first_tp.all_gone()
    second_tp.all_gone()


def dims_names():
    return (
        "probe", "address", "content", "storage", "fade", "extra", "label",
        "picks", "share", "exit", "incoming", "gain1", "gain2", "final",
        "valve", "raise", "lower", "common", "common_raise", "common_low", "channel",
    )


def shards(
    probe, address, content, storage, fade, channel, extra, label, exit_valve, final,
    incoming, gain1, picks, share, valve, raising, lowering, common_valve, common_raising,
    common_lowering, gain2,
):
    n_sp, n_tp = lax.axis_size("sp"), lax.axis_size("tp")
    ny = n_tp // 2
    rows, width = probe.shape
    experts = n_sp * valve.shape[0]
    cap = max(2, 9 * rows * picks.shape[1] // (8 * experts))
    stride = -(-(cap + 2) // 16) * 16
    slots = n_sp * cap
    ff, features = valve.shape[2], valve.shape[1]
    sf = common_valve.shape[1]
    dims = (n_sp, n_tp, rows, experts, cap, stride)
    args = {
        "probe": probe, "address": address, "content": content, "storage": storage,
        "fade": fade, "extra": extra, "label": label[None, :], "picks": picks.T,
        "share": share.T, "exit": exit_valve, "incoming": incoming, "gain1": gain1[None, :],
        "gain2": gain2[None, :], "final": final, "valve": valve[0], "raise": raising[0],
        "lower": lowering[0],
        "common": common_valve.T, "common_raise": common_raising.T,
        "common_low": common_lowering, "channel": channel[None, :],
    }
    names = dims_names()
    operands = [
        args[n] if n == "channel" else pltpu.with_memory_space_constraint(args[n], pltpu.HBM)
        for n in names
    ]
    dma = pltpu.SemaphoreType.DMA
    shapes = {n: a.shape for n, a in args.items()}
    shapes["common"] = (2 * sf, features)
    shapes["common_raise"] = (8, 128)
    own = [pltpu.VMEM(shapes[n], args[n].dtype) for n in names]

    def vmem(*shape, kind=BF16):
        return pltpu.VMEM(shape, kind)

    return pl.pallas_call(
        functools.partial(kernel, dims),
        out_shape=jax.ShapeDtypeStruct((rows, width), BF16),
        in_specs=[pl.BlockSpec(memory_space=pltpu.HBM)] * len(operands),
        out_specs=pl.BlockSpec(memory_space=pltpu.VMEM),
        scratch_shapes=own
        + [
            vmem(2 * width + 16, width), vmem(REACH, 2 * width + 16, width),
            vmem(width, width), vmem(width, width),
            vmem(ny, 2, rows, width), vmem(ny, rows, width), vmem(7, rows, width),
            vmem(7, rows, width),
            vmem(n_tp, 1, rows, kind=F32), vmem(n_tp, 1, rows, kind=F32),
            vmem(n_tp, 2, rows, kind=F32),
            vmem(n_sp, stride, width), vmem(n_sp, stride, width),
            vmem(n_sp, 8, width), vmem(n_sp, 8, width),
            vmem(ny, slots, 2 * width), vmem(2, slots, ff, kind=F32), vmem(slots, 2 * sf, kind=F32),
            vmem(ny, 2, slots, width), vmem(ny, slots, width), vmem(7, slots, width),
            vmem(7, slots, width),
            vmem(n_sp, stride, width), vmem(n_sp, stride, width),
            vmem(rows, n_sp * stride), vmem(n_sp * stride, slots),
            pltpu.SemaphoreType.REGULAR, dma((len(operands),)), dma((REACH,)), dma((REACH,)), dma((2,)),
            dma((2 * CHUNKS,)), dma((2 * CHUNKS,)), dma((2,)), dma((2,)), dma((2,)), dma((2,)),
            dma((2,)), dma((2,)), dma((2,)), dma((3 * CHUNKS,)), dma((4 * CHUNKS,)),
            dma((2,)), dma((2 * CHUNKS,)), dma((2 * CHUNKS,)), dma((2,)),
        ],
        compiler_params=pltpu.CompilerParams(
            collective_id=0, has_side_effects=True, vmem_limit_bytes=48 * 1024 * 1024
        ),
        name="layer",
    )(*operands)


def solution(mesh):
    return jax.shard_map(
        shards,
        mesh=mesh,
        in_specs=(
            P("sp", "tp"), P("sp", "tp"), P("sp", "tp"), P("tp", "sp"), P("tp", "sp"), P("tp"),
            P("tp", "sp"), P("sp"), P("sp", "tp"), P("tp", None), P("sp", "tp"), P("tp"),
            P("sp", None), P("sp", None), P("sp", None, "tp"), P("sp", None, "tp"),
            P("sp", "tp", None), P(None, "tp"), P(None, "tp"), P("tp", None), P("tp"),
        ),
        out_specs=P("sp", "tp"),
        check_vma=False,
    )
```
